32 devices in a mesh: dp: 4 (over y, x), kv: 4 (over z), tp: 2 (over core).
Axes of the slice: x: 2, y: 2, z: 4, core: 2. Of those that a mesh axis runs over, the one named last changes fastest.
Arguments:
- resid: bfloat16 [16, 2048], P('dp', ('kv', 'tp')), may hold values from -45 to 45
- norm_gain: bfloat16 [3, 2048], P(None, ('kv', 'tp')), may hold values from 0.099609375 to 1.8984375
- ffn_gate: bfloat16 [2, 2048, 5632], P(None, None, ('kv', 'tp')), may hold values from -0.125 to 0.125
- ffn_up: bfloat16 [2, 2048, 5632], P(None, None, ('kv', 'tp')), may hold values from -0.125 to 0.125
- ffn_down: bfloat16 [2, 5632, 2048], P(None, ('kv', 'tp')), may hold values from -0.109375 to 0.109375
- w_x: bfloat16 [2048, 64, 64], P(None, 'kv', 'tp'), may hold values from -0.125 to 0.125
- w_z: bfloat16 [2048, 64, 64], P(None, 'kv', 'tp'), may hold values from -0.125 to 0.125
- w_bc: bfloat16 [2048, 2, 8, 128], P('kv'), may hold values from -0.125 to 0.125
- w_dt: bfloat16 [2048, 64], P('kv'), may hold values from -0.125 to 0.125
- dt_bias: float32 [64], replicated, may hold values from -2 to 0.5
- a_log: float32 [64], replicated, may hold values from -1.5 to 1.5
- d_skip: float32 [64], replicated, may hold values from 0.5 to 1.5
- conv_wx: bfloat16 [4, 64, 64], P(None, None, 'tp'), may hold values from -3 to 3
- conv_wbc: bfloat16 [4, 2, 8, 128], replicated, may hold values from -3 to 3
- conv_x: bfloat16 [16, 3, 64, 64], P(('dp', 'kv'), None, None, 'tp'), may hold values from -6 to 6
- conv_bc: bfloat16 [16, 3, 2, 8, 128], P(('dp', 'kv')), may hold values from -6 to 6
- ssm_state: float32 [16, 64, 64, 128], P(('dp', 'kv'), None, 'tp'), may hold values from -3 to 3
- w_out: bfloat16 [64, 64, 2048], P(None, 'tp', 'kv'), may hold values from -0.09375 to 0.09375
Outputs:
- final: bfloat16 [16, 2048], P('dp', ('kv', 'tp'))
The draws below stay inside these ranges and needn't reach their ends.
All inputs are finite; a program needn't handle non-finite values.
Results may differ from the reference program's by a relative error of at most 0.018.
Values may be sent and summed in bfloat16 or wider, within the bound.
A program may use at most 64 MiB of HBM per device.

```python
import math
import jax
import jax.numpy as jnp
from jax import lax

D = 2048
FF = 5632
H = 64
P_SIZE = 64
G = 8
STATE = 128
CONV = 4
SEQ_DEV = 1
BATCH = 16


def draw_resid(key, part):
    first_key = jax.random.fold_in(key, 11)
    second_key = jax.random.fold_in(key, 12)
    third_key = jax.random.fold_in(key, 13)
    columns = jnp.arange(D, dtype=jnp.float32) / D
    col_scale = 0.4 * jnp.exp(jnp.log(6.0) * columns) * jax.random.uniform(second_key, (D,), jnp.float32, 0.5, 1.5)
    row_scale = 0.3 * jnp.exp(jax.random.uniform(third_key, (BATCH, 1), jnp.float32, 0.0, jnp.log(10.0)))
    base = jnp.clip(jax.random.normal(first_key, (BATCH, D), jnp.float32), -4.0, 4.0)
    return (base * col_scale[None, :] * row_scale).astype(jnp.bfloat16)


def strengthened(result, stream_key, source, target, parts, factor):
    def block_of(axis_at):
        return (jnp.arange(result.shape[axis_at]) // (result.shape[axis_at] // parts)).reshape((-1,) + (1,) * (result.ndim - 1 - axis_at))

    near = jax.random.permutation(stream_key, parts)[block_of(target)]
    other_side = (block_of(target) + parts // 2) % parts
    return jnp.where((block_of(source) == near) | (block_of(source) == other_side), factor * result, result)


def steps_of(key, dims, split, low, largest):
    level, own = 1.0, jax.random.fold_in(key, 6)
    for dim, parts in split:
        heights = jnp.exp(jax.random.uniform(jax.random.fold_in(own, dim), (parts,), jnp.float32, low / len(split), largest / len(split)))
        level = level * jnp.repeat(heights, dims[dim] // parts).reshape([-1 if axis == dim else 1 for axis in range(len(dims))])
    return level


def noise(own_key, extent, spread, bound, pieces=(), held_as=jnp.bfloat16):
    values = jax.random.normal(own_key, extent, jnp.float32) * spread
    if len(pieces) > 0:
        values = steps_of(own_key, extent, pieces, -0.22, 0.18) * values
    return jnp.clip(values, min=-bound, max=bound).astype(held_as)


def bell_draw_with(stream_key, shape, deviation, reach, pieces, heavy, held_as=jnp.bfloat16):
    values = deviation * jax.random.normal(stream_key, shape, jnp.float32)
    if pieces:
        values = values * steps_of(stream_key, shape, pieces, -0.22, 0.18)
    return jnp.clip(strengthened(values, jax.random.fold_in(stream_key, 3), *heavy), -reach, reach).astype(held_as)


def setup_inputs(seed: int = 0) -> dict:
    key_list = jax.random.split(jax.random.key(seed), 19)
    return {
        "resid": draw_resid(jax.random.fold_in(key_list[18], 71), 0),
        "norm_gain": jnp.clip(1.0 + 0.18 * jax.random.normal(key_list[1], (3, D), jnp.float32), 0.099609375, 1.8984375).astype(jnp.bfloat16),
        "ffn_gate": noise(key_list[2], (2, D, FF), D ** -0.5, 0.125, ((2, 8),)),
        "ffn_up": noise(key_list[3], (2, D, FF), D ** -0.5, 0.125, ((2, 8),)),
        "ffn_down": bell_draw_with(key_list[4], (2, FF, D), FF ** -0.5, 0.109375, ((1, 8),), (1, 2, 8, 2.0)),
        "w_x": noise(key_list[5], (D, H, P_SIZE), D ** -0.5, 0.125, ((1, 4), (2, 2))),
        "w_z": noise(key_list[6], (D, H, P_SIZE), D ** -0.5, 0.125, ((1, 4), (2, 2))),
        "w_bc": noise(key_list[7], (D, 2, G, STATE), D ** -0.5, 0.125, ((0, 4),)),
        "w_dt": noise(key_list[8], (D, H), D ** -0.5, 0.125, ((0, 4),)),
        "dt_bias": jnp.clip(jax.random.uniform(key_list[9], (H,), jnp.float32, -2.0, 0.5), -2.0, 0.5),
        "a_log": jnp.clip(jax.random.uniform(key_list[10], (H,), jnp.float32, -1.5, 1.5), -1.5, 1.5),
        "d_skip": jnp.clip(jnp.exp(jax.random.uniform(key_list[11], (H,), jnp.float32, math.log(0.5), math.log(1.5))), 0.5, 1.5),
        "conv_wx": noise(key_list[12], (CONV, H, P_SIZE), CONV ** -0.5, 3.0, ((2, 2),)),
        "conv_wbc": noise(key_list[13], (CONV, 2, G, STATE), CONV ** -0.5, 3.0),
        "conv_x": noise(key_list[14], (BATCH, CONV - 1, H, P_SIZE), 1.0, 6.0, ((0, 16), (3, 2))),
        "conv_bc": noise(key_list[15], (BATCH, CONV - 1, 2, G, STATE), 1.0, 6.0, ((0, 16),)),
        "ssm_state": noise(key_list[16], (BATCH, H, P_SIZE, STATE), 0.3, 3.0, ((0, 16), (2, 2)), jnp.float32),
        "w_out": noise(key_list[17], (H, P_SIZE, D), (H * P_SIZE) ** -0.5, 0.09375, ((1, 2), (2, 4))),
    }


EPS = 1e-06

def normalize(rows, gain):
    values = rows.astype(jnp.float32)
    scale = lax.rsqrt(lax.optimization_barrier(jnp.mean(values * values, axis=1, keepdims=True)) + EPS)
    return (values * scale * gain.astype(jnp.float32)[None, :]).astype(jnp.bfloat16)

def feed_forward(normed, w_gate, w_up, w_down):
    gate = jnp.dot(normed, w_gate, preferred_element_type=jnp.float32)
    upper = jnp.dot(normed, w_up, preferred_element_type=jnp.float32)
    hidden = (jax.nn.silu(gate) * upper).astype(jnp.bfloat16)
    return jnp.dot(hidden, w_down, preferred_element_type=jnp.float32)

def short_conv(history, newest, taps):
    window = jnp.concatenate([history.astype(jnp.float32), newest.astype(jnp.float32)[:, None]], axis=1)
    return jax.nn.silu(lax.optimization_barrier(jnp.sum(window * taps.astype(jnp.float32)[None], axis=1)))

def state_step(xs_new, zeta, bc_new, dt_raw, conv_x, conv_bc, ssm_state, conv_wx, conv_wbc, dt_bias, a_log, d_skip):
    xconv = short_conv(conv_x, xs_new, conv_wx)
    bconv = short_conv(conv_bc, bc_new, conv_wbc)
    heads = xconv.shape[1]
    groups = bconv.shape[2]
    bmat = jnp.repeat(bconv[:, 0], heads // groups, axis=1)
    cmat = jnp.repeat(bconv[:, 1], heads // groups, axis=1)
    step_size = jax.nn.softplus(dt_raw + dt_bias[None, :])
    decay = jnp.exp(-step_size * jnp.exp(a_log)[None, :])
    updated = decay[:, :, None, None] * ssm_state + (step_size[:, :, None] * xconv)[..., None] * bmat[:, :, None, :]
    mixed = jnp.einsum('shpn,shn->shp', updated, cmat, precision=lax.Precision.HIGHEST) + d_skip[None, :, None] * xconv
    return (mixed * jax.nn.silu(zeta.astype(jnp.float32))).astype(jnp.bfloat16)

def reference(resid, norm_gain, ffn_gate, ffn_up, ffn_down, w_x, w_z, w_bc, w_dt, dt_bias, a_log, d_skip, conv_wx, conv_wbc, conv_x, conv_bc, ssm_state, w_out):
    total = resid.shape[0]
    heads = w_x.shape[1]
    channels = w_x.shape[2]
    normed = normalize(resid, norm_gain[0])
    first = (resid.astype(jnp.float32) + 0.5 * feed_forward(normed, ffn_gate[0], ffn_up[0], ffn_down[0])).astype(jnp.bfloat16)
    normed = normalize(first, norm_gain[1])
    xs_new = jnp.dot(normed, w_x.reshape(D, -1), preferred_element_type=jnp.float32).astype(jnp.bfloat16).reshape(total, heads, channels)
    zeta = jnp.dot(normed, w_z.reshape(D, -1), preferred_element_type=jnp.float32).astype(jnp.bfloat16).reshape(total, heads, channels)
    bc_new = jnp.dot(normed, w_bc.reshape(D, -1), preferred_element_type=jnp.float32).astype(jnp.bfloat16).reshape((total,) + w_bc.shape[1:])
    dt_raw = jnp.dot(normed, w_dt, preferred_element_type=jnp.float32)
    blocks = total // SEQ_DEV

    def fold(values):
        return values.reshape((blocks, SEQ_DEV) + values.shape[1:])

    def per_block(items):
        return state_step(*items, conv_wx, conv_wbc, dt_bias, a_log, d_skip)
    outputs = lax.map(per_block, (fold(xs_new), fold(zeta), fold(bc_new), fold(dt_raw), fold(conv_x), fold(conv_bc), fold(ssm_state)))
    outputs = outputs.reshape(total, heads * channels)
    second = (first.astype(jnp.float32) + jnp.dot(outputs, w_out.reshape(heads * channels, D), preferred_element_type=jnp.float32)).astype(jnp.bfloat16)
    normed = normalize(second, norm_gain[2])
    final = second.astype(jnp.float32) + 0.5 * feed_forward(normed, ffn_gate[1], ffn_up[1], ffn_down[1])
    return final.astype(jnp.bfloat16)
```

```python
import functools

import jax
import jax.numpy as jnp
from jax import lax
from jax.experimental import pallas as pl
from jax.experimental.pallas import tpu as pltpu
from jax.sharding import PartitionSpec as P

D = 2048
F32 = jnp.float32
BF16 = jnp.bfloat16
MESH = pl.DeviceIdType.MESH

EPS = 1e-06


def normalize(rows, gain):
    values = rows.astype(jnp.float32)
    scale = lax.rsqrt(jnp.mean(values * values, axis=1, keepdims=True) + EPS)
    return (values * scale * gain.astype(jnp.float32).reshape(1, -1)).astype(jnp.bfloat16)


def feed_forward(normed, w_gate, w_up, w_down):
    gate = jnp.dot(normed, w_gate, preferred_element_type=jnp.float32)
    upper = jnp.dot(normed, w_up, preferred_element_type=jnp.float32)
    hidden = (jax.nn.silu(gate) * upper).astype(jnp.bfloat16)
    return jnp.dot(hidden, w_down, preferred_element_type=jnp.float32)


def add_half(base, sums):
    return (base.astype(jnp.float32) + 0.5 * sums).astype(jnp.bfloat16)


def ffn_totals(partial_value):
    return lax.psum(partial_value, ("kv", "tp"))


def short_conv(history, newest, taps):
    window = jnp.concatenate(
        [history.astype(jnp.float32), newest.astype(jnp.float32)[:, None]], axis=1
    )
    return jax.nn.silu(jnp.sum(window * taps.astype(jnp.float32)[None], axis=1))


def state_step(
    xs_new,
    zeta,
    bc_new,
    dt_raw,
    conv_x,
    conv_bc,
    ssm_state,
    conv_wx,
    conv_wbc,
    dt_bias,
    a_log,
    d_skip,
):
    xconv = short_conv(conv_x, xs_new, conv_wx)
    bconv = short_conv(conv_bc, bc_new, conv_wbc)
    heads = xconv.shape[1]
    groups = bconv.shape[2]
    bmat = jnp.repeat(bconv[:, 0], heads // groups, axis=1)
    cmat = jnp.repeat(bconv[:, 1], heads // groups, axis=1)
    step_size = jax.nn.softplus(dt_raw + dt_bias[None, :])
    decay = jnp.exp(-step_size * jnp.exp(a_log)[None, :])
    updated = (
        decay[:, :, None, None] * ssm_state
        + (step_size[:, :, None] * xconv)[..., None] * bmat[:, :, None, :]
    )
    mixed = (
        jnp.einsum("shpn,shn->shp", updated, cmat, precision=lax.Precision.HIGHEST)
        + d_skip[None, :, None] * xconv
    )
    return (mixed * jax.nn.silu(zeta.astype(jnp.float32))).astype(jnp.bfloat16)


def group_terms(slab, w_bc, w_dt):
    span = slab.shape[1]
    flat_bc = w_bc.reshape(span, -1)
    bc_part = jnp.dot(slab, flat_bc, preferred_element_type=jnp.float32)
    dt_part = jnp.dot(slab, w_dt, preferred_element_type=jnp.float32)
    return (
        lax.psum_scatter(bc_part, "kv", scatter_dimension=0, tiled=True),
        lax.psum_scatter(dt_part, "kv", scatter_dimension=0, tiled=True),
    )


def mix_partial(
    normed,
    w_x,
    w_z,
    w_bc,
    w_dt,
    dt_bias,
    a_log,
    d_skip,
    conv_wx,
    conv_wbc,
    conv_x,
    conv_bc,
    ssm_state,
    w_out,
):
    rows = normed.shape[0]
    local_heads = w_x.shape[1]
    half = w_x.shape[2]
    xs_part = (
        jnp.dot(normed, w_x.reshape(D, -1), preferred_element_type=jnp.float32)
        .astype(jnp.bfloat16)
        .reshape(rows, local_heads, half)
    )
    zeta_part = (
        jnp.dot(normed, w_z.reshape(D, -1), preferred_element_type=jnp.float32)
        .astype(jnp.bfloat16)
        .reshape(rows, local_heads, half)
    )
    xs_new, zeta = (
        lax.all_to_all(xs_part, "kv", split_axis=0, concat_axis=1, tiled=True),
        lax.all_to_all(zeta_part, "kv", split_axis=0, concat_axis=1, tiled=True),
    )
    span = w_bc.shape[0]
    slab = lax.dynamic_slice_in_dim(normed, lax.axis_index("kv") * span, span, 1)
    bc_sum, dt_raw = group_terms(slab, w_bc, w_dt)
    bc_new = bc_sum.astype(jnp.bfloat16).reshape((bc_sum.shape[0],) + w_bc.shape[1:])
    mixed = state_step(
        xs_new,
        zeta,
        bc_new,
        dt_raw,
        conv_x,
        conv_bc,
        ssm_state,
        conv_wx,
        conv_wbc,
        dt_bias,
        a_log,
        d_skip,
    )
    flat_out = w_out.reshape(-1, w_out.shape[2])
    piece = lax.all_gather(mixed, "kv", axis=0, tiled=True)
    return jnp.dot(piece.reshape(piece.shape[0], -1), flat_out, preferred_element_type=jnp.float32)


def per_device(
    resid,
    norm_gain,
    ffn_gate,
    ffn_up,
    ffn_down,
    w_x,
    w_z,
    w_bc,
    w_dt,
    dt_bias,
    a_log,
    d_skip,
    conv_wx,
    conv_wbc,
    conv_x,
    conv_bc,
    ssm_state,
    w_out,
):
    mixer_args = (
        w_x,
        w_z,
        w_bc,
        w_dt,
        dt_bias,
        a_log,
        d_skip,
        conv_wx,
        conv_wbc,
        conv_x,
        conv_bc,
        ssm_state,
        w_out,
    )
    rows, gains = (
        lax.all_gather(resid, ("kv", "tp"), axis=1, tiled=True),
        lax.all_gather(norm_gain, ("kv", "tp"), axis=1, tiled=True),
    )
    first = add_half(
        rows,
        ffn_totals(feed_forward(normalize(rows, gains[0]), ffn_gate[0], ffn_up[0], ffn_down[0])),
    )
    partial_value = mix_partial(normalize(first, gains[1]), *mixer_args)
    span = partial_value.shape[1]
    block = lax.dynamic_slice_in_dim(first, lax.axis_index("kv") * span, span, 1)
    joined = (block.astype(jnp.float32) + lax.psum(partial_value, "tp")).astype(jnp.bfloat16)
    second = lax.all_gather(joined, "kv", axis=1, tiled=True)
    final = add_half(
        second,
        ffn_totals(feed_forward(normalize(second, gains[2]), ffn_gate[1], ffn_up[1], ffn_down[1])),
    )
    width = resid.shape[1]
    return lax.dynamic_slice_in_dim(final, lax.axis_index(("kv", "tp")) * width, width, 1)


def nt_dot(left, right):
    return lax.dot_general(left, right, (((1,), (1,)), ((), ())), preferred_element_type=F32)


def nn_dot(left, right):
    return jnp.dot(left, right, preferred_element_type=F32)


def silu(value):
    return value * jax.nn.sigmoid(value)


def norm_rows(values, gain):
    scale = lax.rsqrt(jnp.mean(values * values, axis=1, keepdims=True) + EPS)
    return (values * scale * gain).astype(BF16)


def split_two(value):
    high = value.astype(BF16)
    return high, (value - high.astype(F32)).astype(BF16)


def layer_kernel(
    nk,
    nt,
    resid,
    gains,
    gate,
    up,
    down,
    wx,
    wz,
    wbc,
    wdt,
    dt_bias,
    a_log,
    d_skip,
    cwx,
    cwbc,
    cx,
    cbc,
    state,
    wout,
    out,
    gate_v,
    up_v,
    down_v,
    wx_v,
    wz_v,
    wbc_v,
    wdt_v,
    state_v,
    wout_v,
    state_b,
    small_v,
    cwx_v,
    cwbc_v,
    cx_v,
    cbc_v,
    expand_v,
    repeat_v,
    xn_v,
    rows_s,
    gain_s,
    first_v,
    part_b,
    near_s,
    half_s,
    xz_b,
    bc_b,
    dt_b,
    xz_s,
    bc_s,
    dt_s,
    mix_s,
    proj_s,
    second_v,
    cut_b,
    cut_s,
    load_sem,
    rows_send,
    rows_recv,
    gain_send,
    gain_recv,
    near_send,
    near_recv,
    half_send,
    half_recv,
    xz_send,
    xz_recv,
    bc_send,
    bc_recv,
    dt_send,
    dt_recv,
    mix_send,
    mix_recv,
    proj_send,
    proj_recv,
    cut_send,
    cut_recv,
):
    me_k, me_t = lax.axis_index("kv"), lax.axis_index("tp")
    n = nk * nt
    me = me_k * nt + me_t
    rows, width = rows_s.shape[1], rows_s.shape[2]
    dim = n * width

    def target(index):
        return {"kv": lax.div(index, nt), "tp": lax.rem(index, nt)}

    def flipped(index, mask):
        bit = 1
        while bit < nk:
            if mask & bit:
                index = index + bit - 2 * bit * lax.rem(lax.div(index, bit), 2)
            bit *= 2
        return index

    def all_peers():
        order = [(x, d) for x in range(nk) for d in range(nt)][1:]
        return [flipped(me_k, x) * nt + lax.rem(me_t + d, nt) for x, d in order]

    def kv_peers():
        return [flipped(me_k, x) for x in range(1, nk)]

    loads = {}

    def load(name, src, dst):
        copy = pltpu.make_async_copy(src, dst, load_sem.at[len(loads)])
        copy.start()
        loads[name] = copy

    load("rows", resid, rows_s.at[me])
    load("gains", gains, gain_s.at[me])
    load("gate0", gate.at[0], gate_v.at[0])
    load("up0", up.at[0], up_v.at[0])
    load("down0", down.at[0], down_v.at[0])
    load("bias", dt_bias, small_v.at[0])
    load("alog", a_log, small_v.at[1])
    load("skip", d_skip, small_v.at[2])
    load("cwx", cwx, cwx_v)
    load("cwbc", cwbc, cwbc_v)
    load("cx", cx, cx_v)
    load("cbc", cbc, cbc_v)
    load("wx", wx, wx_v)
    load("wz", wz, wz_v)
    load("wbc", wbc, wbc_v)
    load("wdt", wdt, wdt_v)
    load("state", state, state_v)
    load("wout", wout, wout_v)
    load("gate1", gate.at[1], gate_v.at[1])
    load("up1", up.at[1], up_v.at[1])
    load("down1", down.at[1], down_v.at[1])

    barrier = pltpu.get_barrier_semaphore()
    for q in all_peers():
        pl.semaphore_signal(barrier, inc=1, device_id=target(q), device_id_type=MESH)
    pl.semaphore_wait(barrier, n - 1)

    def send(src, dst, ssem, rsem, index):
        copy = pltpu.make_async_remote_copy(
            src_ref=src,
            dst_ref=dst,
            send_sem=ssem,
            recv_sem=rsem,
            device_id=target(index),
            device_id_type=MESH,
        )
        copy.start()
        return copy

    def arrived(slots, ssem, rsem, index):
        pltpu.make_async_remote_copy(
            src_ref=slots.at[index],
            dst_ref=slots.at[index],
            send_sem=ssem.at[index],
            recv_sem=rsem.at[index],
            device_id=target(index),
            device_id_type=MESH,
        ).wait_recv()

    sent = []

    loads["rows"].wait()
    loads["gains"].wait()
    for q in all_peers()[::-1]:
        sent.append(send(rows_s.at[me], rows_s.at[me], rows_send.at[q], rows_recv.at[me], q))
    for q in all_peers()[::-1]:
        sent.append(send(gain_s.at[me], gain_s.at[me], gain_send.at[q], gain_recv.at[me], q))

    heads, half = cx_v.shape[2], cx_v.shape[1]
    flat = heads * half
    groups = cwbc_v.shape[1] // 2
    pairs = 2 * groups
    lane = lax.broadcasted_iota(jnp.int32, expand_v.shape, 1)
    head_of = lax.broadcasted_iota(jnp.int32, expand_v.shape, 0) * half
    expand_v[...] = jnp.where((lane >= head_of) & (lane < head_of + half), 1.0, 0.0).astype(BF16)
    lane = lax.broadcasted_iota(jnp.int32, repeat_v.shape, 1)
    src_of = lax.broadcasted_iota(jnp.int32, repeat_v.shape, 0) * pairs
    repeat_v[...] = jnp.where((lane >= src_of) & (lane < src_of + pairs), 1.0, 0.0).astype(BF16)

    units = gate_v.shape[1]

    def gated(blocks, which):
        squares = jnp.zeros((rows, 1), F32)
        g = jnp.zeros((rows, units), F32)
        u = jnp.zeros((rows, units), F32)
        for values, gain, at in blocks:
            squares = squares + jnp.sum(values * values, axis=1, keepdims=True)
            left = (values * gain).astype(BF16)
            g = g + nt_dot(left, gate_v[which, :, at])
            u = u + nt_dot(left, up_v[which, :, at])
        scale = lax.rsqrt(squares / dim + EPS)
        return (silu(g * scale) * (u * scale)).astype(BF16)

    def columns(index, count):
        return pl.ds(pl.multiple_of(index * count, 128), count)

    def arriving_rows():
        for q in [me] + all_peers():
            if q is not me:
                arrived(rows_s, rows_send, rows_recv, q)
                arrived(gain_s, gain_send, gain_recv, q)
            yield rows_s[q].astype(F32), gain_s[q, 0:1, :].astype(F32), columns(q, width)

    loads["gate0"].wait()
    loads["up0"].wait()
    hidden = gated(arriving_rows(), 0)
    loads["down0"].wait()
    wide = dim // nt
    for d in range(1, nt):
        t = lax.rem(me_t + d, nt)
        part_b[t] = nn_dot(hidden, down_v[0, :, columns(t, wide)]).astype(BF16)
        sent.append(
            send(part_b.at[t], near_s.at[me_t], near_send.at[t], near_recv.at[me_t], me_k * nt + t)
        )

    chip = nn_dot(hidden, down_v[0, :, columns(me_t, wide)])

    def gain_row(i):
        return jnp.concatenate(
            [gain_s[q, i : i + 1, :].astype(F32) for q in range(n)], axis=1
        )

    base = jnp.concatenate([rows_s[q].astype(F32) for q in range(n)], axis=1)

    def two_nt(first_w, second_w):
        one = jnp.zeros((rows, first_w.shape[0]), F32)
        two = jnp.zeros((rows, first_w.shape[0]), F32)
        for k in range(n):
            left = xn_v[:, k * width : (k + 1) * width]
            one = one + nt_dot(left, first_w[:, k * width : (k + 1) * width])
            two = two + nt_dot(left, second_w[:, k * width : (k + 1) * width])
        return one, two

    for d in range(1, nt):
        t = lax.rem(me_t + d, nt)
        pltpu.make_async_remote_copy(
            src_ref=near_s.at[t],
            dst_ref=near_s.at[t],
            send_sem=near_send.at[t],
            recv_sem=near_recv.at[t],
            device_id=target(me_k * nt + t),
            device_id_type=MESH,
        ).wait_recv()
    for d in range(1, nt):
        chip = chip + near_s[lax.rem(me_t + d, nt)].astype(F32)
    half_s[me] = chip.astype(BF16)
    for q in all_peers()[::-1]:
        sent.append(send(half_s.at[me], half_s.at[me], half_send.at[q], half_recv.at[me], q))
    for name in ("bias", "alog", "skip", "cwx", "cwbc", "cx", "cbc"):
        loads[name].wait()

    def expand(value):
        return nn_dot(value, expand_v[...])

    known = sum(cx_v[i].astype(F32) * cwx_v[i].astype(F32) for i in range(cx_v.shape[0]))
    high, low = split_two(known)
    lane = lax.broadcasted_iota(jnp.int32, (half, flat), 1)
    row = lax.broadcasted_iota(jnp.int32, (half, flat), 0)
    own = (lane & (half - 1)) == row
    hist_x = jnp.sum(jnp.where(own, expand(high) + expand(low), 0.0), axis=0, keepdims=True)
    tap_x = jnp.sum(jnp.where(own, expand(cwx_v[cx_v.shape[0]]), 0.0), axis=0, keepdims=True)
    skip_high, skip_low = split_two(small_v[2])
    skip_row = expand(skip_high) + expand(skip_low)
    hist_bc = sum(cbc_v[i].astype(F32) * cwbc_v[i].astype(F32) for i in range(cbc_v.shape[0]))
    tap_bc = cwbc_v[cbc_v.shape[0]].astype(F32)

    loads["state"].wait()
    state_b[...] = state_v[...].astype(BF16)
    for q in all_peers():
        arrived(half_s, half_send, half_recv, q)
    total = jnp.concatenate(
        [sum(half_s[k * nt + t].astype(F32) for k in range(nk)) for t in range(nt)], axis=1
    )
    first = (base + 0.5 * total).astype(BF16).astype(F32)
    xn_v[...] = norm_rows(first, gain_row(1))
    block = nt * width
    for k in range(nk):
        first_v[k] = first[:, k * block : (k + 1) * block]

    span = wdt_v.shape[1]
    loads["wbc"].wait()
    loads["wdt"].wait()
    tile = repeat_v.shape[0]
    spread = repeat_v.shape[1]
    lane = lax.broadcasted_iota(jnp.int32, (rows * pairs, spread), 1)
    row = lax.broadcasted_iota(jnp.int32, (rows * pairs, spread), 0)
    same = (lane & (pairs - 1)) == (row & (pairs - 1))
    slab = xn_v[:, pl.ds(pl.multiple_of(me_k * span, 128), span)]
    bc_part = jnp.zeros((rows * pairs, wbc_v.shape[1]), F32)
    for c in range(span // tile):
        piece = slab[:, c * tile : (c + 1) * tile].astype(F32)
        piece = jnp.concatenate(
            [jnp.broadcast_to(piece[r : r + 1], (pairs, tile)) for r in range(rows)], axis=0
        ).astype(BF16)
        wide_x = jnp.where(same, nn_dot(piece, repeat_v[...]), 0.0).astype(BF16)
        bc_part = bc_part + nn_dot(wide_x, wbc_v[c * spread : (c + 1) * spread, :])
    dt_part = nt_dot(slab, wdt_v[...])
    for r in range(rows):
        bc_b[r] = bc_part[r * pairs : (r + 1) * pairs].astype(BF16)
        dt_b[r] = dt_part[r : r + 1]
    bc_s[me_k] = bc_b[me_k]
    dt_s[me_k] = dt_b[me_k]
    for k in kv_peers()[::-1]:
        q = k * nt + me_t
        sent.append(send(bc_b.at[k], bc_s.at[me_k], bc_send.at[k], bc_recv.at[me_k], q))
        sent.append(send(dt_b.at[k], dt_s.at[me_k], dt_send.at[k], dt_recv.at[me_k], q))

    loads["wx"].wait()
    loads["wz"].wait()
    xs_part, z_part = two_nt(wx_v, wz_v)
    cols = xs_part.shape[1]
    for r in range(rows):
        xz_b[r, :, :cols] = xs_part[r : r + 1].astype(BF16)
        xz_b[r, :, cols:] = z_part[r : r + 1].astype(BF16)
    xz_s[me_k] = xz_b[me_k]
    for k in kv_peers()[::-1]:
        q = k * nt + me_t
        sent.append(send(xz_b.at[k], xz_s.at[me_k], xz_send.at[k], xz_recv.at[me_k], q))

    def arrived_kv(slots, ssem, rsem):
        for k in kv_peers():
            pltpu.make_async_remote_copy(
                src_ref=slots.at[k],
                dst_ref=slots.at[k],
                send_sem=ssem.at[k],
                recv_sem=rsem.at[k],
                device_id=target(k * nt + me_t),
                device_id_type=MESH,
            ).wait_recv()

    arrived_kv(dt_s, dt_send, dt_recv)
    raw = sum(dt_s[k] for k in range(nk)) + small_v[0]
    step = jnp.maximum(raw, 0.0) + jnp.log1p(jnp.exp(-jnp.abs(raw)))
    decay = jnp.exp(-step * jnp.exp(small_v[1]))
    step_high, step_low = split_two(step)
    decay_high, decay_low = split_two(decay)
    decay_row = expand(decay_high) + expand(decay_low)
    step_row = expand(step_high) + expand(step_low)
    arrived_kv(bc_s, bc_send, bc_recv)
    bc_new = sum(bc_s[k].astype(F32) for k in range(nk)).astype(BF16).astype(F32)
    bconv = silu(hist_bc + bc_new * tap_bc)
    bmat, cmat = bconv[:groups], bconv[groups:]
    weight = jnp.sum(bmat * cmat, axis=1, keepdims=True)
    per_group = nt_dot(cmat.astype(BF16), state_b[...])
    lane = lax.broadcasted_iota(jnp.int32, (groups, flat), 1)
    low_end = lax.broadcasted_iota(jnp.int32, (groups, flat), 0) * (flat // groups)
    mine = (lane >= low_end) & (lane < low_end + flat // groups)
    read = jnp.sum(jnp.where(mine, per_group, 0.0), axis=0, keepdims=True)
    cross = jnp.sum(jnp.where(mine, weight, 0.0), axis=0, keepdims=True)
    arrived_kv(xz_s, xz_send, xz_recv)
    xs_row = jnp.concatenate([xz_s[k, :, :cols].astype(F32) for k in range(nk)], axis=1)
    z_row = jnp.concatenate([xz_s[k, :, cols:].astype(F32) for k in range(nk)], axis=1)
    xconv = silu(hist_x + xs_row * tap_x)
    mixed = decay_row * read + (step_row * cross + skip_row) * xconv
    mix_s[me_k] = (mixed * silu(z_row)).astype(BF16)
    for k in kv_peers()[::-1]:
        q = k * nt + me_t
        sent.append(send(mix_s.at[me_k], mix_s.at[me_k], mix_send.at[k], mix_recv.at[me_k], q))
    loads["wout"].wait()
    arrived_kv(mix_s, mix_send, mix_recv)
    mixed = jnp.concatenate([mix_s[k].astype(F32) for k in range(nk)], axis=0).astype(BF16)
    proj_s[me] = nn_dot(mixed, wout_v[...]).astype(BF16)
    for q in all_peers()[::-1]:
        sent.append(send(proj_s.at[me], proj_s.at[me], proj_send.at[q], proj_recv.at[me], q))

    def arriving_blocks():
        for x in range(nk):
            k = flipped(me_k, x)
            for d in range(nt):
                if x or d:
                    q = k * nt + lax.rem(me_t + d, nt)
                    arrived(proj_s, proj_send, proj_recv, q)
            total = sum(proj_s[k * nt + t].astype(F32) for t in range(nt))
            second = (first_v[k] + total).astype(BF16).astype(F32)
            if x == 0:
                for t in range(nt):
                    second_v[t] = second[:, t * width : (t + 1) * width]
            gain = jnp.concatenate(
                [gain_s[k * nt + t, 2:3, :].astype(F32) for t in range(nt)], axis=1
            )
            yield second, gain, columns(k, block)

    loads["gate1"].wait()
    loads["up1"].wait()
    hidden = gated(arriving_blocks(), 1)
    loads["down1"].wait()
    for q in all_peers()[::-1]:
        cut_b[q] = nn_dot(hidden, down_v[1, :, columns(q, width)]).astype(BF16)
        sent.append(send(cut_b.at[q], cut_s.at[me], cut_send.at[q], cut_recv.at[me], q))
    total = nn_dot(hidden, down_v[1, :, columns(me, width)])
    for q in all_peers():
        arrived(cut_s, cut_send, cut_recv, q)
        total = total + cut_s[q].astype(F32)
    out[...] = (second_v[me_t] + 0.5 * total).astype(BF16)
    for copy in sent:
        copy.wait_send()


def fused_layer(
    nk,
    nt,
    resid,
    norm_gain,
    ffn_gate,
    ffn_up,
    ffn_down,
    w_x,
    w_z,
    w_bc,
    w_dt,
    dt_bias,
    a_log,
    d_skip,
    conv_wx,
    conv_wbc,
    conv_x,
    conv_bc,
    ssm_state,
    w_out,
):
    n = nk * nt
    rows, width = resid.shape
    dim = ffn_gate.shape[1]
    units = ffn_gate.shape[2]
    local = w_x.shape[1] * w_x.shape[2]
    heads, half = conv_x.shape[2], conv_x.shape[3]
    flat = heads * half
    span = w_bc.shape[0]
    lanes = w_bc.shape[3]
    pairs = w_bc.shape[1] * w_bc.shape[2]
    out_cols = w_out.shape[2]
    taps = conv_wx.shape[0]
    tile = 128
    args = (
        resid,
        norm_gain,
        jnp.swapaxes(ffn_gate, 1, 2),
        jnp.swapaxes(ffn_up, 1, 2),
        ffn_down,
        jnp.transpose(w_x, (1, 2, 0)).reshape(local, dim),
        jnp.transpose(w_z, (1, 2, 0)).reshape(local, dim),
        w_bc.reshape(span * pairs, lanes),
        w_dt.T,
        dt_bias.reshape(1, heads),
        a_log.reshape(1, heads),
        d_skip.reshape(1, heads),
        jnp.swapaxes(conv_wx, 1, 2),
        conv_wbc.reshape(taps, pairs, lanes),
        jnp.swapaxes(conv_x, 2, 3).reshape(taps - 1, half, heads),
        conv_bc.reshape(taps - 1, pairs, lanes),
        ssm_state.reshape(flat, lanes),
        w_out.reshape(flat, out_cols),
    )
    dma = pltpu.SemaphoreType.DMA
    vmem = pltpu.VMEM
    scratch = [
        vmem((2, units, dim), BF16),
        vmem((2, units, dim), BF16),
        vmem((2, units, dim), BF16),
        vmem((local, dim), BF16),
        vmem((local, dim), BF16),
        vmem((span * pairs, lanes), BF16),
        vmem((heads, span), BF16),
        vmem((flat, lanes), F32),
        vmem((flat, out_cols), BF16),
        vmem((flat, lanes), BF16),
        vmem((3, 1, heads), F32),
        vmem((taps, half, heads), BF16),
        vmem((taps, pairs, lanes), BF16),
        vmem((taps - 1, half, heads), BF16),
        vmem((taps - 1, pairs, lanes), BF16),
        vmem((heads, flat), BF16),
        vmem((tile, tile * pairs), BF16),
        vmem((rows, dim), BF16),
        vmem((n, rows, width), BF16),
        vmem((n, 3, width), BF16),
        vmem((nk, rows, dim // nk), F32),
        vmem((nt, rows, dim // nt), BF16),
        vmem((nt, rows, dim // nt), BF16),
        vmem((n, rows, dim // nt), BF16),
        vmem((nk, 1, 2 * local), BF16),
        vmem((nk, pairs, lanes), BF16),
        vmem((nk, 1, heads), F32),
        vmem((nk, 1, 2 * local), BF16),
        vmem((nk, pairs, lanes), BF16),
        vmem((nk, 1, heads), F32),
        vmem((nk, 1, flat), BF16),
        vmem((n, rows, out_cols), BF16),
        vmem((nt, rows, width), F32),
        vmem((n, rows, width), BF16),
        vmem((n, rows, width), BF16),
    ]
    sems = [dma((21,))]
    for count in (n, n, nt, n, nk, nk, nk, nk, n, n):
        sems += [dma((count,)), dma((count,))]

    def scoped(*refs):
        pl.run_scoped(functools.partial(layer_kernel, nk, nt, *refs), *sems)

    return pl.pallas_call(
        scoped,
        out_shape=pltpu.VMEM(resid.shape, resid.dtype),
        in_specs=[pl.BlockSpec(memory_space=pl.ANY)] * len(args),
        out_specs=pl.BlockSpec(memory_space=pltpu.VMEM),
        scratch_shapes=scratch,
        compiler_params=pltpu.CompilerParams(
            collective_id=0, has_side_effects=True, vmem_limit_bytes=60 * 1024 * 1024
        ),
    )(*args)


def fits(nk, nt, resid, w_x, w_bc, conv_x):
    rows, width = resid.shape
    half = conv_x.shape[3]
    pairs = w_bc.shape[1] * w_bc.shape[2]
    return (
        conv_x.shape[0] == 1
        and rows == nk
        and nt > 1
        and nk & (nk - 1) == 0
        and w_bc.shape[0] == nt * width
        and width % 128 == 0
        and w_bc.shape[0] % 128 == 0
        and (w_x.shape[1] * w_x.shape[2]) % 128 == 0
        and half & (half - 1) == 0
        and pairs & (pairs - 1) == 0
    )


def solution(mesh):
    placed = (
        P("dp", ("kv", "tp")),
        P(None, ("kv", "tp")),
        P(None, None, ("kv", "tp")),
        P(None, None, ("kv", "tp")),
        P(None, ("kv", "tp"), None),
        P(None, "kv", "tp"),
        P(None, "kv", "tp"),
        P("kv", None, None, None),
        P("kv", None),
        P(),
        P(),
        P(),
        P(None, None, "tp"),
        P(),
        P(("dp", "kv"), None, None, "tp"),
        P(("dp", "kv"), None, None, None, None),
        P(("dp", "kv"), None, "tp", None),
        P(None, "tp", "kv"),
    )
    nk, nt = mesh.shape["kv"], mesh.shape["tp"]

    def layer(*args):
        if fits(nk, nt, args[0], args[5], args[7], args[14]):
            return fused_layer(nk, nt, *args)
        return per_device(*args)

    return jax.shard_map(
        layer, mesh=mesh, in_specs=placed, out_specs=P("dp", ("kv", "tp")), check_vma=False
    )
```

```python
from types import SimpleNamespace

import jax
import jax.numpy as jnp
from jax import lax
from jax.experimental import pallas as pl
from jax.experimental.pallas import tpu as pltpu
from jax.sharding import PartitionSpec as P

D = 2048
F32 = jnp.float32
BF16 = jnp.bfloat16
MESH = pl.DeviceIdType.MESH

EPS = 1e-06


def normalize(rows, gain):
    values = rows.astype(jnp.float32)
    scale = lax.rsqrt(jnp.mean(values * values, axis=1, keepdims=True) + EPS)
    return (values * scale * gain.astype(jnp.float32).reshape(1, -1)).astype(jnp.bfloat16)


def feed_forward(normed, w_gate, w_up, w_down):
    gate = jnp.dot(normed, w_gate, preferred_element_type=jnp.float32)
    upper = jnp.dot(normed, w_up, preferred_element_type=jnp.float32)
    hidden = (jax.nn.silu(gate) * upper).astype(jnp.bfloat16)
    return jnp.dot(hidden, w_down, preferred_element_type=jnp.float32)


def add_half(base, sums):
    return (base.astype(jnp.float32) + 0.5 * sums).astype(jnp.bfloat16)


def ffn_totals(partial_value):
    return lax.psum(partial_value, ("kv", "tp"))


def short_conv(history, newest, taps):
    window = jnp.concatenate(
        [history.astype(jnp.float32), newest.astype(jnp.float32)[:, None]], axis=1
    )
    return jax.nn.silu(jnp.sum(window * taps.astype(jnp.float32)[None], axis=1))


def state_step(
    xs_new,
    zeta,
    bc_new,
    dt_raw,
    conv_x,
    conv_bc,
    ssm_state,
    conv_wx,
    conv_wbc,
    dt_bias,
    a_log,
    d_skip,
):
    xconv = short_conv(conv_x, xs_new, conv_wx)
    bconv = short_conv(conv_bc, bc_new, conv_wbc)
    heads = xconv.shape[1]
    groups = bconv.shape[2]
    bmat = jnp.repeat(bconv[:, 0], heads // groups, axis=1)
    cmat = jnp.repeat(bconv[:, 1], heads // groups, axis=1)
    step_size = jax.nn.softplus(dt_raw + dt_bias[None, :])
    decay = jnp.exp(-step_size * jnp.exp(a_log)[None, :])
    updated = (
        decay[:, :, None, None] * ssm_state
        + (step_size[:, :, None] * xconv)[..., None] * bmat[:, :, None, :]
    )
    mixed = (
        jnp.einsum("shpn,shn->shp", updated, cmat, precision=lax.Precision.HIGHEST)
        + d_skip[None, :, None] * xconv
    )
    return (mixed * jax.nn.silu(zeta.astype(jnp.float32))).astype(jnp.bfloat16)


def group_terms(slab, w_bc, w_dt):
    span = slab.shape[1]
    flat_bc = w_bc.reshape(span, -1)
    bc_part = jnp.dot(slab, flat_bc, preferred_element_type=jnp.float32)
    dt_part = jnp.dot(slab, w_dt, preferred_element_type=jnp.float32)
    return (
        lax.psum_scatter(bc_part, "kv", scatter_dimension=0, tiled=True),
        lax.psum_scatter(dt_part, "kv", scatter_dimension=0, tiled=True),
    )


def mix_partial(
    normed,
    w_x,
    w_z,
    w_bc,
    w_dt,
    dt_bias,
    a_log,
    d_skip,
    conv_wx,
    conv_wbc,
    conv_x,
    conv_bc,
    ssm_state,
    w_out,
):
    rows = normed.shape[0]
    local_heads = w_x.shape[1]
    half = w_x.shape[2]
    xs_part = (
        jnp.dot(normed, w_x.reshape(D, -1), preferred_element_type=jnp.float32)
        .astype(jnp.bfloat16)
        .reshape(rows, local_heads, half)
    )
    zeta_part = (
        jnp.dot(normed, w_z.reshape(D, -1), preferred_element_type=jnp.float32)
        .astype(jnp.bfloat16)
        .reshape(rows, local_heads, half)
    )
    xs_new, zeta = (
        lax.all_to_all(xs_part, "kv", split_axis=0, concat_axis=1, tiled=True),
        lax.all_to_all(zeta_part, "kv", split_axis=0, concat_axis=1, tiled=True),
    )
    span = w_bc.shape[0]
    slab = lax.dynamic_slice_in_dim(normed, lax.axis_index("kv") * span, span, 1)
    bc_sum, dt_raw = group_terms(slab, w_bc, w_dt)
    bc_new = bc_sum.astype(jnp.bfloat16).reshape((bc_sum.shape[0],) + w_bc.shape[1:])
    mixed = state_step(
        xs_new,
        zeta,
        bc_new,
        dt_raw,
        conv_x,
        conv_bc,
        ssm_state,
        conv_wx,
        conv_wbc,
        dt_bias,
        a_log,
        d_skip,
    )
    flat_out = w_out.reshape(-1, w_out.shape[2])
    piece = lax.all_gather(mixed, "kv", axis=0, tiled=True)
    return jnp.dot(piece.reshape(piece.shape[0], -1), flat_out, preferred_element_type=jnp.float32)


def per_device(
    resid,
    norm_gain,
    ffn_gate,
    ffn_up,
    ffn_down,
    w_x,
    w_z,
    w_bc,
    w_dt,
    dt_bias,
    a_log,
    d_skip,
    conv_wx,
    conv_wbc,
    conv_x,
    conv_bc,
    ssm_state,
    w_out,
):
    mixer_args = (
        w_x,
        w_z,
        w_bc,
        w_dt,
        dt_bias,
        a_log,
        d_skip,
        conv_wx,
        conv_wbc,
        conv_x,
        conv_bc,
        ssm_state,
        w_out,
    )
    rows, gains = (
        lax.all_gather(resid, ("kv", "tp"), axis=1, tiled=True),
        lax.all_gather(norm_gain, ("kv", "tp"), axis=1, tiled=True),
    )
    first = add_half(
        rows,
        ffn_totals(feed_forward(normalize(rows, gains[0]), ffn_gate[0], ffn_up[0], ffn_down[0])),
    )
    partial_value = mix_partial(normalize(first, gains[1]), *mixer_args)
    span = partial_value.shape[1]
    block = lax.dynamic_slice_in_dim(first, lax.axis_index("kv") * span, span, 1)
    joined = (block.astype(jnp.float32) + lax.psum(partial_value, "tp")).astype(jnp.bfloat16)
    second = lax.all_gather(joined, "kv", axis=1, tiled=True)
    final = add_half(
        second,
        ffn_totals(feed_forward(normalize(second, gains[2]), ffn_gate[1], ffn_up[1], ffn_down[1])),
    )
    width = resid.shape[1]
    return lax.dynamic_slice_in_dim(final, lax.axis_index(("kv", "tp")) * width, width, 1)


def nt_dot(left, right):
    return lax.dot_general(left, right, (((1,), (1,)), ((), ())), preferred_element_type=F32)


def nn_dot(left, right):
    return jnp.dot(left, right, preferred_element_type=F32)


def silu(value):
    return value * jax.nn.sigmoid(value)


def norm_rows(values, gain):
    scale = lax.rsqrt(jnp.mean(values * values, axis=1, keepdims=True) + EPS)
    return (values * scale * gain).astype(BF16)


def split_two(value):
    high = value.astype(BF16)
    return high, (value - high.astype(F32)).astype(BF16)


def layer_kernel(
    nk,
    nt,
    resid,
    gains,
    gate,
    up,
    down,
    wx,
    wz,
    wbc,
    wdt,
    dt_bias,
    a_log,
    d_skip,
    cwx,
    cwbc,
    cx,
    cbc,
    state,
    wout,
    out,
    v,
    m,
):
    me_k, me_t = lax.axis_index("kv"), lax.axis_index("tp")
    n = nk * nt
    me = me_k * nt + me_t
    lead = nt - 1
    rows, width = resid.shape
    dim = n * width
    block = nt * width
    scope = jax.named_scope

    def target(index):
        return {"kv": lax.div(index, nt), "tp": lax.rem(index, nt)}

    def flipped(index, mask):
        bit = 1
        while bit < nk:
            if mask & bit:
                index = index + bit - 2 * bit * lax.rem(lax.div(index, bit), 2)
            bit *= 2
        return index

    def all_peers():
        order = [(x, d) for x in range(nk) for d in range(nt)][1:]
        return [flipped(me_k, x) * nt + lax.rem(me_t + d, nt) for x, d in order]

    def kv_peers():
        return [flipped(me_k, x) for x in range(1, nk)]

    loads = {}

    def load(name, src, dst):
        copy = pltpu.make_async_copy(src, dst, m.load.at[len(loads)])
        copy.start()
        loads[name] = copy

    def loaded(*names):
        with scope("w_" + names[0]):
            for name in names:
                loads[name].wait()

    load("rows", resid, v.rows.at[me])
    load("gains", gains, v.gain.at[me])
    barrier = pltpu.get_barrier_semaphore()
    for q in all_peers()[::-1]:
        pl.semaphore_signal(barrier, inc=1, device_id=target(q), device_id_type=MESH)
    load("gate0", gate.at[0], v.gate.at[0])
    load("up0", up.at[0], v.up.at[0])
    load("down0", down.at[0], v.down.at[0])
    load("wbc", wbc, v.wbc)
    load("bias", dt_bias, v.small.at[0])
    load("alog", a_log, v.small.at[1])
    load("skip", d_skip, v.small.at[2])
    load("cwx", cwx, v.cwx)
    load("cwbc", cwbc, v.cwbc)
    load("cx", cx, v.cx)
    load("cbc", cbc, v.cbc)
    load("wdt", wdt, v.wdt)
    load("state", state, v.state)
    load("wx", wx, v.wx)
    load("wz", wz, v.wz)
    load("wout", wout, v.wout)
    load("gate1", gate.at[1], v.gate.at[1])
    load("up1", up.at[1], v.up.at[1])
    load("down1", down.at[1], v.down.at[1])
    with scope("w_barrier"):
        pl.semaphore_wait(barrier, n - 1)

    def remote(src, dst, ssem, rsem, index):
        return pltpu.make_async_remote_copy(
            src_ref=src,
            dst_ref=dst,
            send_sem=ssem,
            recv_sem=rsem,
            device_id=target(index),
            device_id_type=MESH,
        )

    sent = []

    def send(src, dst, ssem, rsem, index):
        copy = remote(src, dst, ssem, rsem, index)
        copy.start()
        sent.append(copy)

    def arrived(slots, sems, slot, index):
        remote(slots.at[slot], slots.at[slot], sems[0].at[slot], sems[1].at[slot], index).wait_recv()

    loaded("rows", "gains")
    for q in all_peers()[::-1]:
        send(v.rows.at[me], v.rows.at[me], m.rows[0].at[q], m.rows[1].at[me], q)
    for q in all_peers()[::-1]:
        send(v.gain.at[me], v.gain.at[me], m.gain[0].at[q], m.gain[1].at[me], q)

    heads, half = v.cx.shape[2], v.cx.shape[1]
    flat = heads * half
    groups = v.cwbc.shape[1] // 2
    pairs = 2 * groups
    lane = lax.broadcasted_iota(jnp.int32, v.expand.shape, 1)
    head_of = lax.broadcasted_iota(jnp.int32, v.expand.shape, 0) * half
    v.expand[...] = jnp.where((lane >= head_of) & (lane < head_of + half), 1.0, 0.0).astype(BF16)
    tile = v.perm.shape[0]
    deep = tile // pairs
    row = lax.broadcasted_iota(jnp.int32, v.perm.shape, 0)
    lane = lax.broadcasted_iota(jnp.int32, v.perm.shape, 1)
    source = (row & (deep - 1)) * pairs + lax.shift_right_logical(row, deep.bit_length() - 1)
    v.perm[...] = jnp.where(lane == source, 1.0, 0.0).astype(BF16)

    units = v.gate.shape[1]

    def gated(blocks, which):
        squares = jnp.zeros((rows, 1), F32)
        g = jnp.zeros((rows, units), F32)
        u = jnp.zeros((rows, units), F32)
        for values, gain, at in blocks:
            squares = squares + jnp.sum(values * values, axis=1, keepdims=True)
            left = (values * gain).astype(BF16)
            g = g + nt_dot(left, v.gate[which, :, at])
            u = u + nt_dot(left, v.up[which, :, at])
        scale = lax.rsqrt(squares / dim + EPS)
        return (silu(g * scale) * (u * scale)).astype(BF16)

    def columns(index, count):
        return pl.ds(pl.multiple_of(index * count, 128), count)

    def arriving_rows():
        for q in [me] + all_peers():
            if q is not me:
                with scope("w_rows"):
                    arrived(v.rows, m.rows, q, q)
                    arrived(v.gain, m.gain, q, q)
            yield v.rows[q].astype(F32), v.gain[q, 0:1, :].astype(F32), columns(q, width)

    loaded("gate0", "up0")
    hidden = gated(arriving_rows(), 0)
    loaded("down0")
    for x in range(nk)[::-1]:
        k = flipped(me_k, x)
        v.part[k] = nn_dot(hidden, v.down[0, :, columns(k, block)]).astype(BF16)
        for d in range(nt)[::-1]:
            t = (lead + nt - d) % nt if x else lax.rem(me_t + d, nt)
            if x or d:
                q = k * nt + t
                send(v.part.at[k], v.slab.at[me], m.slab[0].at[q], m.slab[1].at[me], q)
    v.slab[me] = v.part[me_k]
    for q in all_peers()[::-1]:
        send(v.part, v.full.at[me], m.full[0].at[q], m.full[1].at[me], q)

    def gain_cut(index, i):
        return jnp.concatenate(
            [v.gain[index * nt + t, i : i + 1, :].astype(F32) for t in range(nt)], axis=1
        )

    def rows_cut(index):
        return jnp.concatenate([v.rows[index * nt + t].astype(F32) for t in range(nt)], axis=1)

    def expand(value):
        return nn_dot(value, v.expand[...])

    loaded("wbc")
    span = v.wdt.shape[1]
    for c in range(span // deep):
        piece = nn_dot(v.perm[...], v.wbc[c * tile : (c + 1) * tile, :]).astype(BF16)
        for p in range(pairs):
            v.wide[c * deep : (c + 1) * deep, p * 128 : (p + 1) * 128] = piece[
                p * deep : (p + 1) * deep, :
            ]

    loaded("bias", "alog", "skip", "cwx", "cwbc", "cx", "cbc")
    taps = v.cx.shape[0]
    known = sum(v.cx[i].astype(F32) * v.cwx[i].astype(F32) for i in range(taps))
    high, low = split_two(known)
    lane = lax.broadcasted_iota(jnp.int32, (half, flat), 1)
    row = lax.broadcasted_iota(jnp.int32, (half, flat), 0)
    own = (lane & (half - 1)) == row
    v.hist[me_k] = jnp.sum(jnp.where(own, expand(high) + expand(low), 0.0), axis=0, keepdims=True)
    for k in kv_peers()[::-1]:
        q = k * nt + me_t
        send(v.hist.at[me_k], v.hist.at[me_k], m.hist[0].at[k], m.hist[1].at[me_k], q)
    tap_x = jnp.sum(jnp.where(own, expand(v.cwx[taps]), 0.0), axis=0, keepdims=True)
    skip_high, skip_low = split_two(v.small[2])
    v.line[0] = tap_x
    v.line[1] = expand(skip_high) + expand(skip_low)
    hist_bc = sum(v.cbc[i].astype(F32) * v.cwbc[i].astype(F32) for i in range(taps))
    tap_bc = v.cwbc[taps].astype(F32)
    loaded("state", "wdt")
    v.state_b[...] = v.state[...].astype(BF16)

    with scope("w_slab"):
        for q in all_peers():
            arrived(v.slab, m.slab, q, q)
    total = sum(v.slab[q].astype(F32) for q in range(n))
    near = (rows_cut(me_k) + 0.5 * total).astype(BF16).astype(F32)
    left = (near * gain_cut(me_k, 1)).astype(BF16)
    bc_part = nn_dot(left, v.wide[...])
    dt_part = nt_dot(left, v.wdt[...])
    tall = v.bc.shape[1]
    for p in range(pairs):
        v.bc_b[pl.ds(p, rows, stride=tall), :] = bc_part[:, p * 128 : (p + 1) * 128]
    v.bc_b[pl.ds(pairs, rows, stride=tall), :] = jnp.concatenate(
        [dt_part, jnp.zeros((rows, 128 - heads), F32)], axis=1
    )

    def bc_row(k):
        return v.bc_b.at[pl.ds(pl.multiple_of(k * tall, 8), tall), :]

    def bc_sends():
        for k in kv_peers()[::-1]:
            for t in range(nt):
                q = k * nt + t
                yield remote(bc_row(k), v.bc.at[me_k], m.bc[0].at[q], m.bc[1].at[me_k], q)

    @pl.when(me_t == lead)
    def _():
        for copy in bc_sends():
            copy.start()

    with scope("w_full"):
        for q in all_peers():
            arrived(v.full, m.full, q, q)
    squares = jnp.zeros((rows, 1), F32)
    v.full[me] = v.part[...]
    for k in range(nk):
        total = sum(v.full[q, k].astype(F32) for q in range(n))
        first = (rows_cut(k) + 0.5 * total).astype(BF16).astype(F32)
        v.first[k] = first
        v.xn[k] = (first * gain_cut(k, 1)).astype(BF16)
        squares = squares + jnp.sum(first * first, axis=1, keepdims=True)
    scale = lax.rsqrt(squares / dim + EPS)
    v.scale[...] = jnp.broadcast_to(scale, v.scale.shape)

    loaded("wx", "wz")
    local = v.wx.shape[0]
    xs_part = jnp.zeros((rows, local), F32)
    z_part = jnp.zeros((rows, local), F32)
    for k in range(nk):
        xs_part = xs_part + nt_dot(v.xn[k], v.wx[:, k * block : (k + 1) * block])
        z_part = z_part + nt_dot(v.xn[k], v.wz[:, k * block : (k + 1) * block])
    v.xz[me_k] = jnp.concatenate([xs_part * scale, z_part * scale], axis=1).astype(BF16)
    for k in kv_peers()[::-1]:
        q = k * nt + me_t
        send(v.xz.at[me_k], v.xz.at[me_k], m.xz[0].at[k], m.xz[1].at[me_k], q)

    with scope("w_bc"):
        for k in kv_peers():
            arrived(v.bc, m.bc, k, k * nt + lead)
    v.bc[me_k] = bc_row(me_k)[...]
    summed = sum(v.bc[k] for k in range(nk)) * v.scale[pl.ds(me_k, 1), :]
    raw = summed[pairs : pairs + 1, :heads] + v.small[0]
    step = jnp.maximum(raw, 0.0) + jnp.log1p(jnp.exp(-jnp.abs(raw)))
    decay = jnp.exp(-step * jnp.exp(v.small[1]))
    step_high, step_low = split_two(step)
    decay_high, decay_low = split_two(decay)
    spread = expand(jnp.concatenate([decay_high, decay_low, step_high, step_low], axis=0))
    decay_row = spread[0:1] + spread[1:2]
    step_row = spread[2:3] + spread[3:4]
    bc_new = summed[:pairs].astype(BF16).astype(F32)
    bconv = silu(hist_bc + bc_new * tap_bc)
    bmat, cmat = bconv[:groups], bconv[groups:]
    weight = jnp.sum(bmat * cmat, axis=1, keepdims=True)
    per_group = nt_dot(cmat.astype(BF16), v.state_b[...])
    lane = lax.broadcasted_iota(jnp.int32, (groups, flat), 1)
    low_end = lax.broadcasted_iota(jnp.int32, (groups, flat), 0) * (flat // groups)
    mine = (lane >= low_end) & (lane < low_end + flat // groups)
    read = jnp.sum(jnp.where(mine, per_group, 0.0), axis=0, keepdims=True)
    cross = jnp.sum(jnp.where(mine, weight, 0.0), axis=0, keepdims=True)
    v.mix[me_k] = jnp.concatenate(
        [decay_row * read, step_row * cross + v.line[1]], axis=0
    ).astype(BF16)
    for k in kv_peers()[::-1]:
        q = k * nt + me_t
        send(v.mix.at[me_k], v.mix.at[me_k], m.mix[0].at[k], m.mix[1].at[me_k], q)

    with scope("w_xz"):
        for k in kv_peers():
            arrived(v.hist, m.hist, k, k * nt + me_t)
            arrived(v.xz, m.xz, k, k * nt + me_t)
    for k in range(nk):
        at = slice(k * local, (k + 1) * local)
        past = jnp.concatenate([v.hist[i][:, at] for i in range(nk)], axis=0)
        v.xconv[:, at] = silu(past + v.xz[k][:, :local].astype(F32) * v.line[0][:, at])
        v.open[:, at] = silu(v.xz[k][:, local:].astype(F32))
    loaded("wout")
    with scope("w_mix"):
        for k in kv_peers():
            arrived(v.mix, m.mix, k, k * nt + me_t)
    pieces = [v.mix[k].astype(F32) for k in range(nk)]
    read = jnp.concatenate([piece[0:1] for piece in pieces], axis=0)
    direct = jnp.concatenate([piece[1:2] for piece in pieces], axis=0)
    mixed = ((read + direct * v.xconv[...]) * v.open[...]).astype(BF16)
    v.proj[me] = nn_dot(mixed, v.wout[...]).astype(BF16)
    for q in all_peers()[::-1]:
        send(v.proj.at[me], v.proj.at[me], m.proj[0].at[q], m.proj[1].at[me], q)

    def arriving_blocks():
        for x in range(nk):
            k = flipped(me_k, x)
            with scope("w_proj"):
                for d in range(nt):
                    if x or d:
                        q = k * nt + lax.rem(me_t + d, nt)
                        arrived(v.proj, m.proj, q, q)
            total = sum(v.proj[k * nt + t].astype(F32) for t in range(nt))
            second = (v.first[k] + total).astype(BF16).astype(F32)
            if x == 0:
                for t in range(nt):
                    v.second[t] = second[:, t * width : (t + 1) * width]
            yield second, gain_cut(k, 2), columns(k, block)

    loaded("gate1", "up1")
    hidden = gated(arriving_blocks(), 1)
    loaded("down1")
    for x in range(nk)[::-1]:
        k = flipped(me_k, x)
        piece = nn_dot(hidden, v.down[1, :, columns(k, block)])
        for t in range(nt):
            v.cut_b[k * nt + t] = piece[:, t * width : (t + 1) * width].astype(BF16)
        for d in range(nt)[::-1]:
            if x or d:
                q = k * nt + lax.rem(me_t + d, nt)
                send(v.cut_b.at[q], v.cut.at[me], m.cut[0].at[q], m.cut[1].at[me], q)
    v.cut[me] = v.cut_b[me]
    with scope("w_cut"):
        for q in all_peers():
            arrived(v.cut, m.cut, q, q)
    total = sum(v.cut[q].astype(F32) for q in range(n))
    out[...] = (v.second[me_t] + 0.5 * total).astype(BF16)
    with scope("w_sent"):
        for copy in sent:
            copy.wait_send()

        @pl.when(me_t == lead)
        def _():
            for copy in bc_sends():
                copy.wait_send()


def fused_layer(
    nk,
    nt,
    resid,
    norm_gain,
    ffn_gate,
    ffn_up,
    ffn_down,
    w_x,
    w_z,
    w_bc,
    w_dt,
    dt_bias,
    a_log,
    d_skip,
    conv_wx,
    conv_wbc,
    conv_x,
    conv_bc,
    ssm_state,
    w_out,
):
    n = nk * nt
    rows, width = resid.shape
    dim = ffn_gate.shape[1]
    units = ffn_gate.shape[2]
    local = w_x.shape[1] * w_x.shape[2]
    heads, half = conv_x.shape[2], conv_x.shape[3]
    flat = heads * half
    span = w_bc.shape[0]
    lanes = w_bc.shape[3]
    pairs = w_bc.shape[1] * w_bc.shape[2]
    out_cols = w_out.shape[2]
    taps = conv_wx.shape[0]
    block = nt * width
    args = (
        resid,
        norm_gain,
        jnp.swapaxes(ffn_gate, 1, 2),
        jnp.swapaxes(ffn_up, 1, 2),
        ffn_down,
        jnp.transpose(w_x, (1, 2, 0)).reshape(local, dim),
        jnp.transpose(w_z, (1, 2, 0)).reshape(local, dim),
        w_bc.reshape(span * pairs, lanes),
        w_dt.T,
        dt_bias.reshape(1, heads),
        a_log.reshape(1, heads),
        d_skip.reshape(1, heads),
        jnp.swapaxes(conv_wx, 1, 2),
        conv_wbc.reshape(taps, pairs, lanes),
        jnp.swapaxes(conv_x, 2, 3).reshape(taps - 1, half, heads),
        conv_bc.reshape(taps - 1, pairs, lanes),
        ssm_state.reshape(flat, lanes),
        w_out.reshape(flat, out_cols),
    )
    dma = pltpu.SemaphoreType.DMA
    vmem = pltpu.VMEM
    scratch = dict(
        gate=vmem((2, units, dim), BF16),
        up=vmem((2, units, dim), BF16),
        down=vmem((2, units, dim), BF16),
        wx=vmem((local, dim), BF16),
        wz=vmem((local, dim), BF16),
        wbc=vmem((span * pairs, lanes), BF16),
        wide=vmem((span, pairs * lanes), BF16),
        wdt=vmem((heads, span), BF16),
        state=vmem((flat, lanes), F32),
        state_b=vmem((flat, lanes), BF16),
        wout=vmem((flat, out_cols), BF16),
        small=vmem((3, 1, heads), F32),
        cwx=vmem((taps, half, heads), BF16),
        cwbc=vmem((taps, pairs, lanes), BF16),
        cx=vmem((taps - 1, half, heads), BF16),
        cbc=vmem((taps - 1, pairs, lanes), BF16),
        expand=vmem((heads, flat), BF16),
        perm=vmem((256, 256), BF16),
        rows=vmem((n, rows, width), BF16),
        gain=vmem((n, 3, width), BF16),
        part=vmem((nk, rows, block), BF16),
        slab=vmem((n, rows, block), BF16),
        full=vmem((n, nk, rows, block), BF16),
        first=vmem((nk, rows, block), F32),
        xn=vmem((nk, rows, block), BF16),
        scale=vmem((rows, lanes), F32),
        bc_b=vmem((nk * (pairs + 8), lanes), F32),
        bc=vmem((nk, pairs + 8, lanes), F32),
        hist=vmem((nk, 1, flat), F32),
        line=vmem((2, 1, flat), F32),
        xz=vmem((nk, rows, 2 * local), BF16),
        xconv=vmem((rows, flat), F32),
        open=vmem((rows, flat), F32),
        mix=vmem((nk, 2, flat), BF16),
        proj=vmem((n, rows, out_cols), BF16),
        second=vmem((nt, rows, width), F32),
        cut_b=vmem((n, rows, width), BF16),
        cut=vmem((n, rows, width), BF16),
    )
    rounds = dict(
        rows=n, gain=n, slab=n, full=n, bc=n, hist=nk, xz=nk, mix=nk, proj=n, cut=n
    )
    sems = {name: (dma((count,)), dma((count,))) for name, count in rounds.items()}
    sems["load"] = dma((21,))

    def kernel(*refs, **held):
        def body(**flags):
            layer_kernel(nk, nt, *refs, SimpleNamespace(**held), SimpleNamespace(**flags))

        pl.run_scoped(body, **sems)

    return pl.pallas_call(
        kernel,
        out_shape=pltpu.VMEM(resid.shape, resid.dtype),
        in_specs=[pl.BlockSpec(memory_space=pl.ANY)] * len(args),
        out_specs=pl.BlockSpec(memory_space=pltpu.VMEM),
        scratch_shapes=scratch,
        compiler_params=pltpu.CompilerParams(
            collective_id=0, has_side_effects=True, vmem_limit_bytes=60 * 1024 * 1024
        ),
    )(*args)


def fits(nk, nt, resid, w_x, w_bc, conv_x):
    rows, width = resid.shape
    half = conv_x.shape[3]
    pairs = w_bc.shape[1] * w_bc.shape[2]
    return (
        conv_x.shape[0] == 1
        and rows == nk
        and nt > 1
        and nk & (nk - 1) == 0
        and w_bc.shape[0] == nt * width
        and width % 128 == 0
        and w_bc.shape[0] % 128 == 0
        and (w_x.shape[1] * w_x.shape[2]) % 128 == 0
        and half & (half - 1) == 0
        and pairs & (pairs - 1) == 0
        and pairs % 8 == 0
        and 256 % pairs == 0
        and (w_bc.shape[0] * pairs) % 256 == 0
        and w_bc.shape[3] == 128
        and conv_x.shape[2] < 128
    )


def solution(mesh):
    placed = (
        P("dp", ("kv", "tp")),
        P(None, ("kv", "tp")),
        P(None, None, ("kv", "tp")),
        P(None, None, ("kv", "tp")),
        P(None, ("kv", "tp"), None),
        P(None, "kv", "tp"),
        P(None, "kv", "tp"),
        P("kv", None, None, None),
        P("kv", None),
        P(),
        P(),
        P(),
        P(None, None, "tp"),
        P(),
        P(("dp", "kv"), None, None, "tp"),
        P(("dp", "kv"), None, None, None, None),
        P(("dp", "kv"), None, "tp", None),
        P(None, "tp", "kv"),
    )
    nk, nt = mesh.shape["kv"], mesh.shape["tp"]

    def layer(*args):
        if fits(nk, nt, args[0], args[5], args[7], args[14]):
            return fused_layer(nk, nt, *args)
        return per_device(*args)

    return jax.shard_map(
        layer, mesh=mesh, in_specs=placed, out_specs=P("dp", ("kv", "tp")), check_vma=False
    )
```

```python
from types import SimpleNamespace

import jax
import jax.numpy as jnp
from jax import lax
from jax.experimental import pallas as pl
from jax.experimental.pallas import tpu as pltpu
from jax.sharding import PartitionSpec as P

D = 2048
F32 = jnp.float32
BF16 = jnp.bfloat16
MESH = pl.DeviceIdType.MESH

EPS = 1e-06


def normalize(rows, gain):
    values = rows.astype(jnp.float32)
    scale = lax.rsqrt(jnp.mean(values * values, axis=1, keepdims=True) + EPS)
    return (values * scale * gain.astype(jnp.float32).reshape(1, -1)).astype(jnp.bfloat16)


def feed_forward(normed, w_gate, w_up, w_down):
    gate = jnp.dot(normed, w_gate, preferred_element_type=jnp.float32)
    upper = jnp.dot(normed, w_up, preferred_element_type=jnp.float32)
    hidden = (jax.nn.silu(gate) * upper).astype(jnp.bfloat16)
    return jnp.dot(hidden, w_down, preferred_element_type=jnp.float32)


def add_half(base, sums):
    return (base.astype(jnp.float32) + 0.5 * sums).astype(jnp.bfloat16)


def ffn_totals(partial_value):
    return lax.psum(partial_value, ("kv", "tp"))


def short_conv(history, newest, taps):
    window = jnp.concatenate(
        [history.astype(jnp.float32), newest.astype(jnp.float32)[:, None]], axis=1
    )
    return jax.nn.silu(jnp.sum(window * taps.astype(jnp.float32)[None], axis=1))


def state_step(
    xs_new,
    zeta,
    bc_new,
    dt_raw,
    conv_x,
    conv_bc,
    ssm_state,
    conv_wx,
    conv_wbc,
    dt_bias,
    a_log,
    d_skip,
):
    xconv = short_conv(conv_x, xs_new, conv_wx)
    bconv = short_conv(conv_bc, bc_new, conv_wbc)
    heads = xconv.shape[1]
    groups = bconv.shape[2]
    bmat = jnp.repeat(bconv[:, 0], heads // groups, axis=1)
    cmat = jnp.repeat(bconv[:, 1], heads // groups, axis=1)
    step_size = jax.nn.softplus(dt_raw + dt_bias[None, :])
    decay = jnp.exp(-step_size * jnp.exp(a_log)[None, :])
    updated = (
        decay[:, :, None, None] * ssm_state
        + (step_size[:, :, None] * xconv)[..., None] * bmat[:, :, None, :]
    )
    mixed = (
        jnp.einsum("shpn,shn->shp", updated, cmat, precision=lax.Precision.HIGHEST)
        + d_skip[None, :, None] * xconv
    )
    return (mixed * jax.nn.silu(zeta.astype(jnp.float32))).astype(jnp.bfloat16)


def group_terms(slab, w_bc, w_dt):
    span = slab.shape[1]
    flat_bc = w_bc.reshape(span, -1)
    bc_part = jnp.dot(slab, flat_bc, preferred_element_type=jnp.float32)
    dt_part = jnp.dot(slab, w_dt, preferred_element_type=jnp.float32)
    return (
        lax.psum_scatter(bc_part, "kv", scatter_dimension=0, tiled=True),
        lax.psum_scatter(dt_part, "kv", scatter_dimension=0, tiled=True),
    )


def mix_partial(
    normed,
    w_x,
    w_z,
    w_bc,
    w_dt,
    dt_bias,
    a_log,
    d_skip,
    conv_wx,
    conv_wbc,
    conv_x,
    conv_bc,
    ssm_state,
    w_out,
):
    rows = normed.shape[0]
    local_heads = w_x.shape[1]
    half = w_x.shape[2]
    xs_part = (
        jnp.dot(normed, w_x.reshape(D, -1), preferred_element_type=jnp.float32)
        .astype(jnp.bfloat16)
        .reshape(rows, local_heads, half)
    )
    zeta_part = (
        jnp.dot(normed, w_z.reshape(D, -1), preferred_element_type=jnp.float32)
        .astype(jnp.bfloat16)
        .reshape(rows, local_heads, half)
    )
    xs_new, zeta = (
        lax.all_to_all(xs_part, "kv", split_axis=0, concat_axis=1, tiled=True),
        lax.all_to_all(zeta_part, "kv", split_axis=0, concat_axis=1, tiled=True),
    )
    span = w_bc.shape[0]
    slab = lax.dynamic_slice_in_dim(normed, lax.axis_index("kv") * span, span, 1)
    bc_sum, dt_raw = group_terms(slab, w_bc, w_dt)
    bc_new = bc_sum.astype(jnp.bfloat16).reshape((bc_sum.shape[0],) + w_bc.shape[1:])
    mixed = state_step(
        xs_new,
        zeta,
        bc_new,
        dt_raw,
        conv_x,
        conv_bc,
        ssm_state,
        conv_wx,
        conv_wbc,
        dt_bias,
        a_log,
        d_skip,
    )
    flat_out = w_out.reshape(-1, w_out.shape[2])
    piece = lax.all_gather(mixed, "kv", axis=0, tiled=True)
    return jnp.dot(piece.reshape(piece.shape[0], -1), flat_out, preferred_element_type=jnp.float32)


def per_device(
    resid,
    norm_gain,
    ffn_gate,
    ffn_up,
    ffn_down,
    w_x,
    w_z,
    w_bc,
    w_dt,
    dt_bias,
    a_log,
    d_skip,
    conv_wx,
    conv_wbc,
    conv_x,
    conv_bc,
    ssm_state,
    w_out,
):
    mixer_args = (
        w_x,
        w_z,
        w_bc,
        w_dt,
        dt_bias,
        a_log,
        d_skip,
        conv_wx,
        conv_wbc,
        conv_x,
        conv_bc,
        ssm_state,
        w_out,
    )
    rows, gains = (
        lax.all_gather(resid, ("kv", "tp"), axis=1, tiled=True),
        lax.all_gather(norm_gain, ("kv", "tp"), axis=1, tiled=True),
    )
    first = add_half(
        rows,
        ffn_totals(feed_forward(normalize(rows, gains[0]), ffn_gate[0], ffn_up[0], ffn_down[0])),
    )
    partial_value = mix_partial(normalize(first, gains[1]), *mixer_args)
    span = partial_value.shape[1]
    block = lax.dynamic_slice_in_dim(first, lax.axis_index("kv") * span, span, 1)
    joined = (block.astype(jnp.float32) + lax.psum(partial_value, "tp")).astype(jnp.bfloat16)
    second = lax.all_gather(joined, "kv", axis=1, tiled=True)
    final = add_half(
        second,
        ffn_totals(feed_forward(normalize(second, gains[2]), ffn_gate[1], ffn_up[1], ffn_down[1])),
    )
    width = resid.shape[1]
    return lax.dynamic_slice_in_dim(final, lax.axis_index(("kv", "tp")) * width, width, 1)


def nt_dot(left, right):
    return lax.dot_general(left, right, (((1,), (1,)), ((), ())), preferred_element_type=F32)


def nn_dot(left, right):
    return jnp.dot(left, right, preferred_element_type=F32)


def silu(value):
    return value * jax.nn.sigmoid(value)


def norm_rows(values, gain):
    scale = lax.rsqrt(jnp.mean(values * values, axis=1, keepdims=True) + EPS)
    return (values * scale * gain).astype(BF16)


def split_two(value):
    high = value.astype(BF16)
    return high, (value - high.astype(F32)).astype(BF16)


def layer_kernel(
    nk,
    nt,
    resid,
    gains,
    gate,
    up,
    down,
    wx,
    wz,
    wbc,
    wdt,
    dt_bias,
    a_log,
    d_skip,
    cwx,
    cwbc,
    cx,
    cbc,
    state,
    wout,
    out,
    v,
    m,
):
    me_k, me_t = lax.axis_index("kv"), lax.axis_index("tp")
    n = nk * nt
    me = me_k * nt + me_t
    lead = nt - 1
    rows, width = resid.shape
    dim = n * width
    block = nt * width
    scope = jax.named_scope

    def target(index):
        return {"kv": lax.div(index, nt), "tp": lax.rem(index, nt)}

    def flipped(index, mask):
        bit = 1
        while bit < nk:
            if mask & bit:
                index = index + bit - 2 * bit * lax.rem(lax.div(index, bit), 2)
            bit *= 2
        return index

    def all_peers():
        order = [(x, d) for x in range(nk) for d in range(nt)][1:]
        return [flipped(me_k, x) * nt + lax.rem(me_t + d, nt) for x, d in order]

    def kv_peers():
        return [flipped(me_k, x) for x in range(1, nk)]

    loads = {}

    def load(name, src, dst):
        copy = pltpu.make_async_copy(src, dst, m.load.at[len(loads)])
        copy.start()
        loads[name] = copy

    def loaded(*names):
        with scope("w_" + names[0]):
            for name in names:
                loads[name].wait()

    load("rows", resid, v.rows.at[me])
    load("gains", gains, v.gain.at[me])
    barrier = pltpu.get_barrier_semaphore()
    for q in all_peers()[::-1]:
        pl.semaphore_signal(barrier, inc=1, device_id=target(q), device_id_type=MESH)
    load("bias", dt_bias, v.small.at[0])
    load("alog", a_log, v.small.at[1])
    load("skip", d_skip, v.small.at[2])
    load("cwx", cwx, v.cwx)
    load("cwbc", cwbc, v.cwbc)
    load("cx", cx, v.cx)
    load("cbc", cbc, v.cbc)
    load("gate0", gate.at[0], v.gate.at[0])
    load("up0", up.at[0], v.up.at[0])
    load("down0", down.at[0], v.down.at[0])
    lead_loads = (
        (wbc, v.wbc),
        (wdt, v.wdt),
        (state, v.state.at[lead]),
        (wout, v.wout.at[lead]),
    )

    def lead_load(i):
        return pltpu.make_async_copy(*lead_loads[i], m.lead.at[i])

    @pl.when(me_t == lead)
    def _():
        for i in range(3):
            lead_load(i).start()

    load("wx", wx, v.wx)
    load("wz", wz, v.wz)

    @pl.when(me_t == lead)
    def _():
        lead_load(3).start()

    load("gate1", gate.at[1], v.gate.at[1])
    load("up1", up.at[1], v.up.at[1])
    load("down1", down.at[1], v.down.at[1])
    with scope("w_barrier"):
        pl.semaphore_wait(barrier, n - 1)

    def remote(src, dst, ssem, rsem, index):
        return pltpu.make_async_remote_copy(
            src_ref=src,
            dst_ref=dst,
            send_sem=ssem,
            recv_sem=rsem,
            device_id=target(index),
            device_id_type=MESH,
        )

    sent = []

    def send(src, dst, ssem, rsem, index):
        copy = remote(src, dst, ssem, rsem, index)
        copy.start()
        sent.append(copy)

    def arrived(slots, sems, slot, index):
        remote(slots.at[slot], slots.at[slot], sems[0].at[slot], sems[1].at[slot], index).wait_recv()

    loaded("rows", "gains")
    for q in all_peers()[::-1]:
        send(v.rows.at[me], v.rows.at[me], m.rows[0].at[q], m.rows[1].at[me], q)
    for q in all_peers()[::-1]:
        send(v.gain.at[me], v.gain.at[me], m.gain[0].at[q], m.gain[1].at[me], q)

    home = me_k * nt + lead

    def pushes():
        yield remote(state, v.state.at[me_t], m.state[0].at[me_t], m.state[1].at[me_t], home)
        yield remote(wout, v.wout.at[me_t], m.wout[0].at[me_t], m.wout[1].at[me_t], home)

    @pl.when(me_t != lead)
    def _():
        for copy in pushes():
            copy.start()

    heads, half = v.cx.shape[2], v.cx.shape[1]
    flat = heads * half
    groups = v.cwbc.shape[1] // 2
    pairs = 2 * groups
    lane = lax.broadcasted_iota(jnp.int32, v.expand.shape, 1)
    head_of = lax.broadcasted_iota(jnp.int32, v.expand.shape, 0) * half
    v.expand[...] = jnp.where((lane >= head_of) & (lane < head_of + half), 1.0, 0.0).astype(BF16)
    tile = v.perm.shape[0]
    deep = tile // pairs
    row = lax.broadcasted_iota(jnp.int32, v.perm.shape, 0)
    lane = lax.broadcasted_iota(jnp.int32, v.perm.shape, 1)
    source = (row & (deep - 1)) * pairs + lax.shift_right_logical(row, deep.bit_length() - 1)
    v.perm[...] = jnp.where(lane == source, 1.0, 0.0).astype(BF16)

    def expand(value):
        return nn_dot(value, v.expand[...])

    loaded("bias", "alog", "skip", "cwx", "cwbc", "cx", "cbc")
    taps = v.cx.shape[0]
    known = sum(v.cx[i].astype(F32) * v.cwx[i].astype(F32) for i in range(taps))
    high, low = split_two(known)
    lane = lax.broadcasted_iota(jnp.int32, (half, flat), 1)
    row = lax.broadcasted_iota(jnp.int32, (half, flat), 0)
    own = (lane & (half - 1)) == row
    v.hist[me_k, me_t] = jnp.sum(
        jnp.where(own, expand(high) + expand(low), 0.0), axis=0, keepdims=True
    )
    v.tap[me_t] = jnp.sum(jnp.where(own, expand(v.cwx[taps]), 0.0), axis=0, keepdims=True)
    skip_high, skip_low = split_two(v.small[2])
    v.line[...] = expand(skip_high) + expand(skip_low)

    def to_leads(ref, sems):
        for k in kv_peers()[::-1]:
            q = k * nt + lead
            yield remote(ref.at[me_k, me_t], ref.at[me_k, me_t], sems[0].at[k], sems[1].at[me], q)

    def to_home(ref, sems):
        return remote(
            ref.at[me_k, me_t], ref.at[me_k, me_t], sems[0].at[me_k], sems[1].at[me], home
        )

    def tap_home():
        return remote(v.tap.at[me_t], v.tap.at[me_t], m.tap[0].at[me_t], m.tap[1].at[me_t], home)

    for copy in to_leads(v.hist, m.hist):
        copy.start()
        sent.append(copy)

    @pl.when(me_t != lead)
    def _():
        to_home(v.hist, m.hist).start()
        tap_home().start()

    hist_bc = sum(v.cbc[i].astype(F32) * v.cwbc[i].astype(F32) for i in range(taps))
    tap_bc = v.cwbc[taps].astype(F32)

    units = v.gate.shape[1]

    def gated(blocks, which, kept):
        squares = jnp.zeros((rows, 1), F32)
        g = jnp.zeros((rows, units), F32)
        u = jnp.zeros((rows, units), F32)
        for step, (values, gain, at) in enumerate(blocks):
            squares = squares + jnp.sum(values * values, axis=1, keepdims=True)
            left = (values * gain).astype(BF16)
            g = g + nt_dot(left, v.gate[which, :, at])
            u = u + nt_dot(left, v.up[which, :, at])
            if step < kept:
                v.held[step, 0] = g
                v.held[step, 1] = u
                g = jnp.zeros((rows, units), F32)
                u = jnp.zeros((rows, units), F32)
        for step in range(kept):
            g = g + v.held[step, 0]
            u = u + v.held[step, 1]
        scale = lax.rsqrt(squares / dim + EPS)
        return (silu(g * scale) * (u * scale)).astype(BF16)

    def columns(index, count):
        return pl.ds(pl.multiple_of(index * count, 128), count)

    def arriving_rows():
        for q in [me] + all_peers():
            if q is not me:
                with scope("w_rows"):
                    arrived(v.rows, m.rows, q, q)
                    arrived(v.gain, m.gain, q, q)
            yield v.rows[q].astype(F32), v.gain[q, 0:1, :].astype(F32), columns(q, width)

    loaded("gate0", "up0")
    hidden = gated(arriving_rows(), 0, 0)
    loaded("down0")
    for x in range(nk)[::-1]:
        k = flipped(me_k, x)
        v.part[k] = nn_dot(hidden, v.down[0, :, columns(k, block)]).astype(BF16)
        q = k * nt + lead
        if x:
            send(v.part.at[k], v.slab.at[me], m.slab[0].at[q], m.slab[1].at[me], q)

    def slab_home():
        q = me_k * nt + lead
        return remote(v.part.at[me_k], v.slab.at[me], m.slab[0].at[q], m.slab[1].at[me], q)

    @pl.when(me_t != lead)
    def _():
        slab_home().start()

    def gain_cut(index, i):
        return jnp.concatenate(
            [v.gain[index * nt + t, i : i + 1, :].astype(F32) for t in range(nt)], axis=1
        )

    def rows_cut(index):
        return jnp.concatenate([v.rows[index * nt + t].astype(F32) for t in range(nt)], axis=1)

    tall = v.bc.shape[1]

    def bc_row(k):
        return v.bc_b.at[pl.ds(pl.multiple_of(k * tall, 8), tall), :]

    def first_sends():
        for q in all_peers()[::-1]:
            yield remote(v.near.at[me_k], v.near.at[me_k], m.near[0].at[q], m.near[1].at[me_k], q)

    def bc_sends():
        for k in kv_peers()[::-1]:
            q = k * nt + lead
            yield remote(bc_row(k), v.bc.at[me_k], m.bc[0].at[k], m.bc[1].at[me_k], q)

    @pl.when(me_t == lead)
    def _():
        with scope("w_wbc"):
            lead_load(0).wait()
            lead_load(1).wait()
        span = v.wdt.shape[1]
        for c in range(span // deep):
            piece = nn_dot(v.perm[...], v.wbc[c * tile : (c + 1) * tile, :]).astype(BF16)
            for p in range(pairs):
                v.wide[c * deep : (c + 1) * deep, p * 128 : (p + 1) * 128] = piece[
                    p * deep : (p + 1) * deep, :
                ]
        v.slab[me] = v.part[me_k]
        with scope("w_slab"):
            for q in all_peers():
                arrived(v.slab, m.slab, q, q)
        total = sum(v.slab[q].astype(F32) for q in range(n))
        first = (rows_cut(me_k) + 0.5 * total).astype(BF16)
        v.near[me_k] = first
        for copy in first_sends():
            copy.start()
        left = (first.astype(F32) * gain_cut(me_k, 1)).astype(BF16)
        bc_part = nn_dot(left, v.wide[...])
        dt_part = nt_dot(left, v.wdt[...])
        for p in range(pairs):
            v.bc_b[pl.ds(p, rows, stride=tall), :] = bc_part[:, p * 128 : (p + 1) * 128]
        v.bc_b[pl.ds(pairs, rows, stride=tall), :] = jnp.concatenate(
            [dt_part, jnp.zeros((rows, 128 - heads), F32)], axis=1
        )
        for copy in bc_sends():
            copy.start()
        v.bc[me_k] = bc_row(me_k)[...]

    def arrived_at(slots, sems, k, t):
        q = k * nt + t
        remote(slots.at[k, t], slots.at[k, t], sems[0].at[k], sems[1].at[q], q).wait_recv()

    def arrived_from_lead(slots, sems, k):
        @pl.when(k * nt + lead != me)
        def _():
            arrived(slots, sems, k, k * nt + lead)

    loaded("wx", "wz")
    local = v.wx.shape[0]
    xs_part = jnp.zeros((rows, local), F32)
    z_part = jnp.zeros((rows, local), F32)
    squares = jnp.zeros((rows, 1), F32)
    for x in range(nk):
        k = flipped(me_k, x)
        with scope("w_near"):
            if x:
                arrived(v.near, m.near, k, k * nt + lead)
            else:
                arrived_from_lead(v.near, m.near, k)
        first = v.near[k].astype(F32)
        v.first[k] = first
        left = (first * gain_cut(k, 1)).astype(BF16)
        squares = squares + jnp.sum(first * first, axis=1, keepdims=True)
        xs_part = xs_part + nt_dot(left, v.wx[:, columns(k, block)])
        z_part = z_part + nt_dot(left, v.wz[:, columns(k, block)])
    scale = lax.rsqrt(squares / dim + EPS)
    v.scale[...] = jnp.broadcast_to(scale, v.scale.shape)
    v.xz[me_k, me_t] = jnp.concatenate([xs_part * scale, z_part * scale], axis=1).astype(BF16)
    for copy in to_leads(v.xz, m.xz):
        copy.start()
        sent.append(copy)

    @pl.when(me_t != lead)
    def _():
        to_home(v.xz, m.xz).start()

    def proj_sends():
        for q in all_peers()[::-1]:
            yield remote(v.proj.at[me_k], v.proj.at[me_k], m.proj[0].at[q], m.proj[1].at[me_k], q)

    @pl.when(me_t == lead)
    def _():
        with scope("w_state"):
            lead_load(2).wait()
            for t in range(lead):
                arrived(v.state, m.state, t, me_k * nt + t)
        for t in range(nt):
            v.state_b[t] = v.state[t].astype(BF16)
        with scope("w_bc"):
            for k in kv_peers():
                arrived(v.bc, m.bc, k, k * nt + lead)
        summed = sum(v.bc[k] for k in range(nk)) * v.scale[pl.ds(me_k, 1), :]
        raw = summed[pairs : pairs + 1, :heads] + v.small[0]
        step = jnp.maximum(raw, 0.0) + jnp.log1p(jnp.exp(-jnp.abs(raw)))
        decay = jnp.exp(-step * jnp.exp(v.small[1]))
        step_high, step_low = split_two(step)
        decay_high, decay_low = split_two(decay)
        spread = expand(jnp.concatenate([decay_high, decay_low, step_high, step_low], axis=0))
        decay_row = spread[0:1] + spread[1:2]
        step_row = spread[2:3] + spread[3:4]
        bc_new = summed[:pairs].astype(BF16).astype(F32)
        bconv = silu(hist_bc + bc_new * tap_bc)
        bmat, cmat = bconv[:groups], bconv[groups:]
        weight = jnp.sum(bmat * cmat, axis=1, keepdims=True)
        lane = lax.broadcasted_iota(jnp.int32, (groups, flat), 1)
        low_end = lax.broadcasted_iota(jnp.int32, (groups, flat), 0) * (flat // groups)
        mine = (lane >= low_end) & (lane < low_end + flat // groups)
        lines = []
        for t in range(nt):
            per_group = nt_dot(cmat.astype(BF16), v.state_b[t])
            read = jnp.sum(jnp.where(mine, per_group, 0.0), axis=0, keepdims=True)
            lines.append(decay_row * read)
        cross = jnp.sum(jnp.where(mine, weight, 0.0), axis=0, keepdims=True)
        lines.append(step_row * cross + v.line[...])
        v.mix[me_k] = jnp.concatenate(lines, axis=0).astype(BF16)

        def mix_sends():
            for k in kv_peers()[::-1]:
                q = k * nt + lead
                yield remote(v.mix.at[me_k], v.mix.at[me_k], m.mix[0].at[k], m.mix[1].at[me_k], q)

        for copy in mix_sends():
            copy.start()
        with scope("w_hist"):
            for t in range(lead):
                arrived(v.tap, m.tap, t, me_k * nt + t)
                arrived_at(v.hist, m.hist, me_k, t)
            for k in kv_peers():
                for t in range(nt):
                    arrived_at(v.hist, m.hist, k, t)
        with scope("w_wout"):
            lead_load(3).wait()
            for t in range(lead):
                arrived(v.wout, m.wout, t, me_k * nt + t)
        with scope("w_xz"):
            for t in range(lead):
                arrived_at(v.xz, m.xz, me_k, t)
            for k in kv_peers():
                for t in range(nt):
                    arrived_at(v.xz, m.xz, k, t)
        for t in range(nt):
            for k in range(nk):
                at = slice(k * local, (k + 1) * local)
                past = jnp.concatenate([v.hist[i, t][:, at] for i in range(nk)], axis=0)
                xs_new = v.xz[k, t][:, :local].astype(F32)
                v.xconv[t, :, at] = silu(past + xs_new * v.tap[t][:, at])
                v.open[t, :, at] = silu(v.xz[k, t][:, local:].astype(F32))
        with scope("w_mix"):
            for k in kv_peers():
                arrived(v.mix, m.mix, k, k * nt + lead)
        pieces = [v.mix[k].astype(F32) for k in range(nk)]
        direct = jnp.concatenate([piece[nt : nt + 1] for piece in pieces], axis=0)
        total = jnp.zeros((rows, v.wout.shape[2]), F32)
        for t in range(nt):
            read = jnp.concatenate([piece[t : t + 1] for piece in pieces], axis=0)
            mixed = ((read + direct * v.xconv[t]) * v.open[t]).astype(BF16)
            total = total + nn_dot(mixed, v.wout[t])
        v.proj[me_k] = total.astype(BF16)
        for copy in proj_sends():
            copy.start()
        for copy in mix_sends():
            copy.wait_send()

    def arriving_blocks():
        for x in range(nk):
            k = flipped(me_k, x)
            with scope("w_proj"):
                if x:
                    arrived(v.proj, m.proj, k, k * nt + lead)
                else:
                    arrived_from_lead(v.proj, m.proj, k)
            second = (v.first[k] + v.proj[k].astype(F32)).astype(BF16).astype(F32)
            if x == 0:
                for t in range(nt):
                    v.second[t] = second[:, t * width : (t + 1) * width]
            yield second, gain_cut(k, 2), columns(k, block)

    loaded("gate1", "up1")
    hidden = gated(arriving_blocks(), 1, nk - 1)
    loaded("down1")
    for x in range(nk)[::-1]:
        k = flipped(me_k, x)
        piece = nn_dot(hidden, v.down[1, :, columns(k, block)])
        for t in range(nt):
            v.cut_b[k * nt + t] = piece[:, t * width : (t + 1) * width].astype(BF16)
        for d in range(nt)[::-1]:
            if x or d:
                q = k * nt + lax.rem(me_t + d, nt)
                send(v.cut_b.at[q], v.cut.at[me], m.cut[0].at[q], m.cut[1].at[me], q)
    v.cut[me] = v.cut_b[me]
    with scope("w_cut"):
        for q in all_peers():
            arrived(v.cut, m.cut, q, q)
    total = sum(v.cut[q].astype(F32) for q in range(n))
    out[...] = (v.second[me_t] + 0.5 * total).astype(BF16)
    with scope("w_sent"):
        for copy in sent:
            copy.wait_send()

        @pl.when(me_t == lead)
        def _():
            for copy in first_sends():
                copy.wait_send()
            for copy in bc_sends():
                copy.wait_send()
            for copy in proj_sends():
                copy.wait_send()

        @pl.when(me_t != lead)
        def _():
            slab_home().wait_send()
            to_home(v.hist, m.hist).wait_send()
            to_home(v.xz, m.xz).wait_send()
            tap_home().wait_send()
            for copy in pushes():
                copy.wait_send()


def fused_layer(
    nk,
    nt,
    resid,
    norm_gain,
    ffn_gate,
    ffn_up,
    ffn_down,
    w_x,
    w_z,
    w_bc,
    w_dt,
    dt_bias,
    a_log,
    d_skip,
    conv_wx,
    conv_wbc,
    conv_x,
    conv_bc,
    ssm_state,
    w_out,
):
    n = nk * nt
    rows, width = resid.shape
    dim = ffn_gate.shape[1]
    units = ffn_gate.shape[2]
    local = w_x.shape[1] * w_x.shape[2]
    heads, half = conv_x.shape[2], conv_x.shape[3]
    flat = heads * half
    span = w_bc.shape[0]
    lanes = w_bc.shape[3]
    pairs = w_bc.shape[1] * w_bc.shape[2]
    out_cols = w_out.shape[2]
    taps = conv_wx.shape[0]
    block = nt * width
    args = (
        resid,
        norm_gain,
        jnp.swapaxes(ffn_gate, 1, 2),
        jnp.swapaxes(ffn_up, 1, 2),
        ffn_down,
        jnp.transpose(w_x, (1, 2, 0)).reshape(local, dim),
        jnp.transpose(w_z, (1, 2, 0)).reshape(local, dim),
        w_bc.reshape(span * pairs, lanes),
        w_dt.T,
        dt_bias.reshape(1, heads),
        a_log.reshape(1, heads),
        d_skip.reshape(1, heads),
        jnp.swapaxes(conv_wx, 1, 2),
        conv_wbc.reshape(taps, pairs, lanes),
        jnp.swapaxes(conv_x, 2, 3).reshape(taps - 1, half, heads),
        conv_bc.reshape(taps - 1, pairs, lanes),
        ssm_state.reshape(flat, lanes),
        w_out.reshape(flat, out_cols),
    )
    dma = pltpu.SemaphoreType.DMA
    vmem = pltpu.VMEM
    scratch = dict(
        gate=vmem((2, units, dim), BF16),
        up=vmem((2, units, dim), BF16),
        down=vmem((2, units, dim), BF16),
        wx=vmem((local, dim), BF16),
        wz=vmem((local, dim), BF16),
        wbc=vmem((span * pairs, lanes), BF16),
        wide=vmem((span, pairs * lanes), BF16),
        wdt=vmem((heads, span), BF16),
        state=vmem((nt, flat, lanes), F32),
        state_b=vmem((nt, flat, lanes), BF16),
        wout=vmem((nt, flat, out_cols), BF16),
        small=vmem((3, 1, heads), F32),
        cwx=vmem((taps, half, heads), BF16),
        cwbc=vmem((taps, pairs, lanes), BF16),
        cx=vmem((taps - 1, half, heads), BF16),
        cbc=vmem((taps - 1, pairs, lanes), BF16),
        expand=vmem((heads, flat), BF16),
        perm=vmem((256, 256), BF16),
        rows=vmem((n, rows, width), BF16),
        gain=vmem((n, 3, width), BF16),
        part=vmem((nk, rows, block), BF16),
        slab=vmem((n, rows, block), BF16),
        near=vmem((nk, rows, block), BF16),
        held=vmem((nk - 1, 2, rows, units), F32),
        first=vmem((nk, rows, block), F32),
        scale=vmem((rows, lanes), F32),
        bc_b=vmem((nk * (pairs + 8), lanes), F32),
        bc=vmem((nk, pairs + 8, lanes), F32),
        hist=vmem((nk, nt, 1, flat), F32),
        tap=vmem((nt, 1, flat), F32),
        line=vmem((1, flat), F32),
        xz=vmem((nk, nt, rows, 2 * local), BF16),
        xconv=vmem((nt, rows, flat), F32),
        open=vmem((nt, rows, flat), F32),
        mix=vmem((nk, nt + 1, flat), BF16),
        proj=vmem((nk, rows, out_cols), BF16),
        second=vmem((nt, rows, width), F32),
        cut_b=vmem((n, rows, width), BF16),
        cut=vmem((n, rows, width), BF16),
    )
    rounds = dict(
        rows=n, gain=n, slab=n, near=n, bc=n, hist=n, xz=n, mix=nk, state=nt, wout=nt, tap=nt, proj=n, cut=n
    )
    sems = {name: (dma((count,)), dma((count,))) for name, count in rounds.items()}
    sems["load"] = dma((17,))
    sems["lead"] = dma((4,))

    def kernel(*refs, **held):
        def body(**flags):
            layer_kernel(nk, nt, *refs, SimpleNamespace(**held), SimpleNamespace(**flags))

        pl.run_scoped(body, **sems)

    return pl.pallas_call(
        kernel,
        out_shape=pltpu.VMEM(resid.shape, resid.dtype),
        in_specs=[pl.BlockSpec(memory_space=pl.ANY)] * len(args),
        out_specs=pl.BlockSpec(memory_space=pltpu.VMEM),
        scratch_shapes=scratch,
        compiler_params=pltpu.CompilerParams(
            collective_id=0, has_side_effects=True, vmem_limit_bytes=60 * 1024 * 1024
        ),
    )(*args)


def fits(nk, nt, resid, w_x, w_bc, conv_x):
    rows, width = resid.shape
    half = conv_x.shape[3]
    pairs = w_bc.shape[1] * w_bc.shape[2]
    return (
        conv_x.shape[0] == 1
        and rows == nk
        and nt > 1
        and nk & (nk - 1) == 0
        and w_bc.shape[0] == nt * width
        and width % 128 == 0
        and w_bc.shape[0] % 128 == 0
        and (w_x.shape[1] * w_x.shape[2]) % 128 == 0
        and half & (half - 1) == 0
        and pairs & (pairs - 1) == 0
        and pairs % 8 == 0
        and 256 % pairs == 0
        and (w_bc.shape[0] * pairs) % 256 == 0
        and w_bc.shape[3] == 128
        and conv_x.shape[2] < 128
    )


def solution(mesh):
    placed = (
        P("dp", ("kv", "tp")),
        P(None, ("kv", "tp")),
        P(None, None, ("kv", "tp")),
        P(None, None, ("kv", "tp")),
        P(None, ("kv", "tp"), None),
        P(None, "kv", "tp"),
        P(None, "kv", "tp"),
        P("kv", None, None, None),
        P("kv", None),
        P(),
        P(),
        P(),
        P(None, None, "tp"),
        P(),
        P(("dp", "kv"), None, None, "tp"),
        P(("dp", "kv"), None, None, None, None),
        P(("dp", "kv"), None, "tp", None),
        P(None, "tp", "kv"),
    )
    nk, nt = mesh.shape["kv"], mesh.shape["tp"]

    def layer(*args):
        if fits(nk, nt, args[0], args[5], args[7], args[14]):
            return fused_layer(nk, nt, *args)
        return per_device(*args)

    return jax.shard_map(
        layer, mesh=mesh, in_specs=placed, out_specs=P("dp", ("kv", "tp")), check_vma=False
    )
```

```python
from types import SimpleNamespace

import jax
import jax.numpy as jnp
from jax import lax
from jax.experimental import pallas as pl
from jax.experimental.pallas import tpu as pltpu
from jax.sharding import PartitionSpec as P

D = 2048
F32 = jnp.float32
BF16 = jnp.bfloat16
MESH = pl.DeviceIdType.MESH

EPS = 1e-06


def normalize(rows, gain):
    values = rows.astype(jnp.float32)
    scale = lax.rsqrt(jnp.mean(values * values, axis=1, keepdims=True) + EPS)
    return (values * scale * gain.astype(jnp.float32).reshape(1, -1)).astype(jnp.bfloat16)


def feed_forward(normed, w_gate, w_up, w_down):
    gate = jnp.dot(normed, w_gate, preferred_element_type=jnp.float32)
    upper = jnp.dot(normed, w_up, preferred_element_type=jnp.float32)
    hidden = (jax.nn.silu(gate) * upper).astype(jnp.bfloat16)
    return jnp.dot(hidden, w_down, preferred_element_type=jnp.float32)


def add_half(base, sums):
    return (base.astype(jnp.float32) + 0.5 * sums).astype(jnp.bfloat16)


def ffn_totals(partial_value):
    return lax.psum(partial_value, ("kv", "tp"))


def short_conv(history, newest, taps):
    window = jnp.concatenate(
        [history.astype(jnp.float32), newest.astype(jnp.float32)[:, None]], axis=1
    )
    return jax.nn.silu(jnp.sum(window * taps.astype(jnp.float32)[None], axis=1))


def state_step(
    xs_new,
    zeta,
    bc_new,
    dt_raw,
    conv_x,
    conv_bc,
    ssm_state,
    conv_wx,
    conv_wbc,
    dt_bias,
    a_log,
    d_skip,
):
    xconv = short_conv(conv_x, xs_new, conv_wx)
    bconv = short_conv(conv_bc, bc_new, conv_wbc)
    heads = xconv.shape[1]
    groups = bconv.shape[2]
    bmat = jnp.repeat(bconv[:, 0], heads // groups, axis=1)
    cmat = jnp.repeat(bconv[:, 1], heads // groups, axis=1)
    step_size = jax.nn.softplus(dt_raw + dt_bias[None, :])
    decay = jnp.exp(-step_size * jnp.exp(a_log)[None, :])
    updated = (
        decay[:, :, None, None] * ssm_state
        + (step_size[:, :, None] * xconv)[..., None] * bmat[:, :, None, :]
    )
    mixed = (
        jnp.einsum("shpn,shn->shp", updated, cmat, precision=lax.Precision.HIGHEST)
        + d_skip[None, :, None] * xconv
    )
    return (mixed * jax.nn.silu(zeta.astype(jnp.float32))).astype(jnp.bfloat16)


def group_terms(slab, w_bc, w_dt):
    span = slab.shape[1]
    flat_bc = w_bc.reshape(span, -1)
    bc_part = jnp.dot(slab, flat_bc, preferred_element_type=jnp.float32)
    dt_part = jnp.dot(slab, w_dt, preferred_element_type=jnp.float32)
    return (
        lax.psum_scatter(bc_part, "kv", scatter_dimension=0, tiled=True),
        lax.psum_scatter(dt_part, "kv", scatter_dimension=0, tiled=True),
    )


def mix_partial(
    normed,
    w_x,
    w_z,
    w_bc,
    w_dt,
    dt_bias,
    a_log,
    d_skip,
    conv_wx,
    conv_wbc,
    conv_x,
    conv_bc,
    ssm_state,
    w_out,
):
    rows = normed.shape[0]
    local_heads = w_x.shape[1]
    half = w_x.shape[2]
    xs_part = (
        jnp.dot(normed, w_x.reshape(D, -1), preferred_element_type=jnp.float32)
        .astype(jnp.bfloat16)
        .reshape(rows, local_heads, half)
    )
    zeta_part = (
        jnp.dot(normed, w_z.reshape(D, -1), preferred_element_type=jnp.float32)
        .astype(jnp.bfloat16)
        .reshape(rows, local_heads, half)
    )
    xs_new, zeta = (
        lax.all_to_all(xs_part, "kv", split_axis=0, concat_axis=1, tiled=True),
        lax.all_to_all(zeta_part, "kv", split_axis=0, concat_axis=1, tiled=True),
    )
    span = w_bc.shape[0]
    slab = lax.dynamic_slice_in_dim(normed, lax.axis_index("kv") * span, span, 1)
    bc_sum, dt_raw = group_terms(slab, w_bc, w_dt)
    bc_new = bc_sum.astype(jnp.bfloat16).reshape((bc_sum.shape[0],) + w_bc.shape[1:])
    mixed = state_step(
        xs_new,
        zeta,
        bc_new,
        dt_raw,
        conv_x,
        conv_bc,
        ssm_state,
        conv_wx,
        conv_wbc,
        dt_bias,
        a_log,
        d_skip,
    )
    flat_out = w_out.reshape(-1, w_out.shape[2])
    piece = lax.all_gather(mixed, "kv", axis=0, tiled=True)
    return jnp.dot(piece.reshape(piece.shape[0], -1), flat_out, preferred_element_type=jnp.float32)


def per_device(
    resid,
    norm_gain,
    ffn_gate,
    ffn_up,
    ffn_down,
    w_x,
    w_z,
    w_bc,
    w_dt,
    dt_bias,
    a_log,
    d_skip,
    conv_wx,
    conv_wbc,
    conv_x,
    conv_bc,
    ssm_state,
    w_out,
):
    mixer_args = (
        w_x,
        w_z,
        w_bc,
        w_dt,
        dt_bias,
        a_log,
        d_skip,
        conv_wx,
        conv_wbc,
        conv_x,
        conv_bc,
        ssm_state,
        w_out,
    )
    rows, gains = (
        lax.all_gather(resid, ("kv", "tp"), axis=1, tiled=True),
        lax.all_gather(norm_gain, ("kv", "tp"), axis=1, tiled=True),
    )
    first = add_half(
        rows,
        ffn_totals(feed_forward(normalize(rows, gains[0]), ffn_gate[0], ffn_up[0], ffn_down[0])),
    )
    partial_value = mix_partial(normalize(first, gains[1]), *mixer_args)
    span = partial_value.shape[1]
    block = lax.dynamic_slice_in_dim(first, lax.axis_index("kv") * span, span, 1)
    joined = (block.astype(jnp.float32) + lax.psum(partial_value, "tp")).astype(jnp.bfloat16)
    second = lax.all_gather(joined, "kv", axis=1, tiled=True)
    final = add_half(
        second,
        ffn_totals(feed_forward(normalize(second, gains[2]), ffn_gate[1], ffn_up[1], ffn_down[1])),
    )
    width = resid.shape[1]
    return lax.dynamic_slice_in_dim(final, lax.axis_index(("kv", "tp")) * width, width, 1)


def nt_dot(left, right):
    return lax.dot_general(left, right, (((1,), (1,)), ((), ())), preferred_element_type=F32)


def nn_dot(left, right):
    return jnp.dot(left, right, preferred_element_type=F32)


def silu(value):
    return value * jax.nn.sigmoid(value)


def norm_rows(values, gain):
    scale = lax.rsqrt(jnp.mean(values * values, axis=1, keepdims=True) + EPS)
    return (values * scale * gain).astype(BF16)


def split_two(value):
    high = value.astype(BF16)
    return high, (value - high.astype(F32)).astype(BF16)


def layer_kernel(
    nk,
    nt,
    resid,
    gains,
    gate,
    up,
    down,
    wx,
    wz,
    wbc,
    wdt,
    dt_bias,
    a_log,
    d_skip,
    cwx,
    cwbc,
    cx,
    cbc,
    state,
    wout,
    out,
    v,
    m,
):
    me_k, me_t = lax.axis_index("kv"), lax.axis_index("tp")
    n = nk * nt
    me = me_k * nt + me_t
    lead = nt - 1
    rows, width = resid.shape
    dim = n * width
    block = nt * width
    scope = jax.named_scope

    def target(index):
        return {"kv": lax.div(index, nt), "tp": lax.rem(index, nt)}

    def flipped(index, mask):
        bit = 1
        while bit < nk:
            if mask & bit:
                index = index + bit - 2 * bit * lax.rem(lax.div(index, bit), 2)
            bit *= 2
        return index

    def all_peers():
        order = [(x, d) for x in range(nk) for d in range(nt)][1:]
        return [flipped(me_k, x) * nt + lax.rem(me_t + d, nt) for x, d in order]

    def kv_peers():
        return [flipped(me_k, x) for x in range(1, nk)]

    loads = {}

    def load(name, src, dst):
        copy = pltpu.make_async_copy(src, dst, m.load.at[len(loads)])
        copy.start()
        loads[name] = copy

    def loaded(*names):
        with scope("w_" + names[0]):
            for name in names:
                loads[name].wait()

    load("rows", resid, v.rows.at[me])
    load("gains", gains, v.gain.at[me])
    barrier = pltpu.get_barrier_semaphore()
    for q in all_peers()[::-1]:
        pl.semaphore_signal(barrier, inc=1, device_id=target(q), device_id_type=MESH)
    load("bias", dt_bias, v.small.at[0])
    load("alog", a_log, v.small.at[1])
    load("skip", d_skip, v.small.at[2])
    load("cwx", cwx, v.cwx)
    load("cwbc", cwbc, v.cwbc)
    load("cx", cx, v.cx)
    load("cbc", cbc, v.cbc)
    load("gate0", gate.at[0], v.gate.at[0])
    load("up0", up.at[0], v.up.at[0])
    load("down0", down.at[0], v.down.at[0])
    lead_loads = (
        (wbc, v.wbc),
        (wdt, v.wdt),
        (state, v.state.at[lead]),
        (wout, v.wout.at[lead]),
    )

    def lead_load(i):
        return pltpu.make_async_copy(*lead_loads[i], m.lead.at[i])

    @pl.when(me_t == lead)
    def _():
        for i in range(3):
            lead_load(i).start()

    load("wx", wx, v.wx)
    load("wz", wz, v.wz)

    @pl.when(me_t == lead)
    def _():
        lead_load(3).start()

    load("gate1", gate.at[1], v.gate.at[1])
    load("up1", up.at[1], v.up.at[1])
    load("down1", down.at[1], v.down.at[1])
    with scope("w_barrier"):
        pl.semaphore_wait(barrier, n - 1)

    def remote(src, dst, ssem, rsem, index):
        return pltpu.make_async_remote_copy(
            src_ref=src,
            dst_ref=dst,
            send_sem=ssem,
            recv_sem=rsem,
            device_id=target(index),
            device_id_type=MESH,
        )

    sent = []

    def send(src, dst, ssem, rsem, index):
        copy = remote(src, dst, ssem, rsem, index)
        copy.start()
        sent.append(copy)

    def arrived(slots, sems, slot, index):
        remote(slots.at[slot], slots.at[slot], sems[0].at[slot], sems[1].at[slot], index).wait_recv()

    loaded("rows", "gains")
    for q in all_peers()[::-1]:
        send(v.rows.at[me], v.rows.at[me], m.rows[0].at[q], m.rows[1].at[me], q)
        send(v.gain.at[me], v.gain.at[me], m.gain[0].at[q], m.gain[1].at[me], q)

    home = me_k * nt + lead

    def pushes():
        yield remote(state, v.state.at[me_t], m.state[0].at[me_t], m.state[1].at[me_t], home)
        yield remote(wout, v.wout.at[me_t], m.wout[0].at[me_t], m.wout[1].at[me_t], home)

    @pl.when(me_t != lead)
    def _():
        for copy in pushes():
            copy.start()

    heads, half = v.cx.shape[2], v.cx.shape[1]
    flat = heads * half
    groups = v.cwbc.shape[1] // 2
    pairs = 2 * groups
    lane = lax.broadcasted_iota(jnp.int32, v.expand.shape, 1)
    head_of = lax.broadcasted_iota(jnp.int32, v.expand.shape, 0) * half
    v.expand[...] = jnp.where((lane >= head_of) & (lane < head_of + half), 1.0, 0.0).astype(BF16)
    tile = v.perm.shape[0]
    deep = tile // pairs
    row = lax.broadcasted_iota(jnp.int32, v.perm.shape, 0)
    lane = lax.broadcasted_iota(jnp.int32, v.perm.shape, 1)
    source = (row & (deep - 1)) * pairs + lax.shift_right_logical(row, deep.bit_length() - 1)
    v.perm[...] = jnp.where(lane == source, 1.0, 0.0).astype(BF16)

    def expand(value):
        return nn_dot(value, v.expand[...])

    loaded("bias", "alog", "skip", "cwx", "cwbc", "cx", "cbc")
    taps = v.cx.shape[0]
    known = sum(v.cx[i].astype(F32) * v.cwx[i].astype(F32) for i in range(taps))
    high, low = split_two(known)
    lane = lax.broadcasted_iota(jnp.int32, (half, flat), 1)
    row = lax.broadcasted_iota(jnp.int32, (half, flat), 0)
    own = (lane & (half - 1)) == row
    v.hist[me_k, me_t] = jnp.sum(
        jnp.where(own, expand(high) + expand(low), 0.0), axis=0, keepdims=True
    )
    v.tap[me_t] = jnp.sum(jnp.where(own, expand(v.cwx[taps]), 0.0), axis=0, keepdims=True)
    skip_high, skip_low = split_two(v.small[2])
    v.line[...] = expand(skip_high) + expand(skip_low)

    def to_leads(ref, sems):
        for k in kv_peers()[::-1]:
            q = k * nt + lead
            yield remote(ref.at[me_k, me_t], ref.at[me_k, me_t], sems[0].at[k], sems[1].at[me], q)

    def to_home(ref, sems):
        return remote(
            ref.at[me_k, me_t], ref.at[me_k, me_t], sems[0].at[me_k], sems[1].at[me], home
        )

    def tap_home():
        return remote(v.tap.at[me_t], v.tap.at[me_t], m.tap[0].at[me_t], m.tap[1].at[me_t], home)

    for copy in to_leads(v.hist, m.hist):
        copy.start()
        sent.append(copy)

    @pl.when(me_t != lead)
    def _():
        to_home(v.hist, m.hist).start()
        tap_home().start()

    hist_bc = sum(v.cbc[i].astype(F32) * v.cwbc[i].astype(F32) for i in range(taps))
    tap_bc = v.cwbc[taps].astype(F32)

    units = v.gate.shape[1]

    def gated(blocks, kept):
        squares = jnp.zeros((rows, 1), F32)
        g = jnp.zeros((rows, units), F32)
        u = jnp.zeros((rows, units), F32)
        for step, (values, gain, at) in enumerate(blocks):
            squares = squares + jnp.sum(values * values, axis=1, keepdims=True)
            left = (values * gain).astype(BF16)
            g = g + nn_dot(left, v.gate_t[at, :])
            u = u + nn_dot(left, v.up_t[at, :])
            if step < kept:
                v.held[step, 0] = g
                v.held[step, 1] = u
                g = jnp.zeros((rows, units), F32)
                u = jnp.zeros((rows, units), F32)
        for step in range(kept):
            g = g + v.held[step, 0]
            u = u + v.held[step, 1]
        scale = lax.rsqrt(squares / dim + EPS)
        return (silu(g * scale) * (u * scale)).astype(BF16)

    def turn(source, dest):
        for k in range(dim // 256):
            at = slice(k * 256, (k + 1) * 256)
            dest[at, :] = source[:, at].T

    def turn_ffn(which):
        loaded(f"gate{which}", f"up{which}")
        turn(v.gate.at[which], v.gate_t)
        turn(v.up.at[which], v.up_t)

    def columns(index, count):
        return pl.ds(pl.multiple_of(index * count, 128), count)

    def arriving_rows():
        for q in [me] + all_peers():
            if q is not me:
                with scope("w_rows"):
                    arrived(v.rows, m.rows, q, q)
                    arrived(v.gain, m.gain, q, q)
            yield v.rows[q].astype(F32), v.gain[q, 0:1, :].astype(F32), columns(q, width)

    turn_ffn(0)
    hidden = gated(arriving_rows(), 0)
    loaded("down0")
    for x in range(nk)[::-1]:
        k = flipped(me_k, x)
        v.part[k] = nn_dot(hidden, v.down[0, :, columns(k, block)]).astype(BF16)
        q = k * nt + lead
        if x:
            send(v.part.at[k], v.slab.at[me], m.slab[0].at[q], m.slab[1].at[me], q)

    def slab_home():
        q = me_k * nt + lead
        return remote(v.part.at[me_k], v.slab.at[me], m.slab[0].at[q], m.slab[1].at[me], q)

    @pl.when(me_t != lead)
    def _():
        slab_home().start()

    def gain_cut(index, i):
        return jnp.concatenate(
            [v.gain[index * nt + t, i : i + 1, :].astype(F32) for t in range(nt)], axis=1
        )

    def rows_cut(index):
        return jnp.concatenate([v.rows[index * nt + t].astype(F32) for t in range(nt)], axis=1)

    tall = v.bc.shape[1]

    def bc_row(k):
        return v.bc_b.at[pl.ds(pl.multiple_of(k * tall, 8), tall), :]

    def first_sends():
        for q in all_peers()[::-1]:
            yield remote(v.near.at[me_k], v.near.at[me_k], m.near[0].at[q], m.near[1].at[me_k], q)

    def bc_sends():
        for k in kv_peers()[::-1]:
            q = k * nt + lead
            yield remote(bc_row(k), v.bc.at[me_k], m.bc[0].at[k], m.bc[1].at[me_k], q)

    @pl.when(me_t == lead)
    def _():
        with scope("w_wbc"):
            lead_load(0).wait()
            lead_load(1).wait()
        span = v.wdt.shape[1]
        for c in range(span // deep):
            piece = nn_dot(v.perm[...], v.wbc[c * tile : (c + 1) * tile, :]).astype(BF16)
            for p in range(pairs):
                v.wide[c * deep : (c + 1) * deep, p * 128 : (p + 1) * 128] = piece[
                    p * deep : (p + 1) * deep, :
                ]
        with scope("w_state"):
            lead_load(2).wait()
            for t in range(lead):
                arrived(v.state, m.state, t, me_k * nt + t)
        for t in range(nt):
            for i in range(flat // 256):
                at = slice(i * 256, (i + 1) * 256)
                v.state_b[t, :, at] = v.state[t, at, :].astype(BF16).T
        v.slab[me] = v.part[me_k]
        with scope("w_slab"):
            for q in all_peers():
                arrived(v.slab, m.slab, q, q)
        total = sum(v.slab[q].astype(F32) for q in range(n))
        first = (rows_cut(me_k) + 0.5 * total).astype(BF16)
        v.near[me_k] = first
        for copy in first_sends():
            copy.start()
        left = (first.astype(F32) * gain_cut(me_k, 1)).astype(BF16)
        bc_part = nn_dot(left, v.wide[...])
        dt_part = nt_dot(left, v.wdt[...])
        for p in range(pairs):
            v.bc_b[pl.ds(p, rows, stride=tall), :] = bc_part[:, p * 128 : (p + 1) * 128]
        v.bc_b[pl.ds(pairs, rows, stride=tall), :] = jnp.concatenate(
            [dt_part, jnp.zeros((rows, 128 - heads), F32)], axis=1
        )
        for copy in bc_sends():
            copy.start()
        v.bc[me_k] = bc_row(me_k)[...]

    def arrived_at(slots, sems, k, t):
        q = k * nt + t
        remote(slots.at[k, t], slots.at[k, t], sems[0].at[k], sems[1].at[q], q).wait_recv()

    def arrived_from_lead(slots, sems, k):
        @pl.when(k * nt + lead != me)
        def _():
            arrived(slots, sems, k, k * nt + lead)

    loaded("wx", "wz")
    turn(v.wx, v.wx_t)
    turn(v.wz, v.wz_t)
    local = v.wx.shape[0]
    xs_part = jnp.zeros((rows, local), F32)
    z_part = jnp.zeros((rows, local), F32)
    squares = jnp.zeros((rows, 1), F32)
    for x in range(nk):
        k = flipped(me_k, x)
        with scope("w_near"):
            if x:
                arrived(v.near, m.near, k, k * nt + lead)
            else:
                arrived_from_lead(v.near, m.near, k)
        first = v.near[k].astype(F32)
        v.first[k] = first
        left = (first * gain_cut(k, 1)).astype(BF16)
        squares = squares + jnp.sum(first * first, axis=1, keepdims=True)
        xs_part = xs_part + nn_dot(left, v.wx_t[columns(k, block), :])
        z_part = z_part + nn_dot(left, v.wz_t[columns(k, block), :])
    scale = lax.rsqrt(squares / dim + EPS)
    v.scale[...] = jnp.broadcast_to(scale, v.scale.shape)
    v.xz[me_k, me_t] = jnp.concatenate([xs_part * scale, z_part * scale], axis=1).astype(BF16)
    for copy in to_leads(v.xz, m.xz):
        copy.start()
        sent.append(copy)

    @pl.when(me_t != lead)
    def _():
        to_home(v.xz, m.xz).start()
        turn_ffn(1)

    def proj_sends():
        for q in all_peers()[::-1]:
            yield remote(v.proj.at[me_k], v.proj.at[me_k], m.proj[0].at[q], m.proj[1].at[me_k], q)

    @pl.when(me_t == lead)
    def _():
        with scope("w_bc"):
            for k in kv_peers():
                arrived(v.bc, m.bc, k, k * nt + lead)
        summed = sum(v.bc[k] for k in range(nk)) * v.scale[pl.ds(me_k, 1), :]
        raw = summed[pairs : pairs + 1, :heads] + v.small[0]
        step = jnp.maximum(raw, 0.0) + jnp.log1p(jnp.exp(-jnp.abs(raw)))
        decay = jnp.exp(-step * jnp.exp(v.small[1]))
        step_high, step_low = split_two(step)
        decay_high, decay_low = split_two(decay)
        spread = expand(jnp.concatenate([decay_high, decay_low, step_high, step_low], axis=0))
        decay_row = spread[0:1] + spread[1:2]
        step_row = spread[2:3] + spread[3:4]
        bc_new = summed[:pairs].astype(BF16).astype(F32)
        bconv = silu(hist_bc + bc_new * tap_bc)
        bmat, cmat = bconv[:groups], bconv[groups:]
        weight = jnp.sum(bmat * cmat, axis=1, keepdims=True)
        lane = lax.broadcasted_iota(jnp.int32, (groups, flat), 1)
        low_end = lax.broadcasted_iota(jnp.int32, (groups, flat), 0) * (flat // groups)
        mine = (lane >= low_end) & (lane < low_end + flat // groups)
        lines = []
        for t in range(nt):
            per_group = nn_dot(cmat.astype(BF16), v.state_b[t])
            read = jnp.sum(jnp.where(mine, per_group, 0.0), axis=0, keepdims=True)
            lines.append(decay_row * read)
        cross = jnp.sum(jnp.where(mine, weight, 0.0), axis=0, keepdims=True)
        lines.append(step_row * cross + v.line[...])
        v.mix[me_k] = jnp.concatenate(lines, axis=0).astype(BF16)

        def mix_sends():
            for k in kv_peers()[::-1]:
                q = k * nt + lead
                yield remote(v.mix.at[me_k], v.mix.at[me_k], m.mix[0].at[k], m.mix[1].at[me_k], q)

        for copy in mix_sends():
            copy.start()
        turn_ffn(1)
        with scope("w_hist"):
            for t in range(lead):
                arrived(v.tap, m.tap, t, me_k * nt + t)
                arrived_at(v.hist, m.hist, me_k, t)
            for k in kv_peers():
                for t in range(nt):
                    arrived_at(v.hist, m.hist, k, t)
        with scope("w_wout"):
            lead_load(3).wait()
            for t in range(lead):
                arrived(v.wout, m.wout, t, me_k * nt + t)
        with scope("w_xz"):
            for t in range(lead):
                arrived_at(v.xz, m.xz, me_k, t)
            for k in kv_peers():
                for t in range(nt):
                    arrived_at(v.xz, m.xz, k, t)
        for t in range(nt):
            for k in range(nk):
                at = slice(k * local, (k + 1) * local)
                past = jnp.concatenate([v.hist[i, t][:, at] for i in range(nk)], axis=0)
                xs_new = v.xz[k, t][:, :local].astype(F32)
                v.xconv[t, :, at] = silu(past + xs_new * v.tap[t][:, at])
                v.open[t, :, at] = silu(v.xz[k, t][:, local:].astype(F32))
        with scope("w_mix"):
            for k in kv_peers():
                arrived(v.mix, m.mix, k, k * nt + lead)
        pieces = [v.mix[k].astype(F32) for k in range(nk)]
        direct = jnp.concatenate([piece[nt : nt + 1] for piece in pieces], axis=0)
        total = jnp.zeros((rows, v.wout.shape[2]), F32)
        for t in range(nt):
            read = jnp.concatenate([piece[t : t + 1] for piece in pieces], axis=0)
            mixed = ((read + direct * v.xconv[t]) * v.open[t]).astype(BF16)
            total = total + nn_dot(mixed, v.wout[t])
        v.proj[me_k] = total.astype(BF16)
        for copy in proj_sends():
            copy.start()
        for copy in mix_sends():
            copy.wait_send()

    def arriving_blocks():
        for x in range(nk):
            k = flipped(me_k, x)
            with scope("w_proj"):
                if x:
                    arrived(v.proj, m.proj, k, k * nt + lead)
                else:
                    arrived_from_lead(v.proj, m.proj, k)
            second = (v.first[k] + v.proj[k].astype(F32)).astype(BF16).astype(F32)
            if x == 0:
                for t in range(nt):
                    v.second[t] = second[:, t * width : (t + 1) * width]
            yield second, gain_cut(k, 2), columns(k, block)

    hidden = gated(arriving_blocks(), nk - 1)
    loaded("down1")
    for x in range(nk)[::-1]:
        k = flipped(me_k, x)
        piece = nn_dot(hidden, v.down[1, :, columns(k, block)])
        for t in range(nt):
            v.cut_b[k * nt + t] = piece[:, t * width : (t + 1) * width].astype(BF16)
        for d in range(nt)[::-1]:
            if x or d:
                q = k * nt + lax.rem(me_t + d, nt)
                send(v.cut_b.at[q], v.cut.at[me], m.cut[0].at[q], m.cut[1].at[me], q)
    v.cut[me] = v.cut_b[me]
    with scope("w_cut"):
        for q in all_peers():
            arrived(v.cut, m.cut, q, q)
    total = sum(v.cut[q].astype(F32) for q in range(n))
    out[...] = (v.second[me_t] + 0.5 * total).astype(BF16)
    with scope("w_sent"):
        for copy in sent:
            copy.wait_send()

        @pl.when(me_t == lead)
        def _():
            for copy in first_sends():
                copy.wait_send()
            for copy in bc_sends():
                copy.wait_send()
            for copy in proj_sends():
                copy.wait_send()

        @pl.when(me_t != lead)
        def _():
            slab_home().wait_send()
            to_home(v.hist, m.hist).wait_send()
            to_home(v.xz, m.xz).wait_send()
            tap_home().wait_send()
            for copy in pushes():
                copy.wait_send()


def fused_layer(
    nk,
    nt,
    resid,
    norm_gain,
    ffn_gate,
    ffn_up,
    ffn_down,
    w_x,
    w_z,
    w_bc,
    w_dt,
    dt_bias,
    a_log,
    d_skip,
    conv_wx,
    conv_wbc,
    conv_x,
    conv_bc,
    ssm_state,
    w_out,
):
    n = nk * nt
    rows, width = resid.shape
    dim = ffn_gate.shape[1]
    units = ffn_gate.shape[2]
    local = w_x.shape[1] * w_x.shape[2]
    heads, half = conv_x.shape[2], conv_x.shape[3]
    flat = heads * half
    span = w_bc.shape[0]
    lanes = w_bc.shape[3]
    pairs = w_bc.shape[1] * w_bc.shape[2]
    out_cols = w_out.shape[2]
    taps = conv_wx.shape[0]
    block = nt * width
    args = (
        resid,
        norm_gain,
        jnp.swapaxes(ffn_gate, 1, 2),
        jnp.swapaxes(ffn_up, 1, 2),
        ffn_down,
        jnp.transpose(w_x, (1, 2, 0)).reshape(local, dim),
        jnp.transpose(w_z, (1, 2, 0)).reshape(local, dim),
        w_bc.reshape(span * pairs, lanes),
        w_dt.T,
        dt_bias.reshape(1, heads),
        a_log.reshape(1, heads),
        d_skip.reshape(1, heads),
        jnp.swapaxes(conv_wx, 1, 2),
        conv_wbc.reshape(taps, pairs, lanes),
        jnp.swapaxes(conv_x, 2, 3).reshape(taps - 1, half, heads),
        conv_bc.reshape(taps - 1, pairs, lanes),
        ssm_state.reshape(flat, lanes),
        w_out.reshape(flat, out_cols),
    )
    dma = pltpu.SemaphoreType.DMA
    vmem = pltpu.VMEM
    scratch = dict(
        gate=vmem((2, units, dim), BF16),
        up=vmem((2, units, dim), BF16),
        down=vmem((2, units, dim), BF16),
        gate_t=vmem((dim, units), BF16),
        up_t=vmem((dim, units), BF16),
        wx_t=vmem((dim, local), BF16),
        wz_t=vmem((dim, local), BF16),
        wx=vmem((local, dim), BF16),
        wz=vmem((local, dim), BF16),
        wbc=vmem((span * pairs, lanes), BF16),
        wide=vmem((span, pairs * lanes), BF16),
        wdt=vmem((heads, span), BF16),
        state=vmem((nt, flat, lanes), F32),
        state_b=vmem((nt, lanes, flat), BF16),
        wout=vmem((nt, flat, out_cols), BF16),
        small=vmem((3, 1, heads), F32),
        cwx=vmem((taps, half, heads), BF16),
        cwbc=vmem((taps, pairs, lanes), BF16),
        cx=vmem((taps - 1, half, heads), BF16),
        cbc=vmem((taps - 1, pairs, lanes), BF16),
        expand=vmem((heads, flat), BF16),
        perm=vmem((256, 256), BF16),
        rows=vmem((n, rows, width), BF16),
        gain=vmem((n, 3, width), BF16),
        part=vmem((nk, rows, block), BF16),
        slab=vmem((n, rows, block), BF16),
        near=vmem((nk, rows, block), BF16),
        held=vmem((nk - 1, 2, rows, units), F32),
        first=vmem((nk, rows, block), F32),
        scale=vmem((rows, lanes), F32),
        bc_b=vmem((nk * (pairs + 8), lanes), F32),
        bc=vmem((nk, pairs + 8, lanes), F32),
        hist=vmem((nk, nt, 1, flat), F32),
        tap=vmem((nt, 1, flat), F32),
        line=vmem((1, flat), F32),
        xz=vmem((nk, nt, rows, 2 * local), BF16),
        xconv=vmem((nt, rows, flat), F32),
        open=vmem((nt, rows, flat), F32),
        mix=vmem((nk, nt + 1, flat), BF16),
        proj=vmem((nk, rows, out_cols), BF16),
        second=vmem((nt, rows, width), F32),
        cut_b=vmem((n, rows, width), BF16),
        cut=vmem((n, rows, width), BF16),
    )
    rounds = dict(
        rows=n, gain=n, slab=n, near=n, bc=n, hist=n, xz=n, mix=nk, state=nt, wout=nt, tap=nt, proj=n, cut=n
    )
    sems = {name: (dma((count,)), dma((count,))) for name, count in rounds.items()}
    sems["load"] = dma((17,))
    sems["lead"] = dma((4,))

    def kernel(*refs, **held):
        def body(**flags):
            layer_kernel(nk, nt, *refs, SimpleNamespace(**held), SimpleNamespace(**flags))

        pl.run_scoped(body, **sems)

    return pl.pallas_call(
        kernel,
        out_shape=pltpu.VMEM(resid.shape, resid.dtype),
        in_specs=[pl.BlockSpec(memory_space=pl.ANY)] * len(args),
        out_specs=pl.BlockSpec(memory_space=pltpu.VMEM),
        scratch_shapes=scratch,
        compiler_params=pltpu.CompilerParams(
            collective_id=0, has_side_effects=True, vmem_limit_bytes=60 * 1024 * 1024
        ),
    )(*args)


def fits(nk, nt, resid, w_x, w_bc, conv_x):
    rows, width = resid.shape
    half = conv_x.shape[3]
    pairs = w_bc.shape[1] * w_bc.shape[2]
    return (
        conv_x.shape[0] == 1
        and rows == nk
        and nt > 1
        and nk & (nk - 1) == 0
        and w_bc.shape[0] == nt * width
        and width % 128 == 0
        and (nk * nt * width) % 256 == 0
        and (conv_x.shape[2] * conv_x.shape[3]) % 256 == 0
        and w_bc.shape[0] % 128 == 0
        and (w_x.shape[1] * w_x.shape[2]) % 128 == 0
        and half & (half - 1) == 0
        and pairs & (pairs - 1) == 0
        and pairs % 8 == 0
        and 256 % pairs == 0
        and (w_bc.shape[0] * pairs) % 256 == 0
        and w_bc.shape[3] == 128
        and conv_x.shape[2] < 128
    )


def solution(mesh):
    placed = (
        P("dp", ("kv", "tp")),
        P(None, ("kv", "tp")),
        P(None, None, ("kv", "tp")),
        P(None, None, ("kv", "tp")),
        P(None, ("kv", "tp"), None),
        P(None, "kv", "tp"),
        P(None, "kv", "tp"),
        P("kv", None, None, None),
        P("kv", None),
        P(),
        P(),
        P(),
        P(None, None, "tp"),
        P(),
        P(("dp", "kv"), None, None, "tp"),
        P(("dp", "kv"), None, None, None, None),
        P(("dp", "kv"), None, "tp", None),
        P(None, "tp", "kv"),
    )
    nk, nt = mesh.shape["kv"], mesh.shape["tp"]

    def layer(*args):
        if fits(nk, nt, args[0], args[5], args[7], args[14]):
            return fused_layer(nk, nt, *args)
        return per_device(*args)

    return jax.shard_map(
        layer, mesh=mesh, in_specs=placed, out_specs=P("dp", ("kv", "tp")), check_vma=False
    )
```

```python
from types import SimpleNamespace

import jax
import jax.numpy as jnp
from jax import lax
from jax.experimental import pallas as pl
from jax.experimental.pallas import tpu as pltpu
from jax.sharding import PartitionSpec as P

D = 2048
F32 = jnp.float32
BF16 = jnp.bfloat16
MESH = pl.DeviceIdType.MESH

EPS = 1e-06


def normalize(rows, gain):
    values = rows.astype(jnp.float32)
    scale = lax.rsqrt(jnp.mean(values * values, axis=1, keepdims=True) + EPS)
    return (values * scale * gain.astype(jnp.float32).reshape(1, -1)).astype(jnp.bfloat16)


def feed_forward(normed, w_gate, w_up, w_down):
    gate = jnp.dot(normed, w_gate, preferred_element_type=jnp.float32)
    upper = jnp.dot(normed, w_up, preferred_element_type=jnp.float32)
    hidden = (jax.nn.silu(gate) * upper).astype(jnp.bfloat16)
    return jnp.dot(hidden, w_down, preferred_element_type=jnp.float32)


def add_half(base, sums):
    return (base.astype(jnp.float32) + 0.5 * sums).astype(jnp.bfloat16)


def ffn_totals(partial_value):
    return lax.psum(partial_value, ("kv", "tp"))


def short_conv(history, newest, taps):
    window = jnp.concatenate(
        [history.astype(jnp.float32), newest.astype(jnp.float32)[:, None]], axis=1
    )
    return jax.nn.silu(jnp.sum(window * taps.astype(jnp.float32)[None], axis=1))


def state_step(
    xs_new,
    zeta,
    bc_new,
    dt_raw,
    conv_x,
    conv_bc,
    ssm_state,
    conv_wx,
    conv_wbc,
    dt_bias,
    a_log,
    d_skip,
):
    xconv = short_conv(conv_x, xs_new, conv_wx)
    bconv = short_conv(conv_bc, bc_new, conv_wbc)
    heads = xconv.shape[1]
    groups = bconv.shape[2]
    bmat = jnp.repeat(bconv[:, 0], heads // groups, axis=1)
    cmat = jnp.repeat(bconv[:, 1], heads // groups, axis=1)
    step_size = jax.nn.softplus(dt_raw + dt_bias[None, :])
    decay = jnp.exp(-step_size * jnp.exp(a_log)[None, :])
    updated = (
        decay[:, :, None, None] * ssm_state
        + (step_size[:, :, None] * xconv)[..., None] * bmat[:, :, None, :]
    )
    mixed = (
        jnp.einsum("shpn,shn->shp", updated, cmat, precision=lax.Precision.HIGHEST)
        + d_skip[None, :, None] * xconv
    )
    return (mixed * jax.nn.silu(zeta.astype(jnp.float32))).astype(jnp.bfloat16)


def group_terms(slab, w_bc, w_dt):
    span = slab.shape[1]
    flat_bc = w_bc.reshape(span, -1)
    bc_part = jnp.dot(slab, flat_bc, preferred_element_type=jnp.float32)
    dt_part = jnp.dot(slab, w_dt, preferred_element_type=jnp.float32)
    return (
        lax.psum_scatter(bc_part, "kv", scatter_dimension=0, tiled=True),
        lax.psum_scatter(dt_part, "kv", scatter_dimension=0, tiled=True),
    )


def mix_partial(
    normed,
    w_x,
    w_z,
    w_bc,
    w_dt,
    dt_bias,
    a_log,
    d_skip,
    conv_wx,
    conv_wbc,
    conv_x,
    conv_bc,
    ssm_state,
    w_out,
):
    rows = normed.shape[0]
    local_heads = w_x.shape[1]
    half = w_x.shape[2]
    xs_part = (
        jnp.dot(normed, w_x.reshape(D, -1), preferred_element_type=jnp.float32)
        .astype(jnp.bfloat16)
        .reshape(rows, local_heads, half)
    )
    zeta_part = (
        jnp.dot(normed, w_z.reshape(D, -1), preferred_element_type=jnp.float32)
        .astype(jnp.bfloat16)
        .reshape(rows, local_heads, half)
    )
    xs_new, zeta = (
        lax.all_to_all(xs_part, "kv", split_axis=0, concat_axis=1, tiled=True),
        lax.all_to_all(zeta_part, "kv", split_axis=0, concat_axis=1, tiled=True),
    )
    span = w_bc.shape[0]
    slab = lax.dynamic_slice_in_dim(normed, lax.axis_index("kv") * span, span, 1)
    bc_sum, dt_raw = group_terms(slab, w_bc, w_dt)
    bc_new = bc_sum.astype(jnp.bfloat16).reshape((bc_sum.shape[0],) + w_bc.shape[1:])
    mixed = state_step(
        xs_new,
        zeta,
        bc_new,
        dt_raw,
        conv_x,
        conv_bc,
        ssm_state,
        conv_wx,
        conv_wbc,
        dt_bias,
        a_log,
        d_skip,
    )
    flat_out = w_out.reshape(-1, w_out.shape[2])
    piece = lax.all_gather(mixed, "kv", axis=0, tiled=True)
    return jnp.dot(piece.reshape(piece.shape[0], -1), flat_out, preferred_element_type=jnp.float32)


def per_device(
    resid,
    norm_gain,
    ffn_gate,
    ffn_up,
    ffn_down,
    w_x,
    w_z,
    w_bc,
    w_dt,
    dt_bias,
    a_log,
    d_skip,
    conv_wx,
    conv_wbc,
    conv_x,
    conv_bc,
    ssm_state,
    w_out,
):
    mixer_args = (
        w_x,
        w_z,
        w_bc,
        w_dt,
        dt_bias,
        a_log,
        d_skip,
        conv_wx,
        conv_wbc,
        conv_x,
        conv_bc,
        ssm_state,
        w_out,
    )
    rows, gains = (
        lax.all_gather(resid, ("kv", "tp"), axis=1, tiled=True),
        lax.all_gather(norm_gain, ("kv", "tp"), axis=1, tiled=True),
    )
    first = add_half(
        rows,
        ffn_totals(feed_forward(normalize(rows, gains[0]), ffn_gate[0], ffn_up[0], ffn_down[0])),
    )
    partial_value = mix_partial(normalize(first, gains[1]), *mixer_args)
    span = partial_value.shape[1]
    block = lax.dynamic_slice_in_dim(first, lax.axis_index("kv") * span, span, 1)
    joined = (block.astype(jnp.float32) + lax.psum(partial_value, "tp")).astype(jnp.bfloat16)
    second = lax.all_gather(joined, "kv", axis=1, tiled=True)
    final = add_half(
        second,
        ffn_totals(feed_forward(normalize(second, gains[2]), ffn_gate[1], ffn_up[1], ffn_down[1])),
    )
    width = resid.shape[1]
    return lax.dynamic_slice_in_dim(final, lax.axis_index(("kv", "tp")) * width, width, 1)


def nt_dot(left, right):
    return lax.dot_general(left, right, (((1,), (1,)), ((), ())), preferred_element_type=F32)


def nn_dot(left, right):
    return jnp.dot(left, right, preferred_element_type=F32)


def silu(value):
    return value * jax.nn.sigmoid(value)


def norm_rows(values, gain):
    scale = lax.rsqrt(jnp.mean(values * values, axis=1, keepdims=True) + EPS)
    return (values * scale * gain).astype(BF16)


def split_two(value):
    high = value.astype(BF16)
    return high, (value - high.astype(F32)).astype(BF16)


def layer_kernel(
    nk,
    nt,
    resid,
    gains,
    gate,
    up,
    down,
    wx,
    wz,
    wbc,
    wdt,
    dt_bias,
    a_log,
    d_skip,
    cwx,
    cwbc,
    cx,
    cbc,
    state,
    wout,
    out,
    v,
    m,
):
    me_k, me_t = lax.axis_index("kv"), lax.axis_index("tp")
    n = nk * nt
    me = me_k * nt + me_t
    lead = nt - 1
    rows, width = resid.shape
    dim = n * width
    block = nt * width
    scope = jax.named_scope

    def target(index):
        return {"kv": lax.div(index, nt), "tp": lax.rem(index, nt)}

    def flipped(index, mask):
        bit = 1
        while bit < nk:
            if mask & bit:
                index = index + bit - 2 * bit * lax.rem(lax.div(index, bit), 2)
            bit *= 2
        return index

    def all_peers():
        order = [(x, d) for x in range(nk) for d in range(nt)][1:]
        return [flipped(me_k, x) * nt + lax.rem(me_t + d, nt) for x, d in order]

    def far_first():
        far = [flipped(me_k, x) * nt + t for x in range(1, nk)[::-1] for t in range(nt)]
        return far + [me_k * nt + lax.rem(me_t + d, nt) for d in range(1, nt)]

    def kv_peers():
        return [flipped(me_k, x) for x in range(1, nk)]

    loads = {}

    def load(name, src, dst):
        copy = pltpu.make_async_copy(src, dst, m.load.at[len(loads)])
        copy.start()
        loads[name] = copy

    def loaded(*names):
        with scope("w_" + names[0]):
            for name in names:
                loads[name].wait()

    load("rows", resid, v.rows.at[me])
    load("gains", gains, v.gain.at[me])
    barrier = pltpu.get_barrier_semaphore()
    for q in far_first():
        pl.semaphore_signal(barrier, inc=1, device_id=target(q), device_id_type=MESH)
    load("bias", dt_bias, v.small.at[0])
    load("alog", a_log, v.small.at[1])
    load("skip", d_skip, v.small.at[2])
    load("cwx", cwx, v.cwx)
    load("cwbc", cwbc, v.cwbc)
    load("cx", cx, v.cx)
    load("cbc", cbc, v.cbc)
    load("gate0", gate.at[0], v.gate.at[0])
    load("up0", up.at[0], v.up.at[0])
    load("down0", down.at[0], v.down.at[0])
    lead_loads = (
        (wbc, v.wbc),
        (wdt, v.wdt),
        (state, v.state.at[lead]),
        (wout, v.wout.at[lead]),
    )

    def lead_load(i):
        return pltpu.make_async_copy(*lead_loads[i], m.lead.at[i])

    @pl.when(me_t == lead)
    def _():
        for i in range(3):
            lead_load(i).start()

    load("wx", wx, v.wx)
    load("wz", wz, v.wz)

    @pl.when(me_t == lead)
    def _():
        lead_load(3).start()

    load("gate1", gate.at[1], v.gate.at[1])
    load("up1", up.at[1], v.up.at[1])
    load("down1", down.at[1], v.down.at[1])
    with scope("w_barrier"):
        pl.semaphore_wait(barrier, n - 1)

    def remote(src, dst, ssem, rsem, index):
        return pltpu.make_async_remote_copy(
            src_ref=src,
            dst_ref=dst,
            send_sem=ssem,
            recv_sem=rsem,
            device_id=target(index),
            device_id_type=MESH,
        )

    sent = []

    def send(src, dst, ssem, rsem, index):
        copy = remote(src, dst, ssem, rsem, index)
        copy.start()
        sent.append(copy)

    def arrived(slots, sems, slot, index):
        remote(slots.at[slot], slots.at[slot], sems[0].at[slot], sems[1].at[slot], index).wait_recv()

    loaded("rows", "gains")
    for q in far_first():
        send(v.rows.at[me], v.rows.at[me], m.rows[0].at[q], m.rows[1].at[me], q)
        send(v.gain.at[me], v.gain.at[me], m.gain[0].at[q], m.gain[1].at[me], q)

    home = me_k * nt + lead

    def pushes():
        yield remote(state, v.state.at[me_t], m.state[0].at[me_t], m.state[1].at[me_t], home)
        yield remote(wout, v.wout.at[me_t], m.wout[0].at[me_t], m.wout[1].at[me_t], home)

    @pl.when(me_t != lead)
    def _():
        for copy in pushes():
            copy.start()

    heads, half = v.cx.shape[2], v.cx.shape[1]
    flat = heads * half
    groups = v.cwbc.shape[1] // 2
    pairs = 2 * groups
    lane = lax.broadcasted_iota(jnp.int32, v.expand.shape, 1)
    head_of = lax.broadcasted_iota(jnp.int32, v.expand.shape, 0) * half
    v.expand[...] = jnp.where((lane >= head_of) & (lane < head_of + half), 1.0, 0.0).astype(BF16)
    tile = v.perm.shape[0]
    deep = tile // pairs
    row = lax.broadcasted_iota(jnp.int32, v.perm.shape, 0)
    lane = lax.broadcasted_iota(jnp.int32, v.perm.shape, 1)
    source = (row & (deep - 1)) * pairs + lax.shift_right_logical(row, deep.bit_length() - 1)
    v.perm[...] = jnp.where(lane == source, 1.0, 0.0).astype(BF16)

    def expand(value):
        return nn_dot(value, v.expand[...])

    loaded("bias", "alog", "skip", "cwx", "cwbc", "cx", "cbc")
    taps = v.cx.shape[0]
    known = sum(v.cx[i].astype(F32) * v.cwx[i].astype(F32) for i in range(taps))
    high, low = split_two(known)
    lane = lax.broadcasted_iota(jnp.int32, (half, flat), 1)
    row = lax.broadcasted_iota(jnp.int32, (half, flat), 0)
    own = (lane & (half - 1)) == row
    v.hist[me_k, me_t] = jnp.sum(
        jnp.where(own, expand(high) + expand(low), 0.0), axis=0, keepdims=True
    )
    v.tap[me_t] = jnp.sum(jnp.where(own, expand(v.cwx[taps]), 0.0), axis=0, keepdims=True)

    def to_leads(ref, sems):
        for k in kv_peers()[::-1]:
            q = k * nt + lead
            yield remote(ref.at[me_k, me_t], ref.at[me_k, me_t], sems[0].at[k], sems[1].at[me], q)

    def to_home(ref, sems):
        return remote(
            ref.at[me_k, me_t], ref.at[me_k, me_t], sems[0].at[me_k], sems[1].at[me], home
        )

    def tap_home():
        return remote(v.tap.at[me_t], v.tap.at[me_t], m.tap[0].at[me_t], m.tap[1].at[me_t], home)

    for copy in to_leads(v.hist, m.hist):
        copy.start()
        sent.append(copy)

    @pl.when(me_t != lead)
    def _():
        to_home(v.hist, m.hist).start()
        tap_home().start()

    hist_bc = sum(v.cbc[i].astype(F32) * v.cwbc[i].astype(F32) for i in range(taps))
    tap_bc = v.cwbc[taps].astype(F32)

    units = v.gate.shape[1]

    def gated(blocks, kept):
        squares = jnp.zeros((rows, 1), F32)
        g = jnp.zeros((rows, units), F32)
        u = jnp.zeros((rows, units), F32)
        for step, (values, gain, at) in enumerate(blocks):
            squares = squares + jnp.sum(values * values, axis=1, keepdims=True)
            left = (values * gain).astype(BF16)
            g = g + nn_dot(left, v.gate_t[at, :])
            u = u + nn_dot(left, v.up_t[at, :])
            if step < kept:
                v.held[step, 0] = g
                v.held[step, 1] = u
                g = jnp.zeros((rows, units), F32)
                u = jnp.zeros((rows, units), F32)
        for step in range(kept):
            g = g + v.held[step, 0]
            u = u + v.held[step, 1]
        scale = lax.rsqrt(squares / dim + EPS)
        return (silu(g * scale) * (u * scale)).astype(BF16)

    def turn(source, dest):
        for k in range(dim // 256):
            at = slice(k * 256, (k + 1) * 256)
            dest[at, :] = source[:, at].T

    def turn_ffn(which):
        loaded(f"gate{which}", f"up{which}")
        turn(v.gate.at[which], v.gate_t)
        turn(v.up.at[which], v.up_t)

    def columns(index, count):
        return pl.ds(pl.multiple_of(index * count, 128), count)

    def by_arrival():
        order = [lead - d for d in range(nt)]
        near = [me_k * nt + lax.rem(me_t + d, nt) for d in range(1, nt)]
        return near + [flipped(me_k, x) * nt + t for x in range(1, nk) for t in order]

    def arriving_rows():
        for q in [me] + by_arrival():
            if q is not me:
                with scope("w_rows"):
                    arrived(v.rows, m.rows, q, q)
                    arrived(v.gain, m.gain, q, q)
            yield v.rows[q].astype(F32), v.gain[q, 0:1, :].astype(F32), columns(q, width)

    turn_ffn(0)
    hidden = gated(arriving_rows(), 0)
    loaded("down0")
    for x in range(nk)[::-1]:
        k = flipped(me_k, x)
        v.part[k] = nn_dot(hidden, v.down[0, :, columns(k, block)]).astype(BF16)
        q = k * nt + lead
        if x:
            send(v.part.at[k], v.slab.at[me], m.slab[0].at[q], m.slab[1].at[me], q)

    def slab_home():
        q = me_k * nt + lead
        return remote(v.part.at[me_k], v.slab.at[me], m.slab[0].at[q], m.slab[1].at[me], q)

    @pl.when(me_t != lead)
    def _():
        slab_home().start()

    def gain_cut(index, i):
        return jnp.concatenate(
            [v.gain[index * nt + t, i : i + 1, :].astype(F32) for t in range(nt)], axis=1
        )

    def rows_cut(index):
        return jnp.concatenate([v.rows[index * nt + t].astype(F32) for t in range(nt)], axis=1)

    tall = v.bc.shape[1]

    def bc_row(k):
        return v.bc_b.at[pl.ds(pl.multiple_of(k * tall, 8), tall), :]

    def first_sends():
        for q in far_first():
            yield remote(v.near.at[me_k], v.near.at[me_k], m.near[0].at[q], m.near[1].at[me_k], q)

    def bc_sends():
        for k in kv_peers()[::-1]:
            q = k * nt + lead
            yield remote(bc_row(k), v.bc.at[me_k], m.bc[0].at[k], m.bc[1].at[me_k], q)

    @pl.when(me_t == lead)
    def _():
        with scope("w_wbc"):
            lead_load(0).wait()
            lead_load(1).wait()
        span = v.wdt.shape[1]
        for c in range(span // deep):
            piece = nn_dot(v.perm[...], v.wbc[c * tile : (c + 1) * tile, :]).astype(BF16)
            for p in range(pairs):
                v.wide[c * deep : (c + 1) * deep, p * 128 : (p + 1) * 128] = piece[
                    p * deep : (p + 1) * deep, :
                ]
        with scope("w_state"):
            lead_load(2).wait()
            for t in range(lead):
                arrived(v.state, m.state, t, me_k * nt + t)
        for t in range(nt):
            for i in range(flat // 256):
                at = slice(i * 256, (i + 1) * 256)
                v.state_b[t, :, at] = v.state[t, at, :].astype(BF16).T
        v.slab[me] = v.part[me_k]
        with scope("w_slab"):
            for q in all_peers():
                arrived(v.slab, m.slab, q, q)
        total = sum(v.slab[q].astype(F32) for q in range(n))
        first = (rows_cut(me_k) + 0.5 * total).astype(BF16)
        v.near[me_k] = first
        for copy in first_sends():
            copy.start()
        left = (first.astype(F32) * gain_cut(me_k, 1)).astype(BF16)
        bc_part = nn_dot(left, v.wide[...])
        dt_part = nt_dot(left, v.wdt[...])
        for p in range(pairs):
            v.bc_b[pl.ds(p, rows, stride=tall), :] = bc_part[:, p * 128 : (p + 1) * 128]
        v.bc_b[pl.ds(pairs, rows, stride=tall), :] = jnp.concatenate(
            [dt_part, jnp.zeros((rows, 128 - heads), F32)], axis=1
        )
        for copy in bc_sends():
            copy.start()
        v.bc[me_k] = bc_row(me_k)[...]

    def arrived_at(slots, sems, k, t):
        q = k * nt + t
        remote(slots.at[k, t], slots.at[k, t], sems[0].at[k], sems[1].at[q], q).wait_recv()

    def arrived_from_lead(slots, sems, k):
        @pl.when(k * nt + lead != me)
        def _():
            arrived(slots, sems, k, k * nt + lead)

    loaded("wx", "wz")
    turn(v.wx, v.wx_t)
    turn(v.wz, v.wz_t)
    local = v.wx.shape[0]
    xs_part = jnp.zeros((rows, local), F32)
    z_part = jnp.zeros((rows, local), F32)
    squares = jnp.zeros((rows, 1), F32)
    for x in range(nk):
        k = flipped(me_k, x)
        with scope("w_near"):
            if x:
                arrived(v.near, m.near, k, k * nt + lead)
            else:
                arrived_from_lead(v.near, m.near, k)
        first = v.near[k].astype(F32)
        v.first[k] = first
        left = (first * gain_cut(k, 1)).astype(BF16)
        squares = squares + jnp.sum(first * first, axis=1, keepdims=True)
        xs_part = xs_part + nn_dot(left, v.wx_t[columns(k, block), :])
        z_part = z_part + nn_dot(left, v.wz_t[columns(k, block), :])
    scale = lax.rsqrt(squares / dim + EPS)
    v.scale[...] = jnp.broadcast_to(scale, v.scale.shape)
    v.xz[me_k, me_t] = jnp.concatenate([xs_part * scale, z_part * scale], axis=1).astype(BF16)
    for copy in to_leads(v.xz, m.xz):
        copy.start()
        sent.append(copy)

    @pl.when(me_t != lead)
    def _():
        to_home(v.xz, m.xz).start()
        turn_ffn(1)

    def proj_sends():
        for q in far_first():
            yield remote(v.proj.at[me_k], v.proj.at[me_k], m.proj[0].at[q], m.proj[1].at[me_k], q)

    @pl.when(me_t == lead)
    def _():
        with scope("w_bc"):
            for k in kv_peers():
                arrived(v.bc, m.bc, k, k * nt + lead)
        summed = sum(v.bc[k] for k in range(nk)) * v.scale[pl.ds(me_k, 1), :]
        raw = summed[pairs : pairs + 1, :heads] + v.small[0]
        step = jnp.maximum(raw, 0.0) + jnp.log1p(jnp.exp(-jnp.abs(raw)))
        decay = jnp.exp(-step * jnp.exp(v.small[1]))
        bc_new = summed[:pairs].astype(BF16).astype(F32)
        bconv = silu(hist_bc + bc_new * tap_bc)
        bmat, cmat = bconv[:groups], bconv[groups:]
        weight = jnp.sum(bmat * cmat, axis=1, keepdims=True)
        lane = lax.broadcasted_iota(jnp.int32, (groups, heads), 1)
        low_end = lax.broadcasted_iota(jnp.int32, (groups, heads), 0) * (heads // groups)
        mine = (lane >= low_end) & (lane < low_end + heads // groups)
        cross = jnp.sum(jnp.where(mine, weight, 0.0), axis=0, keepdims=True)
        v.coef[me_k] = step * cross + v.small[2]

        def coef_sends():
            for k in kv_peers()[::-1]:
                q = k * nt + lead
                yield remote(
                    v.coef.at[me_k], v.coef.at[me_k], m.coef[0].at[k], m.coef[1].at[me_k], q
                )

        for copy in coef_sends():
            copy.start()
        decay_high, decay_low = split_two(decay)
        spread = expand(jnp.concatenate([decay_high, decay_low], axis=0))
        decay_row = spread[0:1] + spread[1:2]
        lane = lax.broadcasted_iota(jnp.int32, (groups, flat), 1)
        low_end = lax.broadcasted_iota(jnp.int32, (groups, flat), 0) * (flat // groups)
        mine = (lane >= low_end) & (lane < low_end + flat // groups)
        lines = []
        for t in range(nt):
            per_group = nn_dot(cmat.astype(BF16), v.state_b[t])
            read = jnp.sum(jnp.where(mine, per_group, 0.0), axis=0, keepdims=True)
            lines.append(decay_row * read)
        v.mix[me_k] = jnp.concatenate(lines, axis=0).astype(BF16)

        def mix_sends():
            for k in kv_peers()[::-1]:
                q = k * nt + lead
                yield remote(v.mix.at[me_k], v.mix.at[me_k], m.mix[0].at[k], m.mix[1].at[me_k], q)

        for copy in mix_sends():
            copy.start()
        turn_ffn(1)
        with scope("w_hist"):
            for t in range(lead):
                arrived(v.tap, m.tap, t, me_k * nt + t)
                arrived_at(v.hist, m.hist, me_k, t)
            for k in kv_peers():
                for t in range(nt):
                    arrived_at(v.hist, m.hist, k, t)
        with scope("w_wout"):
            lead_load(3).wait()
            for t in range(lead):
                arrived(v.wout, m.wout, t, me_k * nt + t)
        for t in range(nt):
            v.past[t] = jnp.concatenate([v.hist[i, t] for i in range(nk)], axis=0)
        with scope("w_coef"):
            for k in kv_peers():
                arrived(v.coef, m.coef, k, k * nt + lead)
        high, low = split_two(jnp.concatenate([v.coef[i] for i in range(nk)], axis=0))
        spread = expand(jnp.concatenate([high, low], axis=0))
        v.direct[...] = spread[:nk] + spread[nk:]
        with scope("w_mix"):
            for k in kv_peers():
                arrived(v.mix, m.mix, k, k * nt + lead)
        total = jnp.zeros((rows, v.wout.shape[2]), F32)
        for x in range(nk):
            k = flipped(me_k, x)
            at = columns(k, local)
            with scope("w_xz"):
                for t in range(nt)[::-1]:
                    if x or t != lead:
                        arrived_at(v.xz, m.xz, k, t)
            direct = v.direct[:, at]
            for t in range(nt):
                read = jnp.concatenate(
                    [v.mix[i, t : t + 1, at].astype(F32) for i in range(nk)], axis=0
                )
                xs_new = v.xz[k, t, :, :local].astype(F32)
                xconv = silu(v.past[t, :, at] + xs_new * v.tap[t, :, at])
                opened = silu(v.xz[k, t, :, local:].astype(F32))
                mixed = ((read + direct * xconv) * opened).astype(BF16)
                total = total + nn_dot(mixed, v.wout[t, at, :])
        v.proj[me_k] = total.astype(BF16)
        for copy in proj_sends():
            copy.start()
        for copy in mix_sends():
            copy.wait_send()
        for copy in coef_sends():
            copy.wait_send()

    def arriving_blocks():
        for x in range(nk):
            k = flipped(me_k, x)
            with scope("w_proj"):
                if x:
                    arrived(v.proj, m.proj, k, k * nt + lead)
                else:
                    arrived_from_lead(v.proj, m.proj, k)
            second = (v.first[k] + v.proj[k].astype(F32)).astype(BF16).astype(F32)
            if x == 0:
                for t in range(nt):
                    v.second[t] = second[:, t * width : (t + 1) * width]
            yield second, gain_cut(k, 2), columns(k, block)

    hidden = gated(arriving_blocks(), nk - 1)
    loaded("down1")
    for x in range(nk)[::-1]:
        k = flipped(me_k, x)
        piece = nn_dot(hidden, v.down[1, :, columns(k, block)])
        for t in range(nt):
            v.cut_b[k * nt + t] = piece[:, t * width : (t + 1) * width].astype(BF16)
        for d in range(nt):
            if x or d:
                q = k * nt + (d if x else lax.rem(me_t + d, nt))
                send(v.cut_b.at[q], v.cut.at[me], m.cut[0].at[q], m.cut[1].at[me], q)
    v.cut[me] = v.cut_b[me]
    with scope("w_sent"):
        for copy in sent[:-(n - 1)]:
            copy.wait_send()

        @pl.when(me_t == lead)
        def _():
            for copy in first_sends():
                copy.wait_send()
            for copy in bc_sends():
                copy.wait_send()
            for copy in proj_sends():
                copy.wait_send()

        @pl.when(me_t != lead)
        def _():
            slab_home().wait_send()
            to_home(v.hist, m.hist).wait_send()
            to_home(v.xz, m.xz).wait_send()
            tap_home().wait_send()
            for copy in pushes():
                copy.wait_send()
    with scope("w_cut"):
        for q in all_peers():
            arrived(v.cut, m.cut, q, q)
    total = sum(v.cut[q].astype(F32) for q in range(n))
    out[...] = (v.second[me_t] + 0.5 * total).astype(BF16)
    for copy in sent[-(n - 1) :]:
        copy.wait_send()


def fused_layer(
    nk,
    nt,
    resid,
    norm_gain,
    ffn_gate,
    ffn_up,
    ffn_down,
    w_x,
    w_z,
    w_bc,
    w_dt,
    dt_bias,
    a_log,
    d_skip,
    conv_wx,
    conv_wbc,
    conv_x,
    conv_bc,
    ssm_state,
    w_out,
):
    n = nk * nt
    rows, width = resid.shape
    dim = ffn_gate.shape[1]
    units = ffn_gate.shape[2]
    local = w_x.shape[1] * w_x.shape[2]
    heads, half = conv_x.shape[2], conv_x.shape[3]
    flat = heads * half
    span = w_bc.shape[0]
    lanes = w_bc.shape[3]
    pairs = w_bc.shape[1] * w_bc.shape[2]
    out_cols = w_out.shape[2]
    taps = conv_wx.shape[0]
    block = nt * width
    args = (
        resid,
        norm_gain,
        jnp.swapaxes(ffn_gate, 1, 2),
        jnp.swapaxes(ffn_up, 1, 2),
        ffn_down,
        jnp.transpose(w_x, (1, 2, 0)).reshape(local, dim),
        jnp.transpose(w_z, (1, 2, 0)).reshape(local, dim),
        w_bc.reshape(span * pairs, lanes),
        w_dt.T,
        dt_bias.reshape(1, heads),
        a_log.reshape(1, heads),
        d_skip.reshape(1, heads),
        jnp.swapaxes(conv_wx, 1, 2),
        conv_wbc.reshape(taps, pairs, lanes),
        jnp.swapaxes(conv_x, 2, 3).reshape(taps - 1, half, heads),
        conv_bc.reshape(taps - 1, pairs, lanes),
        ssm_state.reshape(flat, lanes),
        w_out.reshape(flat, out_cols),
    )
    dma = pltpu.SemaphoreType.DMA
    vmem = pltpu.VMEM
    scratch = dict(
        gate=vmem((2, units, dim), BF16),
        up=vmem((2, units, dim), BF16),
        down=vmem((2, units, dim), BF16),
        gate_t=vmem((dim, units), BF16),
        up_t=vmem((dim, units), BF16),
        wx_t=vmem((dim, local), BF16),
        wz_t=vmem((dim, local), BF16),
        wx=vmem((local, dim), BF16),
        wz=vmem((local, dim), BF16),
        wbc=vmem((span * pairs, lanes), BF16),
        wide=vmem((span, pairs * lanes), BF16),
        wdt=vmem((heads, span), BF16),
        state=vmem((nt, flat, lanes), F32),
        state_b=vmem((nt, lanes, flat), BF16),
        wout=vmem((nt, flat, out_cols), BF16),
        small=vmem((3, 1, heads), F32),
        cwx=vmem((taps, half, heads), BF16),
        cwbc=vmem((taps, pairs, lanes), BF16),
        cx=vmem((taps - 1, half, heads), BF16),
        cbc=vmem((taps - 1, pairs, lanes), BF16),
        expand=vmem((heads, flat), BF16),
        perm=vmem((256, 256), BF16),
        rows=vmem((n, rows, width), BF16),
        gain=vmem((n, 3, width), BF16),
        part=vmem((nk, rows, block), BF16),
        slab=vmem((n, rows, block), BF16),
        near=vmem((nk, rows, block), BF16),
        held=vmem((nk - 1, 2, rows, units), F32),
        first=vmem((nk, rows, block), F32),
        scale=vmem((rows, lanes), F32),
        bc_b=vmem((nk * (pairs + 8), lanes), F32),
        bc=vmem((nk, pairs + 8, lanes), F32),
        hist=vmem((nk, nt, 1, flat), F32),
        tap=vmem((nt, 1, flat), F32),
        xz=vmem((nk, nt, rows, 2 * local), BF16),
        past=vmem((nt, rows, flat), F32),
        coef=vmem((nk, 1, heads), F32),
        direct=vmem((nk, flat), F32),
        mix=vmem((nk, nt, flat), BF16),
        proj=vmem((nk, rows, out_cols), BF16),
        second=vmem((nt, rows, width), F32),
        cut_b=vmem((n, rows, width), BF16),
        cut=vmem((n, rows, width), BF16),
    )
    rounds = dict(
        rows=n, gain=n, slab=n, near=n, bc=n, hist=n, xz=n, mix=nk, coef=nk, state=nt, wout=nt, tap=nt, proj=n, cut=n
    )
    sems = {name: (dma((count,)), dma((count,))) for name, count in rounds.items()}
    sems["load"] = dma((17,))
    sems["lead"] = dma((4,))

    def kernel(*refs, **held):
        def body(**flags):
            layer_kernel(nk, nt, *refs, SimpleNamespace(**held), SimpleNamespace(**flags))

        pl.run_scoped(body, **sems)

    return pl.pallas_call(
        kernel,
        out_shape=pltpu.VMEM(resid.shape, resid.dtype),
        in_specs=[pl.BlockSpec(memory_space=pl.ANY)] * len(args),
        out_specs=pl.BlockSpec(memory_space=pltpu.VMEM),
        scratch_shapes=scratch,
        compiler_params=pltpu.CompilerParams(
            collective_id=0, has_side_effects=True, vmem_limit_bytes=60 * 1024 * 1024
        ),
    )(*args)


def fits(nk, nt, resid, w_x, w_bc, conv_x):
    rows, width = resid.shape
    half = conv_x.shape[3]
    pairs = w_bc.shape[1] * w_bc.shape[2]
    return (
        conv_x.shape[0] == 1
        and rows == nk
        and nt > 1
        and nk & (nk - 1) == 0
        and w_bc.shape[0] == nt * width
        and width % 128 == 0
        and (nk * nt * width) % 256 == 0
        and (conv_x.shape[2] * conv_x.shape[3]) % 256 == 0
        and w_bc.shape[0] % 128 == 0
        and (w_x.shape[1] * w_x.shape[2]) % 128 == 0
        and half & (half - 1) == 0
        and pairs & (pairs - 1) == 0
        and pairs % 8 == 0
        and 256 % pairs == 0
        and (w_bc.shape[0] * pairs) % 256 == 0
        and w_bc.shape[3] == 128
        and conv_x.shape[2] < 128
    )


def solution(mesh):
    placed = (
        P("dp", ("kv", "tp")),
        P(None, ("kv", "tp")),
        P(None, None, ("kv", "tp")),
        P(None, None, ("kv", "tp")),
        P(None, ("kv", "tp"), None),
        P(None, "kv", "tp"),
        P(None, "kv", "tp"),
        P("kv", None, None, None),
        P("kv", None),
        P(),
        P(),
        P(),
        P(None, None, "tp"),
        P(),
        P(("dp", "kv"), None, None, "tp"),
        P(("dp", "kv"), None, None, None, None),
        P(("dp", "kv"), None, "tp", None),
        P(None, "tp", "kv"),
    )
    nk, nt = mesh.shape["kv"], mesh.shape["tp"]

    def layer(*args):
        if fits(nk, nt, args[0], args[5], args[7], args[14]):
            return fused_layer(nk, nt, *args)
        return per_device(*args)

    return jax.shard_map(
        layer, mesh=mesh, in_specs=placed, out_specs=P("dp", ("kv", "tp")), check_vma=False
    )
```

```python
from types import SimpleNamespace

import jax
import jax.numpy as jnp
from jax import lax
from jax.experimental import pallas as pl
from jax.experimental.pallas import tpu as pltpu
from jax.sharding import PartitionSpec as P

D = 2048
F32 = jnp.float32
BF16 = jnp.bfloat16
MESH = pl.DeviceIdType.MESH

EPS = 1e-06


def normalize(rows, gain):
    values = rows.astype(jnp.float32)
    scale = lax.rsqrt(jnp.mean(values * values, axis=1, keepdims=True) + EPS)
    return (values * scale * gain.astype(jnp.float32).reshape(1, -1)).astype(jnp.bfloat16)


def feed_forward(normed, w_gate, w_up, w_down):
    gate = jnp.dot(normed, w_gate, preferred_element_type=jnp.float32)
    upper = jnp.dot(normed, w_up, preferred_element_type=jnp.float32)
    hidden = (jax.nn.silu(gate) * upper).astype(jnp.bfloat16)
    return jnp.dot(hidden, w_down, preferred_element_type=jnp.float32)


def add_half(base, sums):
    return (base.astype(jnp.float32) + 0.5 * sums).astype(jnp.bfloat16)


def ffn_totals(partial_value):
    return lax.psum(partial_value, ("kv", "tp"))


def short_conv(history, newest, taps):
    window = jnp.concatenate(
        [history.astype(jnp.float32), newest.astype(jnp.float32)[:, None]], axis=1
    )
    return jax.nn.silu(jnp.sum(window * taps.astype(jnp.float32)[None], axis=1))


def state_step(
    xs_new,
    zeta,
    bc_new,
    dt_raw,
    conv_x,
    conv_bc,
    ssm_state,
    conv_wx,
    conv_wbc,
    dt_bias,
    a_log,
    d_skip,
):
    xconv = short_conv(conv_x, xs_new, conv_wx)
    bconv = short_conv(conv_bc, bc_new, conv_wbc)
    heads = xconv.shape[1]
    groups = bconv.shape[2]
    bmat = jnp.repeat(bconv[:, 0], heads // groups, axis=1)
    cmat = jnp.repeat(bconv[:, 1], heads // groups, axis=1)
    step_size = jax.nn.softplus(dt_raw + dt_bias[None, :])
    decay = jnp.exp(-step_size * jnp.exp(a_log)[None, :])
    updated = (
        decay[:, :, None, None] * ssm_state
        + (step_size[:, :, None] * xconv)[..., None] * bmat[:, :, None, :]
    )
    mixed = (
        jnp.einsum("shpn,shn->shp", updated, cmat, precision=lax.Precision.HIGHEST)
        + d_skip[None, :, None] * xconv
    )
    return (mixed * jax.nn.silu(zeta.astype(jnp.float32))).astype(jnp.bfloat16)


def group_terms(slab, w_bc, w_dt):
    span = slab.shape[1]
    flat_bc = w_bc.reshape(span, -1)
    bc_part = jnp.dot(slab, flat_bc, preferred_element_type=jnp.float32)
    dt_part = jnp.dot(slab, w_dt, preferred_element_type=jnp.float32)
    return (
        lax.psum_scatter(bc_part, "kv", scatter_dimension=0, tiled=True),
        lax.psum_scatter(dt_part, "kv", scatter_dimension=0, tiled=True),
    )


def mix_partial(
    normed,
    w_x,
    w_z,
    w_bc,
    w_dt,
    dt_bias,
    a_log,
    d_skip,
    conv_wx,
    conv_wbc,
    conv_x,
    conv_bc,
    ssm_state,
    w_out,
):
    rows = normed.shape[0]
    local_heads = w_x.shape[1]
    half = w_x.shape[2]
    xs_part = (
        jnp.dot(normed, w_x.reshape(D, -1), preferred_element_type=jnp.float32)
        .astype(jnp.bfloat16)
        .reshape(rows, local_heads, half)
    )
    zeta_part = (
        jnp.dot(normed, w_z.reshape(D, -1), preferred_element_type=jnp.float32)
        .astype(jnp.bfloat16)
        .reshape(rows, local_heads, half)
    )
    xs_new, zeta = (
        lax.all_to_all(xs_part, "kv", split_axis=0, concat_axis=1, tiled=True),
        lax.all_to_all(zeta_part, "kv", split_axis=0, concat_axis=1, tiled=True),
    )
    span = w_bc.shape[0]
    slab = lax.dynamic_slice_in_dim(normed, lax.axis_index("kv") * span, span, 1)
    bc_sum, dt_raw = group_terms(slab, w_bc, w_dt)
    bc_new = bc_sum.astype(jnp.bfloat16).reshape((bc_sum.shape[0],) + w_bc.shape[1:])
    mixed = state_step(
        xs_new,
        zeta,
        bc_new,
        dt_raw,
        conv_x,
        conv_bc,
        ssm_state,
        conv_wx,
        conv_wbc,
        dt_bias,
        a_log,
        d_skip,
    )
    flat_out = w_out.reshape(-1, w_out.shape[2])
    piece = lax.all_gather(mixed, "kv", axis=0, tiled=True)
    return jnp.dot(piece.reshape(piece.shape[0], -1), flat_out, preferred_element_type=jnp.float32)


def per_device(
    resid,
    norm_gain,
    ffn_gate,
    ffn_up,
    ffn_down,
    w_x,
    w_z,
    w_bc,
    w_dt,
    dt_bias,
    a_log,
    d_skip,
    conv_wx,
    conv_wbc,
    conv_x,
    conv_bc,
    ssm_state,
    w_out,
):
    mixer_args = (
        w_x,
        w_z,
        w_bc,
        w_dt,
        dt_bias,
        a_log,
        d_skip,
        conv_wx,
        conv_wbc,
        conv_x,
        conv_bc,
        ssm_state,
        w_out,
    )
    rows, gains = (
        lax.all_gather(resid, ("kv", "tp"), axis=1, tiled=True),
        lax.all_gather(norm_gain, ("kv", "tp"), axis=1, tiled=True),
    )
    first = add_half(
        rows,
        ffn_totals(feed_forward(normalize(rows, gains[0]), ffn_gate[0], ffn_up[0], ffn_down[0])),
    )
    partial_value = mix_partial(normalize(first, gains[1]), *mixer_args)
    span = partial_value.shape[1]
    block = lax.dynamic_slice_in_dim(first, lax.axis_index("kv") * span, span, 1)
    joined = (block.astype(jnp.float32) + lax.psum(partial_value, "tp")).astype(jnp.bfloat16)
    second = lax.all_gather(joined, "kv", axis=1, tiled=True)
    final = add_half(
        second,
        ffn_totals(feed_forward(normalize(second, gains[2]), ffn_gate[1], ffn_up[1], ffn_down[1])),
    )
    width = resid.shape[1]
    return lax.dynamic_slice_in_dim(final, lax.axis_index(("kv", "tp")) * width, width, 1)


def nt_dot(left, right):
    return lax.dot_general(left, right, (((1,), (1,)), ((), ())), preferred_element_type=F32)


def nn_dot(left, right):
    return jnp.dot(left, right, preferred_element_type=F32)


def silu(value):
    return value * jax.nn.sigmoid(value)


def norm_rows(values, gain):
    scale = lax.rsqrt(jnp.mean(values * values, axis=1, keepdims=True) + EPS)
    return (values * scale * gain).astype(BF16)


def split_two(value):
    high = value.astype(BF16)
    return high, (value - high.astype(F32)).astype(BF16)


def layer_kernel(
    nk,
    nt,
    resid,
    gains,
    gate,
    up,
    down,
    wx,
    wz,
    wbc,
    wdt,
    dt_bias,
    a_log,
    d_skip,
    cwx,
    cwbc,
    cx,
    cbc,
    state,
    wout,
    out,
    v,
    m,
):
    me_k, me_t = lax.axis_index("kv"), lax.axis_index("tp")
    n = nk * nt
    me = me_k * nt + me_t
    lead = nt - 1
    rows, width = resid.shape
    dim = n * width
    block = nt * width
    scope = jax.named_scope

    def target(index):
        return {"kv": lax.div(index, nt), "tp": lax.rem(index, nt)}

    def flipped(index, mask):
        bit = 1
        while bit < nk:
            if mask & bit:
                index = index + bit - 2 * bit * lax.rem(lax.div(index, bit), 2)
            bit *= 2
        return index

    def all_peers():
        order = [(x, d) for x in range(nk) for d in range(nt)][1:]
        return [flipped(me_k, x) * nt + lax.rem(me_t + d, nt) for x, d in order]

    def far_first():
        far = [flipped(me_k, x) * nt + t for x in range(1, nk)[::-1] for t in range(nt)]
        return far + [me_k * nt + lax.rem(me_t + d, nt) for d in range(1, nt)]

    def kv_peers():
        return [flipped(me_k, x) for x in range(1, nk)]

    loads = {}

    def load(name, src, dst):
        copy = pltpu.make_async_copy(src, dst, m.load.at[len(loads)])
        copy.start()
        loads[name] = copy

    def loaded(*names):
        with scope("w_" + names[0]):
            for name in names:
                loads[name].wait()

    load("rows", resid, v.rows.at[me])
    load("gains", gains, v.gain.at[me])
    barrier = pltpu.get_barrier_semaphore()
    for q in far_first():
        pl.semaphore_signal(barrier, inc=1, device_id=target(q), device_id_type=MESH)
    load("bias", dt_bias, v.small.at[0])
    load("alog", a_log, v.small.at[1])
    load("skip", d_skip, v.small.at[2])
    load("cwx", cwx, v.cwx)
    load("cwbc", cwbc, v.cwbc)
    load("cx", cx, v.cx)
    load("cbc", cbc, v.cbc)
    load("gate0", gate.at[0], v.gate.at[0])
    load("up0", up.at[0], v.up.at[0])
    load("down0", down.at[0], v.down.at[0])
    lead_loads = (
        (wbc, v.wbc),
        (wdt, v.wdt),
        (state, v.state.at[lead]),
        (wout, v.wout.at[lead]),
    )

    def lead_load(i):
        return pltpu.make_async_copy(*lead_loads[i], m.lead.at[i])

    @pl.when(me_t == lead)
    def _():
        for i in range(3):
            lead_load(i).start()

    load("wx", wx, v.wx)
    load("wz", wz, v.wz)

    @pl.when(me_t == lead)
    def _():
        lead_load(3).start()

    load("gate1", gate.at[1], v.gate.at[1])
    load("up1", up.at[1], v.up.at[1])
    load("down1", down.at[1], v.down.at[1])
    with scope("w_barrier"):
        pl.semaphore_wait(barrier, n - 1)

    def remote(src, dst, ssem, rsem, index):
        return pltpu.make_async_remote_copy(
            src_ref=src,
            dst_ref=dst,
            send_sem=ssem,
            recv_sem=rsem,
            device_id=target(index),
            device_id_type=MESH,
        )

    sent = []

    def send(src, dst, ssem, rsem, index):
        copy = remote(src, dst, ssem, rsem, index)
        copy.start()
        sent.append(copy)

    def arrived(slots, sems, slot, index):
        remote(slots.at[slot], slots.at[slot], sems[0].at[slot], sems[1].at[slot], index).wait_recv()

    loaded("rows", "gains")
    for q in far_first():
        send(v.rows.at[me], v.rows.at[me], m.rows[0].at[q], m.rows[1].at[me], q)
        send(v.gain.at[me], v.gain.at[me], m.gain[0].at[q], m.gain[1].at[me], q)

    home = me_k * nt + lead

    def pushes():
        yield remote(state, v.state.at[me_t], m.state[0].at[me_t], m.state[1].at[me_t], home)
        yield remote(wout, v.wout.at[me_t], m.wout[0].at[me_t], m.wout[1].at[me_t], home)

    @pl.when(me_t != lead)
    def _():
        for copy in pushes():
            copy.start()

    heads, half = v.cx.shape[2], v.cx.shape[1]
    flat = heads * half
    groups = v.cwbc.shape[1] // 2
    pairs = 2 * groups
    lane = lax.broadcasted_iota(jnp.int32, v.expand.shape, 1)
    head_of = lax.broadcasted_iota(jnp.int32, v.expand.shape, 0) * half
    v.expand[...] = jnp.where((lane >= head_of) & (lane < head_of + half), 1.0, 0.0).astype(BF16)
    tile = v.perm.shape[0]
    deep = tile // pairs
    row = lax.broadcasted_iota(jnp.int32, v.perm.shape, 0)
    lane = lax.broadcasted_iota(jnp.int32, v.perm.shape, 1)
    source = (row & (deep - 1)) * pairs + lax.shift_right_logical(row, deep.bit_length() - 1)
    v.perm[...] = jnp.where(lane == source, 1.0, 0.0).astype(BF16)

    def expand(value):
        return nn_dot(value, v.expand[...])

    loaded("bias", "alog", "skip", "cwx", "cwbc", "cx", "cbc")
    taps = v.cx.shape[0]
    known = sum(v.cx[i].astype(F32) * v.cwx[i].astype(F32) for i in range(taps))
    high, low = split_two(known)
    lane = lax.broadcasted_iota(jnp.int32, (half, flat), 1)
    row = lax.broadcasted_iota(jnp.int32, (half, flat), 0)
    own = (lane & (half - 1)) == row
    v.hist[me_k, me_t] = jnp.sum(
        jnp.where(own, expand(high) + expand(low), 0.0), axis=0, keepdims=True
    )
    v.tap[me_t] = jnp.sum(jnp.where(own, expand(v.cwx[taps]), 0.0), axis=0, keepdims=True)

    def to_leads(ref, sems):
        for k in kv_peers()[::-1]:
            q = k * nt + lead
            yield remote(ref.at[me_k, me_t], ref.at[me_k, me_t], sems[0].at[k], sems[1].at[me], q)

    def to_home(ref, sems):
        return remote(
            ref.at[me_k, me_t], ref.at[me_k, me_t], sems[0].at[me_k], sems[1].at[me], home
        )

    def tap_home():
        return remote(v.tap.at[me_t], v.tap.at[me_t], m.tap[0].at[me_t], m.tap[1].at[me_t], home)

    for copy in to_leads(v.hist, m.hist):
        copy.start()
        sent.append(copy)

    @pl.when(me_t != lead)
    def _():
        to_home(v.hist, m.hist).start()
        tap_home().start()

    hist_bc = sum(v.cbc[i].astype(F32) * v.cwbc[i].astype(F32) for i in range(taps))
    tap_bc = v.cwbc[taps].astype(F32)

    units = v.gate.shape[1]

    def gated(blocks, kept):
        squares = jnp.zeros((rows, 1), F32)
        g = jnp.zeros((rows, units), F32)
        u = jnp.zeros((rows, units), F32)
        for step, (values, gain, at) in enumerate(blocks):
            squares = squares + jnp.sum(values * values, axis=1, keepdims=True)
            left = (values * gain).astype(BF16)
            g = g + nn_dot(left, v.gate_t[at, :])
            u = u + nn_dot(left, v.up_t[at, :])
            if step < kept:
                v.held[step, 0] = g
                v.held[step, 1] = u
                g = jnp.zeros((rows, units), F32)
                u = jnp.zeros((rows, units), F32)
        for step in range(kept):
            g = g + v.held[step, 0]
            u = u + v.held[step, 1]
        scale = lax.rsqrt(squares / dim + EPS)
        return (silu(g * scale) * (u * scale)).astype(BF16)

    def turn(source, dest):
        for k in range(dim // 256):
            at = slice(k * 256, (k + 1) * 256)
            dest[at, :] = source[:, at].T

    def turn_ffn(which):
        loaded(f"gate{which}")
        turn(v.gate.at[which], v.gate_t)
        loaded(f"up{which}")
        turn(v.up.at[which], v.up_t)

    def columns(index, count):
        return pl.ds(pl.multiple_of(index * count, 128), count)

    def by_arrival():
        order = [lead - d for d in range(nt)]
        near = [me_k * nt + lax.rem(me_t + d, nt) for d in range(1, nt)]
        return near + [flipped(me_k, x) * nt + t for x in range(1, nk) for t in order]

    def arriving_rows():
        for q in [me] + by_arrival():
            if q is not me:
                with scope("w_rows"):
                    arrived(v.rows, m.rows, q, q)
                    arrived(v.gain, m.gain, q, q)
            yield v.rows[q].astype(F32), v.gain[q, 0:1, :].astype(F32), columns(q, width)

    turn_ffn(0)
    hidden = gated(arriving_rows(), 0)
    loaded("down0")
    for x in range(nk)[::-1]:
        k = flipped(me_k, x)
        v.part[k] = nn_dot(hidden, v.down[0, :, columns(k, block)]).astype(BF16)
        q = k * nt + lead
        if x:
            send(v.part.at[k], v.slab.at[me], m.slab[0].at[q], m.slab[1].at[me], q)

    def slab_home():
        q = me_k * nt + lead
        return remote(v.part.at[me_k], v.slab.at[me], m.slab[0].at[q], m.slab[1].at[me], q)

    @pl.when(me_t != lead)
    def _():
        slab_home().start()

    def gain_cut(index, i):
        return jnp.concatenate(
            [v.gain[index * nt + t, i : i + 1, :].astype(F32) for t in range(nt)], axis=1
        )

    def rows_cut(index):
        return jnp.concatenate([v.rows[index * nt + t].astype(F32) for t in range(nt)], axis=1)

    tall = v.bc.shape[1]

    def bc_row(k):
        return v.bc_b.at[pl.ds(pl.multiple_of(k * tall, 8), tall), :]

    def first_sends():
        order = far_first()
        for q in order[1:-1:nt] + order[::nt]:
            yield remote(v.near.at[me_k], v.near.at[me_k], m.near[0].at[q], m.near[1].at[me_k], q)

    def bc_sends():
        for k in kv_peers()[::-1]:
            q = k * nt + lead
            yield remote(bc_row(k), v.bc.at[me_k], m.bc[0].at[k], m.bc[1].at[me_k], q)

    @pl.when(me_t == lead)
    def _():
        with scope("w_wbc"):
            lead_load(0).wait()
            lead_load(1).wait()
        span = v.wdt.shape[1]
        for c in range(span // deep):
            piece = nn_dot(v.perm[...], v.wbc[c * tile : (c + 1) * tile, :]).astype(BF16)
            for p in range(pairs):
                v.wide[c * deep : (c + 1) * deep, p * 128 : (p + 1) * 128] = piece[
                    p * deep : (p + 1) * deep, :
                ]
        with scope("w_state"):
            lead_load(2).wait()
            for t in range(lead):
                arrived(v.state, m.state, t, me_k * nt + t)
        for t in range(nt):
            for i in range(flat // 256):
                at = slice(i * 256, (i + 1) * 256)
                v.state_b[t, :, at] = v.state[t, at, :].astype(BF16).T
        v.slab[me] = v.part[me_k]
        with scope("w_slab"):
            for q in all_peers():
                arrived(v.slab, m.slab, q, q)
        total = sum(v.slab[q].astype(F32) for q in range(n))
        first = (rows_cut(me_k) + 0.5 * total).astype(BF16)
        v.near[me_k] = first
        for copy in first_sends():
            copy.start()
        left = (first.astype(F32) * gain_cut(me_k, 1)).astype(BF16)
        bc_part = nn_dot(left, v.wide[...])
        dt_part = nt_dot(left, v.wdt[...])
        for p in range(pairs):
            v.bc_b[pl.ds(p, rows, stride=tall), :] = bc_part[:, p * 128 : (p + 1) * 128]
        v.bc_b[pl.ds(pairs, rows, stride=tall), :] = jnp.concatenate(
            [dt_part, jnp.zeros((rows, 128 - heads), F32)], axis=1
        )
        for copy in bc_sends():
            copy.start()
        v.bc[me_k] = bc_row(me_k)[...]

    def arrived_at(slots, sems, k, t):
        q = k * nt + t
        remote(slots.at[k, t], slots.at[k, t], sems[0].at[k], sems[1].at[q], q).wait_recv()

    def arrived_from_lead(slots, sems, k):
        @pl.when(k * nt + lead != me)
        def _():
            arrived(slots, sems, k, k * nt + lead)

    loaded("wx", "wz")
    turn(v.wx, v.wx_t)
    turn(v.wz, v.wz_t)
    local = v.wx.shape[0]
    xs_part = jnp.zeros((rows, local), F32)
    z_part = jnp.zeros((rows, local), F32)
    squares = jnp.zeros((rows, 1), F32)
    for x in range(nk):
        k = flipped(me_k, x)
        with scope("w_near"):
            if x:
                arrived(v.near, m.near, k, k * nt + lead)
            else:
                arrived_from_lead(v.near, m.near, k)
        first = v.near[k].astype(F32)
        v.first[k] = first
        left = (first * gain_cut(k, 1)).astype(BF16)
        squares = squares + jnp.sum(first * first, axis=1, keepdims=True)
        xs_part = xs_part + nn_dot(left, v.wx_t[columns(k, block), :])
        z_part = z_part + nn_dot(left, v.wz_t[columns(k, block), :])
    scale = lax.rsqrt(squares / dim + EPS)
    v.scale[...] = jnp.broadcast_to(scale, v.scale.shape)
    v.xz[me_k, me_t] = jnp.concatenate([xs_part * scale, z_part * scale], axis=1).astype(BF16)
    for copy in to_leads(v.xz, m.xz):
        copy.start()
        sent.append(copy)

    @pl.when(me_t != lead)
    def _():
        to_home(v.xz, m.xz).start()
        turn_ffn(1)

    def proj_sends():
        for q in far_first():
            yield remote(v.proj.at[me_k], v.proj.at[me_k], m.proj[0].at[q], m.proj[1].at[me_k], q)

    @pl.when(me_t == lead)
    def _():
        with scope("w_bc"):
            for k in kv_peers():
                arrived(v.bc, m.bc, k, k * nt + lead)
        summed = sum(v.bc[k] for k in range(nk)) * v.scale[pl.ds(me_k, 1), :]
        raw = summed[pairs : pairs + 1, :heads] + v.small[0]
        step = jnp.maximum(raw, 0.0) + jnp.log1p(jnp.exp(-jnp.abs(raw)))
        decay = jnp.exp(-step * jnp.exp(v.small[1]))
        bc_new = summed[:pairs].astype(BF16).astype(F32)
        bconv = silu(hist_bc + bc_new * tap_bc)
        bmat, cmat = bconv[:groups], bconv[groups:]
        weight = jnp.sum(bmat * cmat, axis=1, keepdims=True)
        lane = lax.broadcasted_iota(jnp.int32, (groups, heads), 1)
        low_end = lax.broadcasted_iota(jnp.int32, (groups, heads), 0) * (heads // groups)
        mine = (lane >= low_end) & (lane < low_end + heads // groups)
        cross = jnp.sum(jnp.where(mine, weight, 0.0), axis=0, keepdims=True)
        v.coef[me_k] = step * cross + v.small[2]

        def coef_sends():
            for k in kv_peers()[::-1]:
                q = k * nt + lead
                yield remote(
                    v.coef.at[me_k], v.coef.at[me_k], m.coef[0].at[k], m.coef[1].at[me_k], q
                )

        for copy in coef_sends():
            copy.start()
        decay_high, decay_low = split_two(decay)
        spread = expand(jnp.concatenate([decay_high, decay_low], axis=0))
        decay_row = spread[0:1] + spread[1:2]
        lane = lax.broadcasted_iota(jnp.int32, (groups, flat), 1)
        low_end = lax.broadcasted_iota(jnp.int32, (groups, flat), 0) * (flat // groups)
        mine = (lane >= low_end) & (lane < low_end + flat // groups)
        lines = []
        for t in range(nt):
            per_group = nn_dot(cmat.astype(BF16), v.state_b[t])
            read = jnp.sum(jnp.where(mine, per_group, 0.0), axis=0, keepdims=True)
            lines.append(decay_row * read)
        v.mix[me_k] = jnp.concatenate(lines, axis=0).astype(BF16)

        def mix_sends():
            for k in kv_peers()[::-1]:
                q = k * nt + lead
                yield remote(v.mix.at[me_k], v.mix.at[me_k], m.mix[0].at[k], m.mix[1].at[me_k], q)

        for copy in mix_sends():
            copy.start()
        turn_ffn(1)
        with scope("w_hist"):
            for t in range(lead):
                arrived(v.tap, m.tap, t, me_k * nt + t)
                arrived_at(v.hist, m.hist, me_k, t)
            for k in kv_peers():
                for t in range(nt):
                    arrived_at(v.hist, m.hist, k, t)
        with scope("w_wout"):
            lead_load(3).wait()
            for t in range(lead):
                arrived(v.wout, m.wout, t, me_k * nt + t)
        for t in range(nt):
            v.past[t] = jnp.concatenate([v.hist[i, t] for i in range(nk)], axis=0)
        with scope("w_coef"):
            for k in kv_peers():
                arrived(v.coef, m.coef, k, k * nt + lead)
        high, low = split_two(jnp.concatenate([v.coef[i] for i in range(nk)], axis=0))
        spread = expand(jnp.concatenate([high, low], axis=0))
        v.direct[...] = spread[:nk] + spread[nk:]
        with scope("w_mix"):
            for k in kv_peers():
                arrived(v.mix, m.mix, k, k * nt + lead)
        total = jnp.zeros((rows, v.wout.shape[2]), F32)
        for x in range(nk):
            k = flipped(me_k, x)
            at = columns(k, local)
            with scope("w_xz"):
                for t in range(nt)[::-1]:
                    if x or t != lead:
                        arrived_at(v.xz, m.xz, k, t)
            direct = v.direct[:, at]
            for t in range(nt):
                read = jnp.concatenate(
                    [v.mix[i, t : t + 1, at].astype(F32) for i in range(nk)], axis=0
                )
                xs_new = v.xz[k, t, :, :local].astype(F32)
                xconv = silu(v.past[t, :, at] + xs_new * v.tap[t, :, at])
                opened = silu(v.xz[k, t, :, local:].astype(F32))
                mixed = ((read + direct * xconv) * opened).astype(BF16)
                total = total + nn_dot(mixed, v.wout[t, at, :])
        v.proj[me_k] = total.astype(BF16)
        for copy in proj_sends():
            copy.start()
        for copy in mix_sends():
            copy.wait_send()
        for copy in coef_sends():
            copy.wait_send()

    def arriving_blocks():
        for x in range(nk):
            k = flipped(me_k, x)
            with scope("w_proj"):
                if x:
                    arrived(v.proj, m.proj, k, k * nt + lead)
                else:
                    arrived_from_lead(v.proj, m.proj, k)
            second = (v.first[k] + v.proj[k].astype(F32)).astype(BF16).astype(F32)
            if x == 0:
                for t in range(nt):
                    v.second[t] = second[:, t * width : (t + 1) * width]
            yield second, gain_cut(k, 2), columns(k, block)

    hidden = gated(arriving_blocks(), nk - 1)
    loaded("down1")
    for x in range(nk)[::-1]:
        k = flipped(me_k, x)
        piece = nn_dot(hidden, v.down[1, :, columns(k, block)])
        for t in range(nt):
            v.cut_b[k * nt + t] = piece[:, t * width : (t + 1) * width].astype(BF16)
        for d in range(nt):
            if x or d:
                q = k * nt + (d if x else lax.rem(me_t + d, nt))
                send(v.cut_b.at[q], v.cut.at[me], m.cut[0].at[q], m.cut[1].at[me], q)
    v.cut[me] = v.cut_b[me]
    with scope("w_sent"):
        for copy in sent[:-(n - 1)]:
            copy.wait_send()

        @pl.when(me_t == lead)
        def _():
            for copy in first_sends():
                copy.wait_send()
            for copy in bc_sends():
                copy.wait_send()
            for copy in proj_sends():
                copy.wait_send()

        @pl.when(me_t != lead)
        def _():
            slab_home().wait_send()
            to_home(v.hist, m.hist).wait_send()
            to_home(v.xz, m.xz).wait_send()
            tap_home().wait_send()
            for copy in pushes():
                copy.wait_send()
    with scope("w_cut"):
        for q in all_peers():
            arrived(v.cut, m.cut, q, q)
    total = sum(v.cut[q].astype(F32) for q in range(n))
    out[...] = (v.second[me_t] + 0.5 * total).astype(BF16)
    for copy in sent[-(n - 1) :]:
        copy.wait_send()


def fused_layer(
    nk,
    nt,
    resid,
    norm_gain,
    ffn_gate,
    ffn_up,
    ffn_down,
    w_x,
    w_z,
    w_bc,
    w_dt,
    dt_bias,
    a_log,
    d_skip,
    conv_wx,
    conv_wbc,
    conv_x,
    conv_bc,
    ssm_state,
    w_out,
):
    n = nk * nt
    rows, width = resid.shape
    dim = ffn_gate.shape[1]
    units = ffn_gate.shape[2]
    local = w_x.shape[1] * w_x.shape[2]
    heads, half = conv_x.shape[2], conv_x.shape[3]
    flat = heads * half
    span = w_bc.shape[0]
    lanes = w_bc.shape[3]
    pairs = w_bc.shape[1] * w_bc.shape[2]
    out_cols = w_out.shape[2]
    taps = conv_wx.shape[0]
    block = nt * width
    args = (
        resid,
        norm_gain,
        jnp.swapaxes(ffn_gate, 1, 2),
        jnp.swapaxes(ffn_up, 1, 2),
        ffn_down,
        jnp.transpose(w_x, (1, 2, 0)).reshape(local, dim),
        jnp.transpose(w_z, (1, 2, 0)).reshape(local, dim),
        w_bc.reshape(span * pairs, lanes),
        w_dt.T,
        dt_bias.reshape(1, heads),
        a_log.reshape(1, heads),
        d_skip.reshape(1, heads),
        jnp.swapaxes(conv_wx, 1, 2),
        conv_wbc.reshape(taps, pairs, lanes),
        jnp.swapaxes(conv_x, 2, 3).reshape(taps - 1, half, heads),
        conv_bc.reshape(taps - 1, pairs, lanes),
        ssm_state.reshape(flat, lanes),
        w_out.reshape(flat, out_cols),
    )
    dma = pltpu.SemaphoreType.DMA
    vmem = pltpu.VMEM
    scratch = dict(
        gate=vmem((2, units, dim), BF16),
        up=vmem((2, units, dim), BF16),
        down=vmem((2, units, dim), BF16),
        gate_t=vmem((dim, units), BF16),
        up_t=vmem((dim, units), BF16),
        wx_t=vmem((dim, local), BF16),
        wz_t=vmem((dim, local), BF16),
        wx=vmem((local, dim), BF16),
        wz=vmem((local, dim), BF16),
        wbc=vmem((span * pairs, lanes), BF16),
        wide=vmem((span, pairs * lanes), BF16),
        wdt=vmem((heads, span), BF16),
        state=vmem((nt, flat, lanes), F32),
        state_b=vmem((nt, lanes, flat), BF16),
        wout=vmem((nt, flat, out_cols), BF16),
        small=vmem((3, 1, heads), F32),
        cwx=vmem((taps, half, heads), BF16),
        cwbc=vmem((taps, pairs, lanes), BF16),
        cx=vmem((taps - 1, half, heads), BF16),
        cbc=vmem((taps - 1, pairs, lanes), BF16),
        expand=vmem((heads, flat), BF16),
        perm=vmem((256, 256), BF16),
        rows=vmem((n, rows, width), BF16),
        gain=vmem((n, 3, width), BF16),
        part=vmem((nk, rows, block), BF16),
        slab=vmem((n, rows, block), BF16),
        near=vmem((nk, rows, block), BF16),
        held=vmem((nk - 1, 2, rows, units), F32),
        first=vmem((nk, rows, block), F32),
        scale=vmem((rows, lanes), F32),
        bc_b=vmem((nk * (pairs + 8), lanes), F32),
        bc=vmem((nk, pairs + 8, lanes), F32),
        hist=vmem((nk, nt, 1, flat), F32),
        tap=vmem((nt, 1, flat), F32),
        xz=vmem((nk, nt, rows, 2 * local), BF16),
        past=vmem((nt, rows, flat), F32),
        coef=vmem((nk, 1, heads), F32),
        direct=vmem((nk, flat), F32),
        mix=vmem((nk, nt, flat), BF16),
        proj=vmem((nk, rows, out_cols), BF16),
        second=vmem((nt, rows, width), F32),
        cut_b=vmem((n, rows, width), BF16),
        cut=vmem((n, rows, width), BF16),
    )
    rounds = dict(
        rows=n, gain=n, slab=n, near=n, bc=n, hist=n, xz=n, mix=nk, coef=nk, state=nt, wout=nt, tap=nt, proj=n, cut=n
    )
    sems = {name: (dma((count,)), dma((count,))) for name, count in rounds.items()}
    sems["load"] = dma((17,))
    sems["lead"] = dma((4,))

    def kernel(*refs, **held):
        def body(**flags):
            layer_kernel(nk, nt, *refs, SimpleNamespace(**held), SimpleNamespace(**flags))

        pl.run_scoped(body, **sems)

    return pl.pallas_call(
        kernel,
        out_shape=pltpu.VMEM(resid.shape, resid.dtype),
        in_specs=[pl.BlockSpec(memory_space=pl.ANY)] * len(args),
        out_specs=pl.BlockSpec(memory_space=pltpu.VMEM),
        scratch_shapes=scratch,
        compiler_params=pltpu.CompilerParams(
            collective_id=0, has_side_effects=True, vmem_limit_bytes=60 * 1024 * 1024
        ),
    )(*args)


def fits(nk, nt, resid, w_x, w_bc, conv_x):
    rows, width = resid.shape
    half = conv_x.shape[3]
    pairs = w_bc.shape[1] * w_bc.shape[2]
    return (
        conv_x.shape[0] == 1
        and rows == nk
        and nt > 1
        and nk & (nk - 1) == 0
        and w_bc.shape[0] == nt * width
        and width % 128 == 0
        and (nk * nt * width) % 256 == 0
        and (conv_x.shape[2] * conv_x.shape[3]) % 256 == 0
        and w_bc.shape[0] % 128 == 0
        and (w_x.shape[1] * w_x.shape[2]) % 128 == 0
        and half & (half - 1) == 0
        and pairs & (pairs - 1) == 0
        and pairs % 8 == 0
        and 256 % pairs == 0
        and (w_bc.shape[0] * pairs) % 256 == 0
        and w_bc.shape[3] == 128
        and conv_x.shape[2] < 128
    )


def solution(mesh):
    placed = (
        P("dp", ("kv", "tp")),
        P(None, ("kv", "tp")),
        P(None, None, ("kv", "tp")),
        P(None, None, ("kv", "tp")),
        P(None, ("kv", "tp"), None),
        P(None, "kv", "tp"),
        P(None, "kv", "tp"),
        P("kv", None, None, None),
        P("kv", None),
        P(),
        P(),
        P(),
        P(None, None, "tp"),
        P(),
        P(("dp", "kv"), None, None, "tp"),
        P(("dp", "kv"), None, None, None, None),
        P(("dp", "kv"), None, "tp", None),
        P(None, "tp", "kv"),
    )
    nk, nt = mesh.shape["kv"], mesh.shape["tp"]

    def layer(*args):
        if fits(nk, nt, args[0], args[5], args[7], args[14]):
            return fused_layer(nk, nt, *args)
        return per_device(*args)

    return jax.shard_map(
        layer, mesh=mesh, in_specs=placed, out_specs=P("dp", ("kv", "tp")), check_vma=False
    )
```

```python
from types import SimpleNamespace

import jax
import jax.numpy as jnp
from jax import lax
from jax.experimental import pallas as pl
from jax.experimental.pallas import tpu as pltpu
from jax.sharding import PartitionSpec as P

D = 2048
F32 = jnp.float32
BF16 = jnp.bfloat16
MESH = pl.DeviceIdType.MESH

EPS = 1e-06


def normalize(rows, gain):
    values = rows.astype(jnp.float32)
    scale = lax.rsqrt(jnp.mean(values * values, axis=1, keepdims=True) + EPS)
    return (values * scale * gain.astype(jnp.float32).reshape(1, -1)).astype(jnp.bfloat16)


def feed_forward(normed, w_gate, w_up, w_down):
    gate = jnp.dot(normed, w_gate, preferred_element_type=jnp.float32)
    upper = jnp.dot(normed, w_up, preferred_element_type=jnp.float32)
    hidden = (jax.nn.silu(gate) * upper).astype(jnp.bfloat16)
    return jnp.dot(hidden, w_down, preferred_element_type=jnp.float32)


def add_half(base, sums):
    return (base.astype(jnp.float32) + 0.5 * sums).astype(jnp.bfloat16)


def ffn_totals(partial_value):
    return lax.psum(partial_value, ("kv", "tp"))


def short_conv(history, newest, taps):
    window = jnp.concatenate(
        [history.astype(jnp.float32), newest.astype(jnp.float32)[:, None]], axis=1
    )
    return jax.nn.silu(jnp.sum(window * taps.astype(jnp.float32)[None], axis=1))


def state_step(
    xs_new,
    zeta,
    bc_new,
    dt_raw,
    conv_x,
    conv_bc,
    ssm_state,
    conv_wx,
    conv_wbc,
    dt_bias,
    a_log,
    d_skip,
):
    xconv = short_conv(conv_x, xs_new, conv_wx)
    bconv = short_conv(conv_bc, bc_new, conv_wbc)
    heads = xconv.shape[1]
    groups = bconv.shape[2]
    bmat = jnp.repeat(bconv[:, 0], heads // groups, axis=1)
    cmat = jnp.repeat(bconv[:, 1], heads // groups, axis=1)
    step_size = jax.nn.softplus(dt_raw + dt_bias[None, :])
    decay = jnp.exp(-step_size * jnp.exp(a_log)[None, :])
    updated = (
        decay[:, :, None, None] * ssm_state
        + (step_size[:, :, None] * xconv)[..., None] * bmat[:, :, None, :]
    )
    mixed = (
        jnp.einsum("shpn,shn->shp", updated, cmat, precision=lax.Precision.HIGHEST)
        + d_skip[None, :, None] * xconv
    )
    return (mixed * jax.nn.silu(zeta.astype(jnp.float32))).astype(jnp.bfloat16)


def group_terms(slab, w_bc, w_dt):
    span = slab.shape[1]
    flat_bc = w_bc.reshape(span, -1)
    bc_part = jnp.dot(slab, flat_bc, preferred_element_type=jnp.float32)
    dt_part = jnp.dot(slab, w_dt, preferred_element_type=jnp.float32)
    return (
        lax.psum_scatter(bc_part, "kv", scatter_dimension=0, tiled=True),
        lax.psum_scatter(dt_part, "kv", scatter_dimension=0, tiled=True),
    )


def mix_partial(
    normed,
    w_x,
    w_z,
    w_bc,
    w_dt,
    dt_bias,
    a_log,
    d_skip,
    conv_wx,
    conv_wbc,
    conv_x,
    conv_bc,
    ssm_state,
    w_out,
):
    rows = normed.shape[0]
    local_heads = w_x.shape[1]
    half = w_x.shape[2]
    xs_part = (
        jnp.dot(normed, w_x.reshape(D, -1), preferred_element_type=jnp.float32)
        .astype(jnp.bfloat16)
        .reshape(rows, local_heads, half)
    )
    zeta_part = (
        jnp.dot(normed, w_z.reshape(D, -1), preferred_element_type=jnp.float32)
        .astype(jnp.bfloat16)
        .reshape(rows, local_heads, half)
    )
    xs_new, zeta = (
        lax.all_to_all(xs_part, "kv", split_axis=0, concat_axis=1, tiled=True),
        lax.all_to_all(zeta_part, "kv", split_axis=0, concat_axis=1, tiled=True),
    )
    span = w_bc.shape[0]
    slab = lax.dynamic_slice_in_dim(normed, lax.axis_index("kv") * span, span, 1)
    bc_sum, dt_raw = group_terms(slab, w_bc, w_dt)
    bc_new = bc_sum.astype(jnp.bfloat16).reshape((bc_sum.shape[0],) + w_bc.shape[1:])
    mixed = state_step(
        xs_new,
        zeta,
        bc_new,
        dt_raw,
        conv_x,
        conv_bc,
        ssm_state,
        conv_wx,
        conv_wbc,
        dt_bias,
        a_log,
        d_skip,
    )
    flat_out = w_out.reshape(-1, w_out.shape[2])
    piece = lax.all_gather(mixed, "kv", axis=0, tiled=True)
    return jnp.dot(piece.reshape(piece.shape[0], -1), flat_out, preferred_element_type=jnp.float32)


def per_device(
    resid,
    norm_gain,
    ffn_gate,
    ffn_up,
    ffn_down,
    w_x,
    w_z,
    w_bc,
    w_dt,
    dt_bias,
    a_log,
    d_skip,
    conv_wx,
    conv_wbc,
    conv_x,
    conv_bc,
    ssm_state,
    w_out,
):
    mixer_args = (
        w_x,
        w_z,
        w_bc,
        w_dt,
        dt_bias,
        a_log,
        d_skip,
        conv_wx,
        conv_wbc,
        conv_x,
        conv_bc,
        ssm_state,
        w_out,
    )
    rows, gains = (
        lax.all_gather(resid, ("kv", "tp"), axis=1, tiled=True),
        lax.all_gather(norm_gain, ("kv", "tp"), axis=1, tiled=True),
    )
    first = add_half(
        rows,
        ffn_totals(feed_forward(normalize(rows, gains[0]), ffn_gate[0], ffn_up[0], ffn_down[0])),
    )
    partial_value = mix_partial(normalize(first, gains[1]), *mixer_args)
    span = partial_value.shape[1]
    block = lax.dynamic_slice_in_dim(first, lax.axis_index("kv") * span, span, 1)
    joined = (block.astype(jnp.float32) + lax.psum(partial_value, "tp")).astype(jnp.bfloat16)
    second = lax.all_gather(joined, "kv", axis=1, tiled=True)
    final = add_half(
        second,
        ffn_totals(feed_forward(normalize(second, gains[2]), ffn_gate[1], ffn_up[1], ffn_down[1])),
    )
    width = resid.shape[1]
    return lax.dynamic_slice_in_dim(final, lax.axis_index(("kv", "tp")) * width, width, 1)


def nt_dot(left, right):
    return lax.dot_general(left, right, (((1,), (1,)), ((), ())), preferred_element_type=F32)


def nn_dot(left, right):
    return jnp.dot(left, right, preferred_element_type=F32)


def silu(value):
    return value * jax.nn.sigmoid(value)


def norm_rows(values, gain):
    scale = lax.rsqrt(jnp.mean(values * values, axis=1, keepdims=True) + EPS)
    return (values * scale * gain).astype(BF16)


def split_two(value):
    high = value.astype(BF16)
    return high, (value - high.astype(F32)).astype(BF16)


def layer_kernel(
    nk,
    nt,
    resid,
    gains,
    gate,
    up,
    down,
    wx,
    wz,
    wbc,
    wdt,
    dt_bias,
    a_log,
    d_skip,
    cwx,
    cwbc,
    cx,
    cbc,
    state,
    wout,
    out,
    v,
    m,
):
    me_k, me_t = lax.axis_index("kv"), lax.axis_index("tp")
    n = nk * nt
    me = me_k * nt + me_t
    lead = nt - 1
    rows, width = resid.shape
    dim = n * width
    block = nt * width
    scope = jax.named_scope

    def target(index):
        return {"kv": lax.div(index, nt), "tp": lax.rem(index, nt)}

    def flipped(index, mask):
        bit = 1
        while bit < nk:
            if mask & bit:
                index = index + bit - 2 * bit * lax.rem(lax.div(index, bit), 2)
            bit *= 2
        return index

    def all_peers():
        order = [(x, d) for x in range(nk) for d in range(nt)][1:]
        return [flipped(me_k, x) * nt + lax.rem(me_t + d, nt) for x, d in order]

    def far_first():
        far = [flipped(me_k, x) * nt + t for x in range(1, nk)[::-1] for t in range(nt)]
        return far + [me_k * nt + lax.rem(me_t + d, nt) for d in range(1, nt)]

    def kv_peers():
        return [flipped(me_k, x) for x in range(1, nk)]

    loads = {}

    def load(name, src, dst):
        copy = pltpu.make_async_copy(src, dst, m.load.at[len(loads)])
        copy.start()
        loads[name] = copy

    def loaded(*names):
        with scope("w_" + names[0]):
            for name in names:
                loads[name].wait()

    load("rows", resid, v.rows.at[me])
    load("gains", gains, v.gain.at[me])
    barrier = pltpu.get_barrier_semaphore()
    for q in far_first():
        pl.semaphore_signal(barrier, inc=1, device_id=target(q), device_id_type=MESH)
    load("bias", dt_bias, v.small.at[0])
    load("alog", a_log, v.small.at[1])
    load("skip", d_skip, v.small.at[2])
    load("cwx", cwx, v.cwx)
    load("cwbc", cwbc, v.cwbc)
    load("cx", cx, v.cx)
    load("cbc", cbc, v.cbc)
    load("gate0", gate.at[0], v.gate.at[0])
    load("up0", up.at[0], v.up.at[0])
    load("down0", down.at[0], v.down.at[0])
    lead_loads = (
        (wbc, v.wbc),
        (wdt, v.wdt),
        (state, v.state.at[lead]),
        (wout, v.wout.at[lead]),
    )

    def lead_load(i):
        return pltpu.make_async_copy(*lead_loads[i], m.lead.at[i])

    @pl.when(me_t == lead)
    def _():
        for i in range(3):
            lead_load(i).start()

    load("wx", wx, v.wx)
    load("wz", wz, v.wz)

    @pl.when(me_t == lead)
    def _():
        lead_load(3).start()

    load("gate1", gate.at[1], v.gate.at[1])
    load("up1", up.at[1], v.up.at[1])
    load("down1", down.at[1], v.down.at[1])
    with scope("w_barrier"):
        pl.semaphore_wait(barrier, n - 1)

    def remote(src, dst, ssem, rsem, index):
        return pltpu.make_async_remote_copy(
            src_ref=src,
            dst_ref=dst,
            send_sem=ssem,
            recv_sem=rsem,
            device_id=target(index),
            device_id_type=MESH,
        )

    sent = []

    def send(src, dst, ssem, rsem, index):
        copy = remote(src, dst, ssem, rsem, index)
        copy.start()
        sent.append(copy)

    def arrived(slots, sems, slot, index):
        remote(slots.at[slot], slots.at[slot], sems[0].at[slot], sems[1].at[slot], index).wait_recv()

    loaded("rows", "gains")
    for q in far_first():
        send(v.rows.at[me], v.rows.at[me], m.rows[0].at[q], m.rows[1].at[me], q)
        send(v.gain.at[me], v.gain.at[me], m.gain[0].at[q], m.gain[1].at[me], q)

    home = me_k * nt + lead

    def pushes():
        yield remote(state, v.state.at[me_t], m.state[0].at[me_t], m.state[1].at[me_t], home)
        yield remote(wout, v.wout.at[me_t], m.wout[0].at[me_t], m.wout[1].at[me_t], home)

    @pl.when(me_t != lead)
    def _():
        for copy in pushes():
            copy.start()

    heads, half = v.cx.shape[2], v.cx.shape[1]
    flat = heads * half
    groups = v.cwbc.shape[1] // 2
    pairs = 2 * groups
    lane = lax.broadcasted_iota(jnp.int32, v.expand.shape, 1)
    head_of = lax.broadcasted_iota(jnp.int32, v.expand.shape, 0) * half
    v.expand[...] = jnp.where((lane >= head_of) & (lane < head_of + half), 1.0, 0.0).astype(BF16)
    tile = v.perm.shape[0]
    deep = tile // pairs
    row = lax.broadcasted_iota(jnp.int32, v.perm.shape, 0)
    lane = lax.broadcasted_iota(jnp.int32, v.perm.shape, 1)
    source = (row & (deep - 1)) * pairs + lax.shift_right_logical(row, deep.bit_length() - 1)
    v.perm[...] = jnp.where(lane == source, 1.0, 0.0).astype(BF16)

    def expand(value):
        return nn_dot(value, v.expand[...])

    loaded("bias", "alog", "skip", "cwx", "cwbc", "cx", "cbc")
    taps = v.cx.shape[0]
    known = sum(v.cx[i].astype(F32) * v.cwx[i].astype(F32) for i in range(taps))
    high, low = split_two(known)
    lane = lax.broadcasted_iota(jnp.int32, (half, flat), 1)
    row = lax.broadcasted_iota(jnp.int32, (half, flat), 0)
    own = (lane & (half - 1)) == row
    v.hist[me_k, me_t] = jnp.sum(
        jnp.where(own, expand(high) + expand(low), 0.0), axis=0, keepdims=True
    )
    v.tap[me_t] = jnp.sum(jnp.where(own, expand(v.cwx[taps]), 0.0), axis=0, keepdims=True)

    def to_leads(ref, sems):
        for k in kv_peers()[::-1]:
            q = k * nt + lead
            yield remote(ref.at[me_k, me_t], ref.at[me_k, me_t], sems[0].at[k], sems[1].at[me], q)

    def to_home(ref, sems):
        return remote(
            ref.at[me_k, me_t], ref.at[me_k, me_t], sems[0].at[me_k], sems[1].at[me], home
        )

    def tap_home():
        return remote(v.tap.at[me_t], v.tap.at[me_t], m.tap[0].at[me_t], m.tap[1].at[me_t], home)

    for copy in to_leads(v.hist, m.hist):
        copy.start()
        sent.append(copy)

    @pl.when(me_t != lead)
    def _():
        to_home(v.hist, m.hist).start()
        tap_home().start()

    hist_bc = sum(v.cbc[i].astype(F32) * v.cwbc[i].astype(F32) for i in range(taps))
    tap_bc = v.cwbc[taps].astype(F32)

    units = v.gate.shape[1]

    def gated(blocks, kept):
        squares = jnp.zeros((rows, 1), F32)
        g = jnp.zeros((rows, units), F32)
        u = jnp.zeros((rows, units), F32)
        for step, (values, gain, at) in enumerate(blocks):
            squares = squares + jnp.sum(values * values, axis=1, keepdims=True)
            left = (values * gain).astype(BF16)
            g = g + nn_dot(left, v.gate_t[at, :])
            u = u + nn_dot(left, v.up_t[at, :])
            if step < kept:
                v.held[step, 0] = g
                v.held[step, 1] = u
                g = jnp.zeros((rows, units), F32)
                u = jnp.zeros((rows, units), F32)
        for step in range(kept):
            g = g + v.held[step, 0]
            u = u + v.held[step, 1]
        scale = lax.rsqrt(squares / dim + EPS)
        return (silu(g * scale) * (u * scale)).astype(BF16)

    def turn(source, dest):
        for k in range(dim // 256):
            at = slice(k * 256, (k + 1) * 256)
            dest[at, :] = source[:, at].T

    def turn_ffn(which):
        loaded(f"gate{which}")
        turn(v.gate.at[which], v.gate_t)
        loaded(f"up{which}")
        turn(v.up.at[which], v.up_t)

    def columns(index, count):
        return pl.ds(pl.multiple_of(index * count, 128), count)

    def by_arrival():
        order = [lead - d for d in range(nt)]
        near = [me_k * nt + lax.rem(me_t + d, nt) for d in range(1, nt)]
        return near + [flipped(me_k, x) * nt + t for x in range(1, nk) for t in order]

    def arriving_rows():
        for q in [me] + by_arrival():
            if q is not me:
                with scope("w_rows"):
                    arrived(v.rows, m.rows, q, q)
                    arrived(v.gain, m.gain, q, q)
            yield v.rows[q].astype(F32), v.gain[q, 0:1, :].astype(F32), columns(q, width)

    turn_ffn(0)
    hidden = gated(arriving_rows(), 0)
    loaded("down0")
    for far in ((nk - 1,), tuple(range(nk - 1))[::-1]):
        pieces = {x: nn_dot(hidden, v.down[0, :, columns(flipped(me_k, x), block)]) for x in far}
        for x in far:
            v.part[flipped(me_k, x)] = pieces[x].astype(BF16)
        for x in far:
            k = flipped(me_k, x)
            q = k * nt + lead
            if x:
                send(v.part.at[k], v.slab.at[me], m.slab[0].at[q], m.slab[1].at[me], q)

    def slab_home():
        q = me_k * nt + lead
        return remote(v.part.at[me_k], v.slab.at[me], m.slab[0].at[q], m.slab[1].at[me], q)

    @pl.when(me_t != lead)
    def _():
        slab_home().start()

    def gain_cut(index, i):
        return jnp.concatenate(
            [v.gain[index * nt + t, i : i + 1, :].astype(F32) for t in range(nt)], axis=1
        )

    def rows_cut(index):
        return jnp.concatenate([v.rows[index * nt + t].astype(F32) for t in range(nt)], axis=1)

    tall = v.bc.shape[1]

    def bc_row(k):
        return v.bc_b.at[pl.ds(pl.multiple_of(k * tall, 8), tall), :]

    def first_sends():
        order = far_first()
        for q in order[1:-1:nt] + order[::nt]:
            yield remote(v.near.at[me_k], v.near.at[me_k], m.near[0].at[q], m.near[1].at[me_k], q)

    def bc_sends():
        for k in kv_peers()[::-1]:
            q = k * nt + lead
            yield remote(bc_row(k), v.bc.at[me_k], m.bc[0].at[k], m.bc[1].at[me_k], q)

    @pl.when(me_t == lead)
    def _():
        with scope("w_wbc"):
            lead_load(0).wait()
            lead_load(1).wait()
        span = v.wdt.shape[1]
        for c in range(span // deep):
            piece = nn_dot(v.perm[...], v.wbc[c * tile : (c + 1) * tile, :]).astype(BF16)
            for p in range(pairs):
                v.wide[c * deep : (c + 1) * deep, p * 128 : (p + 1) * 128] = piece[
                    p * deep : (p + 1) * deep, :
                ]
        with scope("w_state"):
            lead_load(2).wait()
            for t in range(lead):
                arrived(v.state, m.state, t, me_k * nt + t)
        for t in range(nt):
            for i in range(flat // 256):
                at = slice(i * 256, (i + 1) * 256)
                v.state_b[t, :, at] = v.state[t, at, :].astype(BF16).T
        v.slab[me] = v.part[me_k]
        with scope("w_slab"):
            for q in all_peers():
                arrived(v.slab, m.slab, q, q)
        total = sum(v.slab[q].astype(F32) for q in range(n))
        first = (rows_cut(me_k) + 0.5 * total).astype(BF16)
        v.near[me_k] = first
        for copy in first_sends():
            copy.start()
        left = (first.astype(F32) * gain_cut(me_k, 1)).astype(BF16)
        bc_part = nn_dot(left, v.wide[...])
        dt_part = nt_dot(left, v.wdt[...])
        for p in range(pairs):
            v.bc_b[pl.ds(p, rows, stride=tall), :] = bc_part[:, p * 128 : (p + 1) * 128]
        v.bc_b[pl.ds(pairs, rows, stride=tall), :] = jnp.concatenate(
            [dt_part, jnp.zeros((rows, 128 - heads), F32)], axis=1
        )
        for copy in bc_sends():
            copy.start()
        v.bc[me_k] = bc_row(me_k)[...]

    def arrived_at(slots, sems, k, t):
        q = k * nt + t
        remote(slots.at[k, t], slots.at[k, t], sems[0].at[k], sems[1].at[q], q).wait_recv()

    def arrived_from_lead(slots, sems, k):
        @pl.when(k * nt + lead != me)
        def _():
            arrived(slots, sems, k, k * nt + lead)

    loaded("wx", "wz")
    turn(v.wx, v.wx_t)
    turn(v.wz, v.wz_t)
    local = v.wx.shape[0]
    xs_part = jnp.zeros((rows, local), F32)
    z_part = jnp.zeros((rows, local), F32)
    squares = jnp.zeros((rows, 1), F32)
    for x in range(nk):
        k = flipped(me_k, x)
        with scope("w_near"):
            if x:
                arrived(v.near, m.near, k, k * nt + lead)
            else:
                arrived_from_lead(v.near, m.near, k)
        first = v.near[k].astype(F32)
        v.first[k] = first
        left = (first * gain_cut(k, 1)).astype(BF16)
        squares = squares + jnp.sum(first * first, axis=1, keepdims=True)
        xs_part = xs_part + nn_dot(left, v.wx_t[columns(k, block), :])
        z_part = z_part + nn_dot(left, v.wz_t[columns(k, block), :])
    scale = lax.rsqrt(squares / dim + EPS)
    v.scale[...] = jnp.broadcast_to(scale, v.scale.shape)
    v.xz[me_k, me_t] = jnp.concatenate([xs_part * scale, z_part * scale], axis=1).astype(BF16)
    for copy in to_leads(v.xz, m.xz):
        copy.start()
        sent.append(copy)

    @pl.when(me_t != lead)
    def _():
        to_home(v.xz, m.xz).start()
        turn_ffn(1)

    def proj_sends():
        for q in far_first():
            yield remote(v.proj.at[me_k], v.proj.at[me_k], m.proj[0].at[q], m.proj[1].at[me_k], q)

    @pl.when(me_t == lead)
    def _():
        with scope("w_bc"):
            for k in kv_peers():
                arrived(v.bc, m.bc, k, k * nt + lead)
        summed = sum(v.bc[k] for k in range(nk)) * v.scale[pl.ds(me_k, 1), :]
        raw = summed[pairs : pairs + 1, :heads] + v.small[0]
        step = jnp.maximum(raw, 0.0) + jnp.log1p(jnp.exp(-jnp.abs(raw)))
        decay = jnp.exp(-step * jnp.exp(v.small[1]))
        bc_new = summed[:pairs].astype(BF16).astype(F32)
        bconv = silu(hist_bc + bc_new * tap_bc)
        bmat, cmat = bconv[:groups], bconv[groups:]
        weight = jnp.sum(bmat * cmat, axis=1, keepdims=True)
        lane = lax.broadcasted_iota(jnp.int32, (groups, heads), 1)
        low_end = lax.broadcasted_iota(jnp.int32, (groups, heads), 0) * (heads // groups)
        mine = (lane >= low_end) & (lane < low_end + heads // groups)
        cross = jnp.sum(jnp.where(mine, weight, 0.0), axis=0, keepdims=True)
        v.coef[me_k] = step * cross + v.small[2]

        def coef_sends():
            for k in kv_peers()[::-1]:
                q = k * nt + lead
                yield remote(
                    v.coef.at[me_k], v.coef.at[me_k], m.coef[0].at[k], m.coef[1].at[me_k], q
                )

        for copy in coef_sends():
            copy.start()
        decay_high, decay_low = split_two(decay)
        spread = expand(jnp.concatenate([decay_high, decay_low], axis=0))
        decay_row = spread[0:1] + spread[1:2]
        lane = lax.broadcasted_iota(jnp.int32, (groups, flat), 1)
        low_end = lax.broadcasted_iota(jnp.int32, (groups, flat), 0) * (flat // groups)
        mine = (lane >= low_end) & (lane < low_end + flat // groups)
        lines = []
        for t in range(nt):
            per_group = nn_dot(cmat.astype(BF16), v.state_b[t])
            read = jnp.sum(jnp.where(mine, per_group, 0.0), axis=0, keepdims=True)
            lines.append(decay_row * read)
        v.mix[me_k] = jnp.concatenate(lines, axis=0).astype(BF16)

        def mix_sends():
            for k in kv_peers()[::-1]:
                q = k * nt + lead
                yield remote(v.mix.at[me_k], v.mix.at[me_k], m.mix[0].at[k], m.mix[1].at[me_k], q)

        for copy in mix_sends():
            copy.start()
        turn_ffn(1)
        with scope("w_hist"):
            for t in range(lead):
                arrived(v.tap, m.tap, t, me_k * nt + t)
                arrived_at(v.hist, m.hist, me_k, t)
            for k in kv_peers():
                for t in range(nt):
                    arrived_at(v.hist, m.hist, k, t)
        with scope("w_wout"):
            lead_load(3).wait()
            for t in range(lead):
                arrived(v.wout, m.wout, t, me_k * nt + t)
        for t in range(nt):
            v.past[t] = jnp.concatenate([v.hist[i, t] for i in range(nk)], axis=0)
        with scope("w_coef"):
            for k in kv_peers():
                arrived(v.coef, m.coef, k, k * nt + lead)
        high, low = split_two(jnp.concatenate([v.coef[i] for i in range(nk)], axis=0))
        spread = expand(jnp.concatenate([high, low], axis=0))
        v.direct[...] = spread[:nk] + spread[nk:]
        with scope("w_mix"):
            for k in kv_peers():
                arrived(v.mix, m.mix, k, k * nt + lead)
        total = jnp.zeros((rows, v.wout.shape[2]), F32)
        for x in range(nk):
            k = flipped(me_k, x)
            at = columns(k, local)
            with scope("w_xz"):
                for t in range(nt)[::-1]:
                    if x or t != lead:
                        arrived_at(v.xz, m.xz, k, t)
            direct = v.direct[:, at]
            for t in range(nt):
                read = jnp.concatenate(
                    [v.mix[i, t : t + 1, at].astype(F32) for i in range(nk)], axis=0
                )
                xs_new = v.xz[k, t, :, :local].astype(F32)
                xconv = silu(v.past[t, :, at] + xs_new * v.tap[t, :, at])
                opened = silu(v.xz[k, t, :, local:].astype(F32))
                mixed = ((read + direct * xconv) * opened).astype(BF16)
                total = total + nn_dot(mixed, v.wout[t, at, :])
        v.proj[me_k] = total.astype(BF16)
        for copy in proj_sends():
            copy.start()
        for copy in mix_sends():
            copy.wait_send()
        for copy in coef_sends():
            copy.wait_send()

    def arriving_blocks():
        for x in range(nk):
            k = flipped(me_k, x)
            with scope("w_proj"):
                if x:
                    arrived(v.proj, m.proj, k, k * nt + lead)
                else:
                    arrived_from_lead(v.proj, m.proj, k)
            second = (v.first[k] + v.proj[k].astype(F32)).astype(BF16).astype(F32)
            if x == 0:
                for t in range(nt):
                    v.second[t] = second[:, t * width : (t + 1) * width]
            yield second, gain_cut(k, 2), columns(k, block)

    hidden = gated(arriving_blocks(), nk - 1)
    loaded("down1")
    for far in ((nk - 1,), tuple(range(nk - 1))[::-1]):
        pieces = {x: nn_dot(hidden, v.down[1, :, columns(flipped(me_k, x), block)]) for x in far}
        for x in far:
            k = flipped(me_k, x)
            for t in range(nt):
                v.cut_b[k * nt + t] = pieces[x][:, t * width : (t + 1) * width].astype(BF16)
        for x in far:
            k = flipped(me_k, x)
            for d in range(nt):
                if x or d:
                    q = k * nt + (d if x else lax.rem(me_t + d, nt))
                    send(v.cut_b.at[q], v.cut.at[me], m.cut[0].at[q], m.cut[1].at[me], q)
    v.cut[me] = v.cut_b[me]
    with scope("w_sent"):
        for copy in sent[:-(n - 1)]:
            copy.wait_send()

        @pl.when(me_t == lead)
        def _():
            for copy in first_sends():
                copy.wait_send()
            for copy in bc_sends():
                copy.wait_send()
            for copy in proj_sends():
                copy.wait_send()

        @pl.when(me_t != lead)
        def _():
            slab_home().wait_send()
            to_home(v.hist, m.hist).wait_send()
            to_home(v.xz, m.xz).wait_send()
            tap_home().wait_send()
            for copy in pushes():
                copy.wait_send()
    with scope("w_cut"):
        for q in all_peers():
            arrived(v.cut, m.cut, q, q)
    total = sum(v.cut[q].astype(F32) for q in range(n))
    out[...] = (v.second[me_t] + 0.5 * total).astype(BF16)
    for copy in sent[-(n - 1) :]:
        copy.wait_send()


def fused_layer(
    nk,
    nt,
    resid,
    norm_gain,
    ffn_gate,
    ffn_up,
    ffn_down,
    w_x,
    w_z,
    w_bc,
    w_dt,
    dt_bias,
    a_log,
    d_skip,
    conv_wx,
    conv_wbc,
    conv_x,
    conv_bc,
    ssm_state,
    w_out,
):
    n = nk * nt
    rows, width = resid.shape
    dim = ffn_gate.shape[1]
    units = ffn_gate.shape[2]
    local = w_x.shape[1] * w_x.shape[2]
    heads, half = conv_x.shape[2], conv_x.shape[3]
    flat = heads * half
    span = w_bc.shape[0]
    lanes = w_bc.shape[3]
    pairs = w_bc.shape[1] * w_bc.shape[2]
    out_cols = w_out.shape[2]
    taps = conv_wx.shape[0]
    block = nt * width
    args = (
        resid,
        norm_gain,
        jnp.swapaxes(ffn_gate, 1, 2),
        jnp.swapaxes(ffn_up, 1, 2),
        ffn_down,
        jnp.transpose(w_x, (1, 2, 0)).reshape(local, dim),
        jnp.transpose(w_z, (1, 2, 0)).reshape(local, dim),
        w_bc.reshape(span * pairs, lanes),
        w_dt.T,
        dt_bias.reshape(1, heads),
        a_log.reshape(1, heads),
        d_skip.reshape(1, heads),
        jnp.swapaxes(conv_wx, 1, 2),
        conv_wbc.reshape(taps, pairs, lanes),
        jnp.swapaxes(conv_x, 2, 3).reshape(taps - 1, half, heads),
        conv_bc.reshape(taps - 1, pairs, lanes),
        ssm_state.reshape(flat, lanes),
        w_out.reshape(flat, out_cols),
    )
    dma = pltpu.SemaphoreType.DMA
    vmem = pltpu.VMEM
    scratch = dict(
        gate=vmem((2, units, dim), BF16),
        up=vmem((2, units, dim), BF16),
        down=vmem((2, units, dim), BF16),
        gate_t=vmem((dim, units), BF16),
        up_t=vmem((dim, units), BF16),
        wx_t=vmem((dim, local), BF16),
        wz_t=vmem((dim, local), BF16),
        wx=vmem((local, dim), BF16),
        wz=vmem((local, dim), BF16),
        wbc=vmem((span * pairs, lanes), BF16),
        wide=vmem((span, pairs * lanes), BF16),
        wdt=vmem((heads, span), BF16),
        state=vmem((nt, flat, lanes), F32),
        state_b=vmem((nt, lanes, flat), BF16),
        wout=vmem((nt, flat, out_cols), BF16),
        small=vmem((3, 1, heads), F32),
        cwx=vmem((taps, half, heads), BF16),
        cwbc=vmem((taps, pairs, lanes), BF16),
        cx=vmem((taps - 1, half, heads), BF16),
        cbc=vmem((taps - 1, pairs, lanes), BF16),
        expand=vmem((heads, flat), BF16),
        perm=vmem((256, 256), BF16),
        rows=vmem((n, rows, width), BF16),
        gain=vmem((n, 3, width), BF16),
        part=vmem((nk, rows, block), BF16),
        slab=vmem((n, rows, block), BF16),
        near=vmem((nk, rows, block), BF16),
        held=vmem((nk - 1, 2, rows, units), F32),
        first=vmem((nk, rows, block), F32),
        scale=vmem((rows, lanes), F32),
        bc_b=vmem((nk * (pairs + 8), lanes), F32),
        bc=vmem((nk, pairs + 8, lanes), F32),
        hist=vmem((nk, nt, 1, flat), F32),
        tap=vmem((nt, 1, flat), F32),
        xz=vmem((nk, nt, rows, 2 * local), BF16),
        past=vmem((nt, rows, flat), F32),
        coef=vmem((nk, 1, heads), F32),
        direct=vmem((nk, flat), F32),
        mix=vmem((nk, nt, flat), BF16),
        proj=vmem((nk, rows, out_cols), BF16),
        second=vmem((nt, rows, width), F32),
        cut_b=vmem((n, rows, width), BF16),
        cut=vmem((n, rows, width), BF16),
    )
    rounds = dict(
        rows=n, gain=n, slab=n, near=n, bc=n, hist=n, xz=n, mix=nk, coef=nk, state=nt, wout=nt, tap=nt, proj=n, cut=n
    )
    sems = {name: (dma((count,)), dma((count,))) for name, count in rounds.items()}
    sems["load"] = dma((17,))
    sems["lead"] = dma((4,))

    def kernel(*refs, **held):
        def body(**flags):
            layer_kernel(nk, nt, *refs, SimpleNamespace(**held), SimpleNamespace(**flags))

        pl.run_scoped(body, **sems)

    return pl.pallas_call(
        kernel,
        out_shape=pltpu.VMEM(resid.shape, resid.dtype),
        in_specs=[pl.BlockSpec(memory_space=pl.ANY)] * len(args),
        out_specs=pl.BlockSpec(memory_space=pltpu.VMEM),
        scratch_shapes=scratch,
        compiler_params=pltpu.CompilerParams(
            collective_id=0, has_side_effects=True, vmem_limit_bytes=60 * 1024 * 1024
        ),
    )(*args)


def fits(nk, nt, resid, w_x, w_bc, conv_x):
    rows, width = resid.shape
    half = conv_x.shape[3]
    pairs = w_bc.shape[1] * w_bc.shape[2]
    return (
        conv_x.shape[0] == 1
        and rows == nk
        and nt > 1
        and nk & (nk - 1) == 0
        and w_bc.shape[0] == nt * width
        and width % 128 == 0
        and (nk * nt * width) % 256 == 0
        and (conv_x.shape[2] * conv_x.shape[3]) % 256 == 0
        and w_bc.shape[0] % 128 == 0
        and (w_x.shape[1] * w_x.shape[2]) % 128 == 0
        and half & (half - 1) == 0
        and pairs & (pairs - 1) == 0
        and pairs % 8 == 0
        and 256 % pairs == 0
        and (w_bc.shape[0] * pairs) % 256 == 0
        and w_bc.shape[3] == 128
        and conv_x.shape[2] < 128
    )


def solution(mesh):
    placed = (
        P("dp", ("kv", "tp")),
        P(None, ("kv", "tp")),
        P(None, None, ("kv", "tp")),
        P(None, None, ("kv", "tp")),
        P(None, ("kv", "tp"), None),
        P(None, "kv", "tp"),
        P(None, "kv", "tp"),
        P("kv", None, None, None),
        P("kv", None),
        P(),
        P(),
        P(),
        P(None, None, "tp"),
        P(),
        P(("dp", "kv"), None, None, "tp"),
        P(("dp", "kv"), None, None, None, None),
        P(("dp", "kv"), None, "tp", None),
        P(None, "tp", "kv"),
    )
    nk, nt = mesh.shape["kv"], mesh.shape["tp"]

    def layer(*args):
        if fits(nk, nt, args[0], args[5], args[7], args[14]):
            return fused_layer(nk, nt, *args)
        return per_device(*args)

    return jax.shard_map(
        layer, mesh=mesh, in_specs=placed, out_specs=P("dp", ("kv", "tp")), check_vma=False
    )
```
